128 devices in a mesh: sp: 16 (over z, y), tp: 8 (over x, core).
Axes of the slice: x: 4, y: 4, z: 4, core: 2. Of those that a mesh axis runs over, the one named last changes fastest.
Arguments:
- tokens: bfloat16 [4096, 4096], P('sp'), may hold values from -64 to 64
- norm_gain: float32 [4096], replicated, may hold values from 0.1 to 1.9
- w_query: bfloat16 [4096, 2048], P('sp', 'tp'), may hold values from -1.09375 to 1.09375
- w_key: bfloat16 [4096, 512], P('sp', 'tp'), may hold values from -0.09375 to 0.09375
- w_value: bfloat16 [4096, 512], P('sp', 'tp'), may hold values from -0.09375 to 0.09375
- w_glu: bfloat16 [4096, 2048], P('sp', 'tp'), may hold values from -0.09375 to 0.09375
- w_gate: bfloat16 [4096, 2048], P('sp', 'tp'), may hold values from -0.09375 to 0.09375
- sink_logit: float32 [32], P('tp'), may hold values from 2 to 6
- conv_taps: bfloat16 [31, 2048], P(None, 'tp'), may hold values from -12.9315817 to 12.9315817
- conv_gain: float32 [2048], P('tp'), may hold values from 0.1 to 1.9
- out_attn: bfloat16 [2048, 4096], P('sp', 'tp'), may hold values from -0.5 to 0.5
- out_conv: bfloat16 [2048, 4096], P('sp', 'tp'), may hold values from -0.125 to 0.125
Outputs:
- mixed: bfloat16 [4096, 4096], P('sp', 'tp')
The draws below stay inside these ranges and needn't reach their ends.
All inputs are finite; a program needn't handle non-finite values.
Results may differ from the reference program's by a relative error of at most 0.008.
The reference program's roundings to bfloat16 on the way count: a program that leaves them out, or rounds other values in their place, can miss the bound.
Values may be sent and summed in bfloat16 or wider, within the bound.
A program may use at most 64 MiB of HBM per device.

```python
import math
import jax
import jax.numpy as jnp
from jax import lax

D = 4096
HEADS = 32
HEAD = 64
KV = 8
CONV = 2048
KSIZE = 31
WINDOW = 128
TOKENS = 4096


def draw_tokens(key, part):
    subkeys = jax.random.split(key, 3)
    row_scale = jnp.exp(jax.random.uniform(subkeys[0], (TOKENS, 1), jnp.float32, 0.0, math.log(4.0)))
    col_scale = jnp.exp(jax.random.uniform(subkeys[1], (1, D), jnp.float32, 0.0, math.log(4.0)))
    raw_draw = jnp.clip(jax.random.normal(subkeys[2], (TOKENS, D), jnp.float32), -4.0, 4.0)
    return (raw_draw * row_scale * col_scale).astype(jnp.bfloat16)


def draw_w_query(key, part):
    spread = D ** (-0.5)
    raw_draw = jnp.clip(jax.random.normal(key, (D, HEADS * HEAD), jnp.float32), -4.0, 4.0)
    return (raw_draw * spread).astype(jnp.bfloat16)


def draw_conv_taps(key, part):
    subkeys = jax.random.split(key, 2)
    channel = jnp.arange(CONV, dtype=jnp.float32)[None, :] / CONV
    jitter = jnp.exp(jax.random.uniform(subkeys[0], (1, CONV), jnp.float32, math.log(0.7), math.log(1.4)))
    rising = 10.0 ** channel
    raw_draw = jnp.clip(jax.random.normal(subkeys[1], (KSIZE, CONV), jnp.float32), -4.0, 4.0)
    return (raw_draw * rising * jitter * KSIZE ** (-0.5)).astype(jnp.bfloat16)


def steps_of(rng, shape, shards, smallest, largest):
    level = 1.0
    for dim, blocks in shards:
        heights = jax.random.uniform(jax.random.fold_in(jax.random.fold_in(rng, 6), dim), (blocks,), jnp.float32, smallest / len(shards), largest / len(shards))
        level = level * jnp.repeat(jnp.exp(heights), shape[dim] // blocks).reshape((-1,) + (1,) * (len(shape) - 1 - dim))
    return level


def scatter_about(stream_key, shape, width, limit, pieces=(), held_as=jnp.bfloat16):
    gain = steps_of(stream_key, shape, pieces, -0.22, 0.18) if pieces else 1.0
    array = jax.random.normal(stream_key, shape, jnp.float32) * width * gain
    return jnp.minimum(jnp.maximum(array, -limit), limit).astype(held_as)


def setup_inputs(seed: int = 0) -> dict:
    key_of = jax.random.split(jax.random.key(seed), 13)
    tokens = draw_tokens(jax.random.fold_in(key_of[12], 71), 0)
    norm_gain = jnp.clip(1.0 + 0.18 * jax.random.normal(key_of[1], (D,), jnp.float32), 0.1, 1.9)
    w_query = draw_w_query(jax.random.fold_in(key_of[12], 71), 0)
    w_key = scatter_about(key_of[3], (D, KV * HEAD), D ** -0.5, 0.09375, ((0, 16), (1, 8)))
    w_value = scatter_about(key_of[4], (D, KV * HEAD), D ** -0.5, 0.09375, ((0, 16), (1, 8)))
    w_glu = scatter_about(key_of[5], (D, CONV), D ** -0.5, 0.09375, ((0, 16), (1, 8)))
    w_gate = scatter_about(key_of[6], (D, CONV), D ** -0.5, 0.09375, ((0, 16), (1, 8)))
    sink_logit = jnp.clip(2.0 + 4.0 * jax.random.uniform(key_of[7], (HEADS,), jnp.float32) ** steps_of(key_of[7], (HEADS,), ((0, 8),), -0.2, 0.2), 2.0, 6.0)
    conv_taps = draw_conv_taps(jax.random.fold_in(key_of[12], 71), 0)
    conv_gain = jnp.clip(1.0 + 0.18 * jax.random.normal(key_of[9], (CONV,), jnp.float32), 0.1, 1.9)
    out_attn = scatter_about(key_of[10], (HEADS * HEAD, D), (HEADS * HEAD // 16) ** -0.5, 0.5, ((0, 16), (1, 8)))
    out_conv = scatter_about(key_of[11], (CONV, D), CONV ** -0.5, 0.125, ((0, 16), (1, 8)))
    return {"tokens": tokens, "norm_gain": norm_gain, "w_query": w_query, "w_key": w_key, "w_value": w_value, "w_glu": w_glu, "w_gate": w_gate, "sink_logit": sink_logit, "conv_taps": conv_taps, "conv_gain": conv_gain, "out_attn": out_attn, "out_conv": out_conv}


def rotate_heads(values, positions):
    half_width = values.shape[-1] // 2
    frequency = 10000.0 ** (-jnp.arange(half_width, dtype=jnp.float32) * 2.0 / values.shape[-1])
    angles = positions.astype(jnp.float32)[:, None] * frequency[None, :]
    cosine = jnp.cos(angles)[:, None, :]
    sine_part = jnp.sin(angles)[:, None, :]
    first_half = values[..., :half_width]
    second_half = values[..., half_width:]
    return jnp.concatenate([first_half * cosine - second_half * sine_part, second_half * cosine + first_half * sine_part], axis=-1)

def window_attention(operands):
    queries, keys_rot, values_bf, sinks = operands
    total_rows, group_size, head_dimension = queries.shape
    block_count = total_rows // WINDOW
    query_block_rows = queries.reshape(block_count, WINDOW, group_size, head_dimension).astype(jnp.float32)
    key_blocks = keys_rot.reshape(block_count, WINDOW, head_dimension).astype(jnp.float32)
    value_blocks = values_bf.reshape(block_count, WINDOW, head_dimension).astype(jnp.float32)
    empty_block = jnp.zeros((1, WINDOW, head_dimension), jnp.float32)
    key_pair_rows = jnp.concatenate([jnp.concatenate([empty_block, key_blocks[:-1]], axis=0), key_blocks], axis=1)
    value_pair_rows = jnp.concatenate([jnp.concatenate([empty_block, value_blocks[:-1]], axis=0), value_blocks], axis=1)
    score_matrix = jnp.einsum('schn,svn->shcv', query_block_rows, key_pair_rows) * (1.0 / math.sqrt(head_dimension))
    block_ids = jnp.arange(block_count, dtype=jnp.int32)[:, None, None]
    query_pos = block_ids * WINDOW + jnp.arange(WINDOW, dtype=jnp.int32)[None, :, None]
    key_pos = (block_ids - 1) * WINDOW + jnp.arange(2 * WINDOW, dtype=jnp.int32)[None, None, :]
    distance = query_pos - key_pos
    allowed = (distance >= 0) & (distance < WINDOW) & (key_pos >= 0)
    score_matrix = jnp.where(allowed[:, None], score_matrix, -1e+30)
    sink_col = sinks.astype(jnp.float32)[None, :, None, None]
    highest = jnp.maximum(lax.optimization_barrier(jnp.max(score_matrix, axis=-1, keepdims=True)), sink_col)
    weights_exp = jnp.exp(score_matrix - highest)
    denom_total = lax.optimization_barrier(jnp.sum(weights_exp, axis=-1, keepdims=True)) + jnp.exp(sink_col - highest)
    weights_bfloat_half = (weights_exp / denom_total).astype(jnp.bfloat16)
    attended_values = jnp.einsum('jxcp,jpi->jcxi', weights_bfloat_half.astype(jnp.float32), value_pair_rows).astype(jnp.bfloat16)
    return attended_values.reshape(total_rows, group_size, head_dimension)

def reference(tokens, norm_gain, w_query, w_key, w_value, w_glu, w_gate, sink_logit, conv_taps, conv_gain, out_attn, out_conv):
    total_rows = tokens.shape[0]
    tokens_f = tokens.astype(jnp.float32)
    normed = (tokens_f * lax.rsqrt(lax.optimization_barrier(jnp.mean(tokens_f * tokens_f, axis=1, keepdims=True)) + 1e-06) * norm_gain.astype(jnp.float32)).astype(jnp.bfloat16)
    positions = jnp.arange(total_rows, dtype=jnp.int32)
    queries = rotate_heads(jnp.dot(normed, w_query, preferred_element_type=jnp.float32).reshape(total_rows, HEADS, HEAD), positions).astype(jnp.bfloat16)
    keys_rot = rotate_heads(jnp.dot(normed, w_key, preferred_element_type=jnp.float32).reshape(total_rows, KV, HEAD), positions).astype(jnp.bfloat16)
    values_bf = jnp.dot(normed, w_value, preferred_element_type=jnp.float32).astype(jnp.bfloat16).reshape(total_rows, KV, HEAD)
    group_size = HEADS // KV
    query_heads = jnp.transpose(queries.reshape(total_rows, KV, group_size, HEAD), (1, 0, 2, 3))
    key_heads = jnp.transpose(keys_rot, (1, 0, 2))
    value_heads = jnp.transpose(values_bf, (1, 0, 2))
    sink_heads = sink_logit.reshape(KV, group_size)
    attended_values = lax.map(window_attention, (query_heads, key_heads, value_heads, sink_heads))
    attended_values = jnp.transpose(attended_values, (1, 0, 2, 3)).reshape(total_rows, HEADS * HEAD)
    glu_part = jnp.dot(normed, w_glu, preferred_element_type=jnp.float32)
    gate_part = jnp.dot(normed, w_gate, preferred_element_type=jnp.float32)
    gated = (glu_part * jax.nn.sigmoid(gate_part)).astype(jnp.bfloat16)
    extended = jnp.concatenate([jnp.zeros((KSIZE - 1, CONV), jnp.float32), gated.astype(jnp.float32)], axis=0)
    filtered = lax.conv_general_dilated(extended[None], conv_taps.astype(jnp.float32)[:, None, :], (1,), 'VALID', dimension_numbers=('NWC', 'WIO', 'NWC'), feature_group_count=CONV, precision=lax.Precision.HIGHEST)[0]
    mean_value = lax.optimization_barrier(jnp.sum(filtered, axis=1)) / CONV
    variance = lax.optimization_barrier(jnp.sum(filtered * filtered, axis=1)) / CONV - mean_value * mean_value
    scaled = (filtered - mean_value[:, None]) * lax.rsqrt(variance + 1e-05)[:, None] * conv_gain.astype(jnp.float32)
    conv_out = jax.nn.silu(scaled).astype(jnp.bfloat16)
    mixed = jnp.dot(attended_values, out_attn, preferred_element_type=jnp.float32) + jnp.dot(conv_out, out_conv, preferred_element_type=jnp.float32)
    return mixed.astype(jnp.bfloat16)
```

```python
import functools

import jax
import jax.numpy as jnp
import numpy as np
from jax import lax
from jax.experimental import pallas as pl
from jax.experimental.pallas import tpu as pltpu
from jax.sharding import PartitionSpec as P

MESH = pl.DeviceIdType.MESH
F32 = jnp.float32
BF16 = jnp.bfloat16

ROWS = 256
D = 4096
HEAD = 64
CONV = 2048
KSIZE = 31
WINDOW = 128
WIDTH = 896
KV0, GLU0, GATE0, Q0 = 0, 128, 384, 640
OUTW = 512
N_GATHER = 44


def rope_tables():
    freq = (10000.0 ** (-np.arange(32, dtype=np.float64) * 2.0 / HEAD)).astype(np.float32)
    lanes = np.tile(freq.astype(np.float64), 4)[None, :]
    inner = np.arange(ROWS, dtype=np.float64)[:, None] * lanes
    outer = np.arange(16, dtype=np.float64)[:, None] * ROWS * lanes
    return tuple(f(a).astype(np.float32) for a in (inner, outer) for f in (np.cos, np.sin))


class Gather:
    def __init__(self, piece, half_rows, send_sem, recv_sem, z, y, t):
        self.piece, self.half_rows = piece, half_rows
        self.send_sem, self.recv_sem = send_sem, recv_sem
        self.z, self.y, self.t = z, y, t
        self.index = {}
        self.sent = []

    def rel(self, h, o1, o2):
        dy, dz = (o1, o2) if h == 0 else (o2, o1)
        return lax.rem(self.z + (dz + 4), 4) * 4 + lax.rem(self.y + (dy + 4), 4)

    def rows(self, part):
        n = self.half_rows
        return {"full": (0, n), "lo": (0, n // 2), "hi": (n // 2, n // 2)}[part]

    def make(self, key, h, o1, o2, part, to):
        k = self.index.setdefault(key, len(self.index))
        ref = self.piece(self.rel(h, o1, o2), h, *self.rows(part))
        return pltpu.make_async_remote_copy(
            src_ref=ref,
            dst_ref=ref,
            send_sem=self.send_sem.at[k],
            recv_sem=self.recv_sem.at[k],
            device_id=(self.rel(h, *to), self.t),
            device_id_type=MESH,
        )

    def send(self, key, h, o1, o2, part, to):
        copy = self.make(key, h, o1, o2, part, to)
        copy.start()
        self.sent.append(copy)

    def t1_send(self):
        for h in (0, 1):
            for d in (1, -1):
                self.send(("T1", h, d), h, 0, 0, "full", (d, 0))

    def t1_wait(self):
        for h in (0, 1):
            for d in (1, -1):
                self.make(("T1", h, d), h, -d, 0, "full", (d, 0)).wait_recv()

    def f1_send(self):
        for h in (0, 1):
            for d in (1, -1):
                self.send(("F1", h, d), h, -d, 0, "lo" if d == 1 else "hi", (d, 0))

    def f1_wait(self):
        for h in (0, 1):
            for d in (1, -1):
                self.make(("F1", h, d), h, 2, 0, "lo" if d == 1 else "hi", (d, 0)).wait_recv()

    def t2_send(self, offsets):
        for o, part in offsets:
            for h in (0, 1):
                for d in (1, -1):
                    self.send(("T2", h, o, part, d), h, o, 0, part, (0, d))

    def t2_wait(self, offsets):
        for o, part in offsets:
            for h in (0, 1):
                for d in (1, -1):
                    self.make(("T2", h, o, part, d), h, o, -d, part, (0, d)).wait_recv()

    def f2_send(self, offsets):
        for o in offsets:
            for h in (0, 1):
                for d in (1, -1):
                    self.send(("F2", h, o, d), h, o, -d, "lo" if d == 1 else "hi", (0, d))

    def f2_wait(self, offsets):
        for o in offsets:
            for h in (0, 1):
                for d in (1, -1):
                    self.make(("F2", h, o, d), h, o, 2, "lo" if d == 1 else "hi", (0, d)).wait_recv()

    OWN = ((0, "full"),)
    SIDES = ((-1, "full"), (1, "full"))
    FAR = ((2, "lo"), (2, "hi"))

    def drain(self):
        for copy in self.sent:
            copy.wait_send()


def kernel(
    tokens_hbm,
    gain_ref,
    wq_hbm,
    wk_ref,
    wv_ref,
    wglu_hbm,
    wgate_hbm,
    sink_ref,
    taps_ref,
    cgain_ref,
    oa_hbm,
    oc_hbm,
    cos_in,
    sin_in,
    cos_out,
    sin_out,
    out_ref,
    win,
    wa,
    wc,
    tok,
    normed,
    acc,
    kvext,
    gtail,
    ghalo,
    gext,
    filt,
    taps,
    stat_own,
    stat_all,
    mixa,
    mixc,
    local_sem,
    in_send,
    in_recv,
    out_send,
    out_recv,
    halo_send,
    halo_recv,
    stat_send,
    stat_recv,
    mix_send,
    mix_recv,
):
    s = lax.axis_index("sp")
    t = lax.axis_index("tp")
    z, y = s // 4, lax.rem(s, 4)
    x, core = t // 2, lax.rem(t, 2)

    def al(v, m):
        return pl.multiple_of(v, m)

    own_rows = pl.ds(al(s * ROWS, ROWS), ROWS)
    half = pl.ds(al(s * 128, 128), 128)
    loads = []
    for i, (src, dst) in enumerate(
        (
            (wq_hbm, win.at[own_rows, Q0 : Q0 + 256]),
            (wglu_hbm, win.at[own_rows, GLU0 : GLU0 + 256]),
            (wgate_hbm, win.at[own_rows, GATE0 : GATE0 + 256]),
            (tokens_hbm, tok),
            (oa_hbm, wa.at[half, :]),
            (oc_hbm, wc.at[half, :]),
        )
    ):
        copy = pltpu.make_async_copy(src, dst, local_sem.at[i])
        copy.start()
        loads.append(copy)
    win[own_rows, KV0 : KV0 + 128] = jnp.concatenate([wk_ref[...], wv_ref[...]], axis=1)

    def sp_at(dz, dy):
        return lax.rem(z + (dz + 4), 4) * 4 + lax.rem(y + (dy + 4), 4)

    after, before = lax.rem(s + 1, 16), lax.rem(s + 15, 16)
    barrier = pltpu.get_barrier_semaphore()
    peers = [(sp_at(dz, dy), t) for dz, dy in ((0, 1), (0, -1), (1, 0), (-1, 0))]
    peers += [(after, t), (before, t)]
    peers += [(s, lax.rem(t + i, 8)) for i in range(1, 8)]
    for peer in peers:
        pl.semaphore_signal(barrier, inc=1, device_id=peer, device_id_type=MESH)
    pl.semaphore_wait(barrier, len(peers))
    for copy in loads[:3]:
        copy.wait()

    def in_piece(src, h, lo, n):
        return win.at[pl.ds(al(src * ROWS + (h * 128 + lo), 64), n), :]

    def out_piece(src, h, lo, n):
        return (wa, wc)[h].at[pl.ds(al(src * 128 + lo, 64), n), :]

    g_in = Gather(in_piece, 128, in_send, in_recv, z, y, t)
    g_out = Gather(out_piece, 128, out_send, out_recv, z, y, t)

    g_in.t1_send()
    g_in.t2_send(Gather.OWN)

    loads[3].wait()

    def norm_rows(i, carry):
        rows = pl.ds(al(i * 16, 16), 16)
        v = tok[rows, :].astype(F32)
        scale = lax.rsqrt(jnp.mean(v * v, axis=1, keepdims=True) + 1e-06)
        normed[rows, :] = (v * scale * gain_ref[...]).astype(BF16)
        return carry

    lax.fori_loop(0, ROWS // 16, norm_rows, 0)
    taps[...] = taps_ref[...].astype(F32)

    def block_dot(src, c0, c1):
        rows = pl.ds(al(src * ROWS, ROWS), ROWS)
        return jnp.dot(normed[:, rows], win[rows, c0:c1], preferred_element_type=F32)

    g_in.t1_wait()
    g_in.f1_send()
    acc[...] = block_dot(s, 0, WIDTH)
    g_in.t2_wait(Gather.OWN)
    g_in.f2_send((0,))
    g_in.t2_send(Gather.SIDES)

    def side_block(i, carry):
        d = 1 - 2 * lax.rem(i, 2)
        dz, dy = jnp.where(i < 2, d, 0), jnp.where(i < 2, 0, d)
        src = lax.rem(z + dz + 4, 4) * 4 + lax.rem(y + dy + 4, 4)
        acc[...] += block_dot(src, 0, WIDTH)
        return carry

    def corner_block(i, carry):
        dz, dy = 2 * (i // 2) - 1, 2 * lax.rem(i, 2) - 1
        src = lax.rem(z + dz + 4, 4) * 4 + lax.rem(y + dy + 4, 4)
        acc[...] += block_dot(src, 0, WIDTH)
        return carry

    g_in.f1_wait()
    g_in.t2_send(Gather.FAR)
    lax.fori_loop(0, 4, side_block, 0)
    g_in.t2_wait(Gather.SIDES)
    g_in.f2_send((-1, 1))
    g_in.t2_wait(Gather.FAR)
    g_in.f2_send((2,))
    for copy in loads[4:]:
        copy.wait()
    g_out.t1_send()
    lax.fori_loop(0, 4, corner_block, 0)

    lane = lax.broadcasted_iota(jnp.int32, (ROWS, 128), 1)
    first = lax.rem(lane, 64) < 32
    low = lane < 64
    co, so = cos_out[pl.ds(s, 1), :], sin_out[pl.ds(s, 1), :]
    cosine = co * cos_in[...] - so * sin_in[...]
    sine = so * cos_in[...] + co * sin_in[...]
    sine = jnp.where(first, -sine, sine)

    def rotate(v, cosine, sine):
        other = jnp.where(first, pltpu.roll(v, 96, 1), pltpu.roll(v, 32, 1))
        return v * cosine + other * sine

    g_in.f2_wait((0, -1, 1, 2))

    far_row = pl.ds(al(lax.rem(z + 2, 4) * 1024, 1024), 1024)

    def finish(c0, c1):
        v = acc[:, c0:c1] + jnp.dot(
            normed[:, far_row], win[far_row, c0:c1], preferred_element_type=F32
        )
        for o in (0, 1, -1):
            v = v + block_dot(sp_at(o, 2), c0, c1)
        return v

    halos = []

    def halo(i, src, dst):
        copy = pltpu.make_async_remote_copy(
            src_ref=src,
            dst_ref=dst,
            send_sem=halo_send.at[i],
            recv_sem=halo_recv.at[i],
            device_id=(after, t),
            device_id_type=MESH,
        )
        copy.start()
        halos.append(copy)

    kv = finish(KV0, KV0 + 128)
    kv = rotate(kv, jnp.where(low, cosine, 1.0), jnp.where(low, sine, 0.0))
    kvext[WINDOW:, :] = kv.astype(BF16)
    halo(0, kvext.at[pl.ds(ROWS, WINDOW), :], kvext.at[pl.ds(0, WINDOW), :])

    for c in (0, 128):
        glu = finish(GLU0 + c, GLU0 + c + 128)
        gate = finish(GATE0 + c, GATE0 + c + 128)
        gated = (glu * (1.0 / (1.0 + jnp.exp(-gate)))).astype(BF16)
        gext[32:, c : c + 128] = gated.astype(F32)
        gtail[:, c : c + 128] = gated[ROWS - 32 :, :]
    halo(1, gtail, ghalo)
    g_out.t2_send(Gather.OWN)

    queries = []
    for c in (0, 128):
        q = rotate(finish(Q0 + c, Q0 + c + 128), cosine, sine).astype(BF16)
        queries.append(q)

    halos[1].wait_recv()
    gext[:32, :] = jnp.where(s > 0, ghalo[...].astype(F32), 0.0)

    total = jnp.zeros((ROWS, 1), F32)
    for c in (0, 128):
        for r in range(0, ROWS, 64):
            f = jnp.zeros((64, 128), F32)
            for k in range(KSIZE):
                f = f + taps[k : k + 1, c : c + 128] * gext[r + 2 + k : r + 66 + k, c : c + 128]
            filt[r : r + 64, c : c + 128] = f
    f = filt[...]
    row_sum = jnp.sum(f, axis=1, keepdims=True)
    row_square = jnp.sum(f * f, axis=1, keepdims=True)
    stat = jnp.where(lane == 0, row_sum, jnp.where(lane == 1, row_square, 0.0))
    stat_own[...] = stat.T[:8, :]
    stats = []
    for i in range(1, 8):
        copy = pltpu.make_async_remote_copy(
            src_ref=stat_own,
            dst_ref=stat_all.at[i],
            send_sem=stat_send.at[i - 1],
            recv_sem=stat_recv.at[i - 1],
            device_id=(s, lax.rem(t + i, 8)),
            device_id_type=MESH,
        )
        copy.start()
        stats.append(copy)

    g_out.t1_wait()
    g_out.f1_send()

    halos[0].wait_recv()
    kvf = kvext[...].astype(F32)
    swapped = pltpu.roll(kvf, 64, 1)
    lane_e = lax.broadcasted_iota(jnp.int32, (ROWS + WINDOW, 128), 1)
    low_e = lane_e < 64
    keys = jnp.where(low_e, kvf, swapped).astype(BF16)
    vals = jnp.where(low_e, swapped, kvf).astype(BF16)
    zero = jnp.zeros((WINDOW, 128), BF16)
    low_b = low[:WINDOW, :]
    head = lax.broadcasted_iota(jnp.int32, (4 * WINDOW, 1), 0) // WINDOW
    sink = jnp.where(
        head == 0,
        sink_ref[0, 0],
        jnp.where(head == 1, sink_ref[0, 1], jnp.where(head == 2, sink_ref[0, 2], sink_ref[0, 3])),
    )
    own_cols = pl.ds(al(t * 256, 256), 256)

    row_i = lax.rem(lax.broadcasted_iota(jnp.int32, (4 * WINDOW, 2 * WINDOW), 0), WINDOW)
    col_j = lax.broadcasted_iota(jnp.int32, (4 * WINDOW, 2 * WINDOW), 1)
    distance = row_i + WINDOW - col_j
    for b in (1, 0):
        parts = []
        for q in queries:
            qb = q[b * WINDOW : (b + 1) * WINDOW, :]
            parts += [jnp.where(low_b, qb, zero), jnp.where(low_b, zero, qb)]
        stacked = jnp.concatenate(parts, axis=0)
        kb = keys[b * WINDOW : b * WINDOW + 2 * WINDOW, :]
        vb = vals[b * WINDOW : b * WINDOW + 2 * WINDOW, :]
        scores = lax.dot_general(
            stacked, kb, (((1,), (1,)), ((), ())), preferred_element_type=F32
        ) * 0.125
        key_pos = s * ROWS + (b - 1) * WINDOW + col_j
        allowed = (distance >= 0) & (distance < WINDOW) & (key_pos >= 0)
        scores = jnp.where(allowed, scores, -1e30)
        top = jnp.maximum(jnp.max(scores, axis=1, keepdims=True), sink)
        e = jnp.exp(scores - top)
        denom = jnp.sum(e, axis=1, keepdims=True) + jnp.exp(sink - top)
        probs = (e / denom).astype(BF16)
        att = jnp.dot(probs, vb, preferred_element_type=F32)
        for j in (0, 1):
            tile = jnp.where(
                low_b,
                att[2 * j * WINDOW : (2 * j + 1) * WINDOW, :],
                att[(2 * j + 1) * WINDOW : (2 * j + 2) * WINDOW, :],
            )
            cols = pl.ds(al(t * 256 + j * 128, 128), 128)
            mixa[b * WINDOW : (b + 1) * WINDOW, cols] = tile.astype(BF16)

    mix_sent = []

    def tp_at(dx, dc):
        return lax.rem(x + (dx + 4), 4) * 2 + (core if dc == 0 else 1 - core)

    def mix_make(m, key, dx, dc, part, to):
        order = ("X+", "X-", "P0", "F+", "F-", "P+", "P-", "Q+", "Q-")
        k = m * 9 + order.index(key)
        lo, n = {"full": (0, ROWS), "lo": (0, 128), "hi": (128, 128)}[part]
        ref = (mixa, mixc)[m].at[pl.ds(lo, n), pl.ds(al(tp_at(dx, dc) * 256, 256), 256)]
        return pltpu.make_async_remote_copy(
            src_ref=ref,
            dst_ref=ref,
            send_sem=mix_send.at[k],
            recv_sem=mix_recv.at[k],
            device_id=(s, tp_at(*to)),
            device_id_type=MESH,
        )

    def mix_send_one(*args):
        copy = mix_make(*args)
        copy.start()
        mix_sent.append(copy)

    def mix_first(m):
        mix_send_one(m, "X+", 0, 0, "full", (1, 0))
        mix_send_one(m, "X-", 0, 0, "full", (-1, 0))
        mix_send_one(m, "P0", 0, 0, "full", (0, 1))

    def mix_second(m):
        for key, fkey, pkey, d, part in (("X+", "F+", "P+", 1, "lo"), ("X-", "F-", "P-", -1, "hi")):
            mix_make(m, key, -d, 0, "full", (d, 0)).wait_recv()
            mix_send_one(m, fkey, -d, 0, part, (d, 0))
            mix_send_one(m, pkey, -d, 0, "full", (0, 1))

    def mix_third(m):
        for fkey, qkey, d, part in (("F+", "Q+", 1, "lo"), ("F-", "Q-", -1, "hi")):
            mix_make(m, fkey, 2, 0, part, (d, 0)).wait_recv()
            mix_send_one(m, qkey, 2, 0, part, (0, 1))

    def mix_last(m):
        mix_make(m, "P0", 0, 1, "full", (0, 1)).wait_recv()
        for pkey, qkey, d, part in (("P+", "Q+", 1, "lo"), ("P-", "Q-", -1, "hi")):
            mix_make(m, pkey, -d, 1, "full", (0, 1)).wait_recv()
            mix_make(m, qkey, 2, 1, part, (0, 1)).wait_recv()

    mix_first(0)

    g_out.t2_wait(Gather.OWN)
    g_out.f2_send((0,))
    g_out.t2_send(Gather.SIDES)
    g_out.f1_wait()
    g_out.t2_send(Gather.FAR)

    for copy in stats:
        copy.wait_recv()
    whole = stat_own[...]
    for i in range(1, 8):
        whole = whole + stat_all[i]
    whole = jnp.concatenate([whole, jnp.zeros((120, ROWS), F32)], axis=0).T
    mean_value = whole[:, 0:1] * (1.0 / CONV)
    variance = whole[:, 1:2] * (1.0 / CONV) - mean_value * mean_value
    scaled = (filt[...] - mean_value) * lax.rsqrt(variance + 1e-05) * cgain_ref[...]
    mixc[:, own_cols] = (scaled / (1.0 + jnp.exp(-scaled))).astype(BF16)
    mix_first(1)

    mix_second(0)
    g_out.t2_wait(Gather.SIDES)
    g_out.f2_send((-1, 1))
    mix_second(1)
    mix_third(0)
    g_out.t2_wait(Gather.FAR)
    g_out.f2_send((2,))
    mix_third(1)
    mix_last(0)
    mix_last(1)
    g_out.f2_wait((0, -1, 1, 2))

    for c in range(0, OUTW, 256):
        v = jnp.dot(mixa[...], wa[:, c : c + 256], preferred_element_type=F32)
        v = v + jnp.dot(mixc[...], wc[:, c : c + 256], preferred_element_type=F32)
        out_ref[:, c : c + 256] = v.astype(BF16)

    g_in.drain()
    g_out.drain()
    for copy in halos + stats + mix_sent:
        copy.wait_send()


def per_device(
    tokens,
    norm_gain,
    w_query,
    w_key,
    w_value,
    w_glu,
    w_gate,
    sink_logit,
    conv_taps,
    conv_gain,
    out_attn,
    out_conv,
):
    hbm = pl.BlockSpec(memory_space=pl.ANY)
    vmem = pl.BlockSpec(memory_space=pltpu.VMEM)
    smem = pl.BlockSpec(memory_space=pltpu.SMEM)
    dma = pltpu.SemaphoreType.DMA
    tables = [jnp.asarray(a) for a in rope_tables()]
    return pl.pallas_call(
        kernel,
        name="mixer_layer",
        out_shape=jax.ShapeDtypeStruct((ROWS, OUTW), BF16),
        in_specs=[hbm, vmem, hbm, vmem, vmem, hbm, hbm, smem, vmem, vmem, hbm, hbm] + [vmem] * 4,
        out_specs=vmem,
        scratch_shapes=[
            pltpu.VMEM((D, WIDTH), BF16),
            pltpu.VMEM((2048, OUTW), BF16),
            pltpu.VMEM((2048, OUTW), BF16),
            pltpu.VMEM((ROWS, D), BF16),
            pltpu.VMEM((ROWS, D), BF16),
            pltpu.VMEM((ROWS, WIDTH), F32),
            pltpu.VMEM((ROWS + WINDOW, 128), BF16),
            pltpu.VMEM((32, 256), BF16),
            pltpu.VMEM((32, 256), BF16),
            pltpu.VMEM((ROWS + 32, 256), F32),
            pltpu.VMEM((ROWS, 256), F32),
            pltpu.VMEM((KSIZE, 256), F32),
            pltpu.VMEM((8, ROWS), F32),
            pltpu.VMEM((8, 8, ROWS), F32),
            pltpu.VMEM((ROWS, 2048), BF16),
            pltpu.VMEM((ROWS, 2048), BF16),
            dma((6,)),
            dma((N_GATHER,)),
            dma((N_GATHER,)),
            dma((N_GATHER,)),
            dma((N_GATHER,)),
            dma((2,)),
            dma((2,)),
            dma((7,)),
            dma((7,)),
            dma((18,)),
            dma((18,)),
        ],
        compiler_params=pltpu.CompilerParams(
            collective_id=0, has_side_effects=True, vmem_limit_bytes=48 * 1024 * 1024
        ),
    )(
        tokens,
        norm_gain[None, :],
        w_query,
        w_key,
        w_value,
        w_glu,
        w_gate,
        sink_logit[None, :],
        conv_taps,
        conv_gain[None, :],
        out_attn,
        out_conv,
        *tables,
    )


def solution(mesh):
    return jax.shard_map(
        per_device,
        mesh=mesh,
        in_specs=(
            P("sp", None),
            P(),
            P("sp", "tp"),
            P("sp", "tp"),
            P("sp", "tp"),
            P("sp", "tp"),
            P("sp", "tp"),
            P("tp"),
            P(None, "tp"),
            P("tp"),
            P("sp", "tp"),
            P("sp", "tp"),
        ),
        out_specs=P("sp", "tp"),
        check_vma=False,
    )
```

```python
import functools

import jax
import jax.numpy as jnp
import numpy as np
from jax import lax
from jax.experimental import pallas as pl
from jax.experimental.pallas import tpu as pltpu
from jax.sharding import PartitionSpec as P

MESH = pl.DeviceIdType.MESH
F32 = jnp.float32
BF16 = jnp.bfloat16

ROWS = 256
D = 4096
HEAD = 64
CONV = 2048
KSIZE = 31
WINDOW = 128
WIDTH = 896
KV0, GLU0, GATE0, Q0 = 0, 128, 384, 640
OUTW = 512
N_GATHER = 44


def rope_tables():
    freq = (10000.0 ** (-np.arange(32, dtype=np.float64) * 2.0 / HEAD)).astype(np.float32)
    lanes = np.tile(freq.astype(np.float64), 4)[None, :]
    inner = np.arange(ROWS, dtype=np.float64)[:, None] * lanes
    outer = np.arange(16, dtype=np.float64)[:, None] * ROWS * lanes
    return tuple(
        np.concatenate([np.cos(a), np.sin(a)], axis=1).astype(np.float32) for a in (inner, outer)
    )


class Gather:
    def __init__(self, piece, half_rows, send_sem, recv_sem, z, y, t):
        self.piece, self.half_rows = piece, half_rows
        self.send_sem, self.recv_sem = send_sem, recv_sem
        self.z, self.y, self.t = z, y, t
        self.index = {}
        self.sent = []

    def rel(self, h, o1, o2):
        dy, dz = (o1, o2) if h == 0 else (o2, o1)
        return lax.rem(self.z + (dz + 4), 4) * 4 + lax.rem(self.y + (dy + 4), 4)

    def rows(self, part):
        n = self.half_rows
        return {"full": (0, n), "lo": (0, n // 2), "hi": (n // 2, n // 2)}[part]

    def make(self, key, h, o1, o2, part, to):
        k = self.index.setdefault(key, len(self.index))
        ref = self.piece(self.rel(h, o1, o2), h, *self.rows(part))
        return pltpu.make_async_remote_copy(
            src_ref=ref,
            dst_ref=ref,
            send_sem=self.send_sem.at[k],
            recv_sem=self.recv_sem.at[k],
            device_id=(self.rel(h, *to), self.t),
            device_id_type=MESH,
        )

    def send(self, key, h, o1, o2, part, to):
        copy = self.make(key, h, o1, o2, part, to)
        copy.start()
        self.sent.append(copy)

    def t1_send(self):
        for h in (0, 1):
            for d in (1, -1):
                self.send(("T1", h, d), h, 0, 0, "full", (d, 0))

    def t1_wait(self):
        for h in (0, 1):
            for d in (1, -1):
                self.make(("T1", h, d), h, -d, 0, "full", (d, 0)).wait_recv()

    def f1_send(self):
        for h in (0, 1):
            for d in (1, -1):
                self.send(("F1", h, d), h, -d, 0, "lo" if d == 1 else "hi", (d, 0))

    def f1_wait(self):
        for h in (0, 1):
            for d in (1, -1):
                self.make(("F1", h, d), h, 2, 0, "lo" if d == 1 else "hi", (d, 0)).wait_recv()

    def t2_send(self, offsets):
        for o, part in offsets:
            for h in (0, 1):
                for d in (1, -1):
                    self.send(("T2", h, o, part, d), h, o, 0, part, (0, d))

    def t2_wait(self, offsets):
        for o, part in offsets:
            for h in (0, 1):
                for d in (1, -1):
                    self.make(("T2", h, o, part, d), h, o, -d, part, (0, d)).wait_recv()

    def f2_send(self, offsets):
        for o in offsets:
            for h in (0, 1):
                for d in (1, -1):
                    self.send(("F2", h, o, d), h, o, -d, "lo" if d == 1 else "hi", (0, d))

    def f2_wait(self, offsets):
        for o in offsets:
            for h in (0, 1):
                for d in (1, -1):
                    self.make(("F2", h, o, d), h, o, 2, "lo" if d == 1 else "hi", (0, d)).wait_recv()

    OWN = ((0, "full"),)
    SIDES = ((-1, "full"), (1, "full"))
    FAR = ((2, "lo"), (2, "hi"))

    def drain(self):
        for copy in self.sent:
            copy.wait_send()


def kernel(
    tokens_hbm,
    gain_hbm,
    wq_hbm,
    wk_hbm,
    wv_hbm,
    wglu_hbm,
    wgate_hbm,
    sink_hbm,
    taps_hbm,
    cgain_hbm,
    oa_hbm,
    oc_hbm,
    inner_hbm,
    outer_hbm,
    out_ref,
    win,
    wa,
    wc,
    tok,
    normed,
    acc,
    kvext,
    gtail,
    ghalo,
    gext,
    filt,
    kvt,
    gain_ref,
    sink_ref,
    taps_ref,
    cgain_ref,
    inner,
    outer,
    taps,
    stat_own,
    stat_all,
    mixa,
    mixc,
    local_sem,
    in_send,
    in_recv,
    out_send,
    out_recv,
    halo_send,
    halo_recv,
    stat_send,
    stat_recv,
    mix_send,
    mix_recv,
):
    s = lax.axis_index("sp")
    t = lax.axis_index("tp")
    z, y = s // 4, lax.rem(s, 4)
    x, core = t // 2, lax.rem(t, 2)

    def al(v, m):
        return pl.multiple_of(v, m)

    own_rows = pl.ds(al(s * ROWS, ROWS), ROWS)
    half = pl.ds(al(s * 128, 128), 128)
    loads = []
    for i, (src, dst) in enumerate(
        (
            (wq_hbm, win.at[own_rows, Q0 : Q0 + 256]),
            (wglu_hbm, win.at[own_rows, GLU0 : GLU0 + 256]),
            (wgate_hbm, win.at[own_rows, GATE0 : GATE0 + 256]),
            (wk_hbm, kvt.at[0:64, :]),
            (wv_hbm, kvt.at[64:128, :]),
            (tokens_hbm, tok),
            (gain_hbm, gain_ref),
            (taps_hbm, taps_ref),
            (cgain_hbm, cgain_ref),
            (sink_hbm, sink_ref),
            (inner_hbm, inner),
            (outer_hbm.at[s], outer),
            (oa_hbm, wa.at[half, :]),
            (oc_hbm, wc.at[half, :]),
        )
    ):
        copy = pltpu.make_async_copy(src, dst, local_sem.at[i])
        copy.start()
        loads.append(copy)
    def sp_at(dz, dy):
        return lax.rem(z + (dz + 4), 4) * 4 + lax.rem(y + (dy + 4), 4)

    after, before = lax.rem(s + 1, 16), lax.rem(s + 15, 16)
    barrier = pltpu.get_barrier_semaphore()
    peers = [(sp_at(dz, dy), t) for dz, dy in ((0, 1), (0, -1), (1, 0), (-1, 0))]
    peers += [(after, t), (before, t)]
    peers += [(s, lax.rem(t + i, 8)) for i in range(1, 8)]
    for peer in peers:
        pl.semaphore_signal(barrier, inc=1, device_id=peer, device_id_type=MESH)
    for copy in loads[:5]:
        copy.wait()
    win[own_rows, KV0 : KV0 + 128] = kvt[...].astype(F32).T.astype(BF16)
    pl.semaphore_wait(barrier, len(peers))

    def in_piece(src, h, lo, n):
        return win.at[pl.ds(al(src * ROWS + (h * 128 + lo), 64), n), :]

    def out_piece(src, h, lo, n):
        return (wa, wc)[h].at[pl.ds(al(src * 128 + lo, 64), n), :]

    g_in = Gather(in_piece, 128, in_send, in_recv, z, y, t)
    g_out = Gather(out_piece, 128, out_send, out_recv, z, y, t)

    g_in.t1_send()
    g_in.t2_send(Gather.OWN)

    for copy in loads[5:12]:
        copy.wait()

    def norm_rows(i, carry):
        rows = pl.ds(al(i * 16, 16), 16)
        v = tok[rows, :].astype(F32)
        scale = lax.rsqrt(jnp.mean(v * v, axis=1, keepdims=True) + 1e-06)
        normed[rows, :] = (v * scale * gain_ref[...]).astype(BF16)
        return carry

    lax.fori_loop(0, ROWS // 16, norm_rows, 0)
    taps[...] = taps_ref[...].astype(F32)

    def block_dot(src, c0, c1):
        rows = pl.ds(al(src * ROWS, ROWS), ROWS)
        return jnp.dot(normed[:, rows], win[rows, c0:c1], preferred_element_type=F32)

    g_in.t1_wait()
    g_in.f1_send()
    acc[...] = block_dot(s, 0, WIDTH)
    g_in.t2_wait(Gather.OWN)
    g_in.f2_send((0,))
    g_in.t2_send(Gather.SIDES)

    def side_block(i, carry):
        d = 1 - 2 * lax.rem(i, 2)
        dz, dy = jnp.where(i < 2, d, 0), jnp.where(i < 2, 0, d)
        src = lax.rem(z + dz + 4, 4) * 4 + lax.rem(y + dy + 4, 4)
        acc[...] += block_dot(src, 0, WIDTH)
        return carry

    def corner_block(i, carry):
        dz, dy = 2 * (i // 2) - 1, 2 * lax.rem(i, 2) - 1
        src = lax.rem(z + dz + 4, 4) * 4 + lax.rem(y + dy + 4, 4)
        acc[...] += block_dot(src, 0, WIDTH)
        return carry

    g_in.f1_wait()
    g_in.t2_send(Gather.FAR)
    lax.fori_loop(0, 4, side_block, 0)
    g_in.t2_wait(Gather.SIDES)
    g_in.f2_send((-1, 1))
    g_in.t2_wait(Gather.FAR)
    g_in.f2_send((2,))
    for copy in loads[12:]:
        copy.wait()
    g_out.t1_send()
    lax.fori_loop(0, 4, corner_block, 0)

    lane = lax.broadcasted_iota(jnp.int32, (ROWS, 128), 1)
    first = lax.rem(lane, 64) < 32
    low = lane < 64
    co, so = outer[:, 0:128], outer[:, 128:256]
    cosine = co * inner[:, 0:128] - so * inner[:, 128:256]
    sine = so * inner[:, 0:128] + co * inner[:, 128:256]
    sine = jnp.where(first, -sine, sine)

    def rotate(v, cosine, sine):
        other = jnp.where(first, pltpu.roll(v, 96, 1), pltpu.roll(v, 32, 1))
        return v * cosine + other * sine

    g_in.f2_wait((0, -1, 1, 2))

    far_row = pl.ds(al(lax.rem(z + 2, 4) * 1024, 1024), 1024)

    def finish(c0, c1):
        v = acc[:, c0:c1] + jnp.dot(
            normed[:, far_row], win[far_row, c0:c1], preferred_element_type=F32
        )
        for o in (0, 1, -1):
            v = v + block_dot(sp_at(o, 2), c0, c1)
        return v

    halos = []

    def halo(i, src, dst):
        copy = pltpu.make_async_remote_copy(
            src_ref=src,
            dst_ref=dst,
            send_sem=halo_send.at[i],
            recv_sem=halo_recv.at[i],
            device_id=(after, t),
            device_id_type=MESH,
        )
        copy.start()
        halos.append(copy)

    kv = finish(KV0, KV0 + 128)
    kv = rotate(kv, jnp.where(low, cosine, 1.0), jnp.where(low, sine, 0.0))
    kvext[WINDOW:, :] = kv.astype(BF16)
    halo(0, kvext.at[pl.ds(ROWS, WINDOW), :], kvext.at[pl.ds(0, WINDOW), :])

    for c in (0, 128):
        glu = finish(GLU0 + c, GLU0 + c + 128)
        gate = finish(GATE0 + c, GATE0 + c + 128)
        gated = (glu * (1.0 / (1.0 + jnp.exp(-gate)))).astype(BF16)
        gext[32:, c : c + 128] = gated.astype(F32)
        gtail[:, c : c + 128] = gated[ROWS - 32 :, :]
    halo(1, gtail, ghalo)
    g_out.t2_send(Gather.OWN)

    queries = []
    for c in (0, 128):
        q = rotate(finish(Q0 + c, Q0 + c + 128), cosine, sine).astype(BF16)
        queries.append(q)

    halos[1].wait_recv()
    gext[:32, :] = jnp.where(s > 0, ghalo[...].astype(F32), 0.0)

    total = jnp.zeros((ROWS, 1), F32)
    for c in (0, 128):
        for r in range(0, ROWS, 64):
            f = jnp.zeros((64, 128), F32)
            for k in range(KSIZE):
                f = f + taps[k : k + 1, c : c + 128] * gext[r + 2 + k : r + 66 + k, c : c + 128]
            filt[r : r + 64, c : c + 128] = f
    f = filt[...]
    row_sum = jnp.sum(f, axis=1, keepdims=True)
    row_square = jnp.sum(f * f, axis=1, keepdims=True)
    stat = jnp.where(lane == 0, row_sum, jnp.where(lane == 1, row_square, 0.0))
    stat_own[...] = stat.T[:8, :]
    stats = []
    for i in range(1, 8):
        copy = pltpu.make_async_remote_copy(
            src_ref=stat_own,
            dst_ref=stat_all.at[i],
            send_sem=stat_send.at[i - 1],
            recv_sem=stat_recv.at[i - 1],
            device_id=(s, lax.rem(t + i, 8)),
            device_id_type=MESH,
        )
        copy.start()
        stats.append(copy)

    g_out.t1_wait()
    g_out.f1_send()

    halos[0].wait_recv()
    kvf = kvext[...].astype(F32)
    swapped = pltpu.roll(kvf, 64, 1)
    lane_e = lax.broadcasted_iota(jnp.int32, (ROWS + WINDOW, 128), 1)
    low_e = lane_e < 64
    keys = jnp.where(low_e, kvf, swapped).astype(BF16)
    vals = jnp.where(low_e, swapped, kvf).astype(BF16)
    zero = jnp.zeros((WINDOW, 128), BF16)
    low_b = low[:WINDOW, :]
    head = lax.broadcasted_iota(jnp.int32, (4 * WINDOW, 1), 0) // WINDOW
    sink = jnp.where(
        head == 0,
        sink_ref[0:1, 0:1],
        jnp.where(
            head == 1,
            sink_ref[0:1, 1:2],
            jnp.where(head == 2, sink_ref[0:1, 2:3], sink_ref[0:1, 3:4]),
        ),
    )
    own_cols = pl.ds(al(t * 256, 256), 256)

    row_i = lax.rem(lax.broadcasted_iota(jnp.int32, (4 * WINDOW, 2 * WINDOW), 0), WINDOW)
    col_j = lax.broadcasted_iota(jnp.int32, (4 * WINDOW, 2 * WINDOW), 1)
    distance = row_i + WINDOW - col_j
    for b in (1, 0):
        parts = []
        for q in queries:
            qb = q[b * WINDOW : (b + 1) * WINDOW, :]
            parts += [jnp.where(low_b, qb, zero), jnp.where(low_b, zero, qb)]
        stacked = jnp.concatenate(parts, axis=0)
        kb = keys[b * WINDOW : b * WINDOW + 2 * WINDOW, :]
        vb = vals[b * WINDOW : b * WINDOW + 2 * WINDOW, :]
        scores = lax.dot_general(
            stacked, kb, (((1,), (1,)), ((), ())), preferred_element_type=F32
        ) * 0.125
        key_pos = s * ROWS + (b - 1) * WINDOW + col_j
        allowed = (distance >= 0) & (distance < WINDOW) & (key_pos >= 0)
        scores = jnp.where(allowed, scores, -1e30)
        top = jnp.maximum(jnp.max(scores, axis=1, keepdims=True), sink)
        e = jnp.exp(scores - top)
        denom = jnp.sum(e, axis=1, keepdims=True) + jnp.exp(sink - top)
        probs = (e / denom).astype(BF16)
        att = jnp.dot(probs, vb, preferred_element_type=F32)
        for j in (0, 1):
            tile = jnp.where(
                low_b,
                att[2 * j * WINDOW : (2 * j + 1) * WINDOW, :],
                att[(2 * j + 1) * WINDOW : (2 * j + 2) * WINDOW, :],
            )
            cols = pl.ds(al(t * 256 + j * 128, 128), 128)
            mixa[b * WINDOW : (b + 1) * WINDOW, cols] = tile.astype(BF16)

    mix_sent = []

    def tp_at(dx, dc):
        return lax.rem(x + (dx + 4), 4) * 2 + (core if dc == 0 else 1 - core)

    def mix_make(m, key, dx, dc, part, to):
        order = ("X+", "X-", "P0", "F+", "F-", "P+", "P-", "Q+", "Q-")
        k = m * 9 + order.index(key)
        lo, n = {"full": (0, ROWS), "lo": (0, 128), "hi": (128, 128)}[part]
        ref = (mixa, mixc)[m].at[pl.ds(lo, n), pl.ds(al(tp_at(dx, dc) * 256, 256), 256)]
        return pltpu.make_async_remote_copy(
            src_ref=ref,
            dst_ref=ref,
            send_sem=mix_send.at[k],
            recv_sem=mix_recv.at[k],
            device_id=(s, tp_at(*to)),
            device_id_type=MESH,
        )

    def mix_send_one(*args):
        copy = mix_make(*args)
        copy.start()
        mix_sent.append(copy)

    def mix_first(m):
        mix_send_one(m, "X+", 0, 0, "full", (1, 0))
        mix_send_one(m, "X-", 0, 0, "full", (-1, 0))
        mix_send_one(m, "P0", 0, 0, "full", (0, 1))

    def mix_second(m):
        for key, fkey, pkey, d, part in (("X+", "F+", "P+", 1, "lo"), ("X-", "F-", "P-", -1, "hi")):
            mix_make(m, key, -d, 0, "full", (d, 0)).wait_recv()
            mix_send_one(m, fkey, -d, 0, part, (d, 0))
            mix_send_one(m, pkey, -d, 0, "full", (0, 1))

    def mix_third(m):
        for fkey, qkey, d, part in (("F+", "Q+", 1, "lo"), ("F-", "Q-", -1, "hi")):
            mix_make(m, fkey, 2, 0, part, (d, 0)).wait_recv()
            mix_send_one(m, qkey, 2, 0, part, (0, 1))

    def mix_last(m):
        mix_make(m, "P0", 0, 1, "full", (0, 1)).wait_recv()
        for pkey, qkey, d, part in (("P+", "Q+", 1, "lo"), ("P-", "Q-", -1, "hi")):
            mix_make(m, pkey, -d, 1, "full", (0, 1)).wait_recv()
            mix_make(m, qkey, 2, 1, part, (0, 1)).wait_recv()

    mix_first(0)

    g_out.t2_wait(Gather.OWN)
    g_out.f2_send((0,))
    g_out.t2_send(Gather.SIDES)
    g_out.f1_wait()
    g_out.t2_send(Gather.FAR)

    for copy in stats:
        copy.wait_recv()
    whole = stat_own[...]
    for i in range(1, 8):
        whole = whole + stat_all[i]
    whole = jnp.concatenate([whole, jnp.zeros((120, ROWS), F32)], axis=0).T
    mean_value = whole[:, 0:1] * (1.0 / CONV)
    variance = whole[:, 1:2] * (1.0 / CONV) - mean_value * mean_value
    scaled = (filt[...] - mean_value) * lax.rsqrt(variance + 1e-05) * cgain_ref[...]
    mixc[:, own_cols] = (scaled / (1.0 + jnp.exp(-scaled))).astype(BF16)
    mix_first(1)

    mix_second(0)
    g_out.t2_wait(Gather.SIDES)
    g_out.f2_send((-1, 1))
    mix_second(1)
    mix_third(0)
    g_out.t2_wait(Gather.FAR)
    g_out.f2_send((2,))
    mix_third(1)
    mix_last(0)
    mix_last(1)
    g_out.f2_wait((0, -1, 1, 2))

    for c in range(0, OUTW, 256):
        v = jnp.dot(mixa[...], wa[:, c : c + 256], preferred_element_type=F32)
        v = v + jnp.dot(mixc[...], wc[:, c : c + 256], preferred_element_type=F32)
        out_ref[:, c : c + 256] = v.astype(BF16)

    g_in.drain()
    g_out.drain()
    for copy in halos + stats + mix_sent:
        copy.wait_send()


def per_device(
    tokens,
    norm_gain,
    w_query,
    w_key,
    w_value,
    w_glu,
    w_gate,
    sink_logit,
    conv_taps,
    conv_gain,
    out_attn,
    out_conv,
):
    hbm = pl.BlockSpec(memory_space=pltpu.HBM)
    vmem = pl.BlockSpec(memory_space=pltpu.VMEM)
    dma = pltpu.SemaphoreType.DMA
    inner, outer = rope_tables()
    tables = (jnp.asarray(inner), jnp.asarray(outer[:, None, :]))
    return pl.pallas_call(
        kernel,
        name="mixer_layer",
        out_shape=jax.ShapeDtypeStruct((ROWS, OUTW), BF16),
        in_specs=[hbm] * 14,
        out_specs=vmem,
        scratch_shapes=[
            pltpu.VMEM((D, WIDTH), BF16),
            pltpu.VMEM((2048, OUTW), BF16),
            pltpu.VMEM((2048, OUTW), BF16),
            pltpu.VMEM((ROWS, D), BF16),
            pltpu.VMEM((ROWS, D), BF16),
            pltpu.VMEM((ROWS, WIDTH), F32),
            pltpu.VMEM((ROWS + WINDOW, 128), BF16),
            pltpu.VMEM((32, 256), BF16),
            pltpu.VMEM((32, 256), BF16),
            pltpu.VMEM((ROWS + 32, 256), F32),
            pltpu.VMEM((ROWS, 256), F32),
            pltpu.VMEM((128, ROWS), BF16),
            pltpu.VMEM((1, D), F32),
            pltpu.VMEM((1, 4), F32),
            pltpu.VMEM((KSIZE, 256), BF16),
            pltpu.VMEM((1, 256), F32),
            pltpu.VMEM((ROWS, 256), F32),
            pltpu.VMEM((1, 256), F32),
            pltpu.VMEM((KSIZE, 256), F32),
            pltpu.VMEM((8, ROWS), F32),
            pltpu.VMEM((8, 8, ROWS), F32),
            pltpu.VMEM((ROWS, 2048), BF16),
            pltpu.VMEM((ROWS, 2048), BF16),
            dma((14,)),
            dma((N_GATHER,)),
            dma((N_GATHER,)),
            dma((N_GATHER,)),
            dma((N_GATHER,)),
            dma((2,)),
            dma((2,)),
            dma((7,)),
            dma((7,)),
            dma((18,)),
            dma((18,)),
        ],
        compiler_params=pltpu.CompilerParams(
            collective_id=0, has_side_effects=True, vmem_limit_bytes=67043328
        ),
    )(
        tokens,
        norm_gain[None, :],
        w_query,
        w_key.T,
        w_value.T,
        w_glu,
        w_gate,
        sink_logit[None, :],
        conv_taps,
        conv_gain[None, :],
        out_attn,
        out_conv,
        *tables,
    )


def solution(mesh):
    return jax.shard_map(
        per_device,
        mesh=mesh,
        in_specs=(
            P("sp", None),
            P(),
            P("sp", "tp"),
            P("sp", "tp"),
            P("sp", "tp"),
            P("sp", "tp"),
            P("sp", "tp"),
            P("tp"),
            P(None, "tp"),
            P("tp"),
            P("sp", "tp"),
            P("sp", "tp"),
        ),
        out_specs=P("sp", "tp"),
        check_vma=False,
    )
```

```python
import jax
import jax.numpy as jnp
import numpy as np
from jax import lax
from jax.experimental import pallas as pl
from jax.experimental.pallas import tpu as pltpu
from jax.sharding import PartitionSpec as P

MESH = pl.DeviceIdType.MESH
F32 = jnp.float32
BF16 = jnp.bfloat16

ROWS = 256
GROUP = 1024
D = 4096
HEAD = 64
CONV = 2048
KSIZE = 31
WINDOW = 128
WIDTH = 256
OUTW = 512
XCOLS = 384
DCOLS = 512
OUT_SPLIT = 160
SEMS = 64


def rope_tables():
    freq = (10000.0 ** (-np.arange(32, dtype=np.float64) * 2.0 / HEAD)).astype(np.float32)
    lanes = np.tile(freq.astype(np.float64), 4)[None, :]
    inner = np.arange(ROWS, dtype=np.float64)[:, None] * lanes
    outer = np.arange(16, dtype=np.float64)[:, None] * ROWS * lanes
    return tuple(
        np.concatenate([np.cos(a), np.sin(a)], axis=1).astype(np.float32) for a in (inner, outer)
    )


class Net:
    def __init__(self, send_sem, recv_sem, partner):
        self.send_sem, self.recv_sem, self.partner = send_sem, recv_sem, partner
        self.index, self.sent = {}, []

    def make(self, key, src, dst, device):
        k = self.index.setdefault(key, len(self.index))
        assert k < SEMS
        return pltpu.make_async_remote_copy(
            src_ref=src,
            dst_ref=dst,
            send_sem=self.send_sem.at[k],
            recv_sem=self.recv_sem.at[k],
            device_id=device,
            device_id_type=MESH,
        )

    def send(self, key, src, dst, device):
        copy = self.make(key, src, dst, device)
        copy.start()
        self.sent.append(copy)

    def wait(self, key, ref):
        self.make(key, ref, ref, self.partner).wait_recv()

    def drain(self):
        for copy in self.sent:
            copy.wait_send()


def side(d):
    return "lo" if d == 1 else "hi"


class Ring:
    def __init__(self, net, name, ref, device):
        self.net, self.name, self.ref, self.device = net, name, ref, device

    def first(self, items):
        for o, part in items:
            for d in (1, -1):
                r = self.ref(o, 0, part)
                self.net.send((self.name, "T", o, part, d), r, r, self.device(d))

    def first_wait(self, items):
        for o, part in items:
            for d in (1, -1):
                self.net.wait((self.name, "T", o, part, d), self.ref(o, -d, part))

    def second(self, pieces):
        for o in pieces:
            for d in (1, -1):
                r = self.ref(o, -d, side(d))
                self.net.send((self.name, "F", o, d), r, r, self.device(d))

    def second_wait(self, pieces):
        for o in pieces:
            for d in (1, -1):
                self.net.wait((self.name, "F", o, d), self.ref(o, 2, side(d)))

    def give(self, items):
        for o, off, part in items:
            r = self.ref(o, off, part)
            self.net.send((self.name, "P", o, off, part), r, r, self.net.partner)

    def give_wait(self, items):
        for o, off, part in items:
            self.net.wait((self.name, "P", o, off, part), self.ref(o, off, part, False))


OWN = ((0, "full"),)
SIDES = ((-1, "full"), (1, "full"))
FAR = ((2, "lo"), (2, "hi"))


def spread(items, offs):
    return tuple((o, off, part) for o, part in items for off in offs)


def kernel(
    tokens_hbm,
    gain_hbm,
    wq_hbm,
    wk_hbm,
    wv_hbm,
    wglu_hbm,
    wgate_hbm,
    sink_hbm,
    taps_hbm,
    cgain_hbm,
    oa_hbm,
    oc_hbm,
    inner_hbm,
    outer_hbm,
    out_ref,
    wst,
    transit,
    win,
    wo,
    tok,
    nrm,
    acc,
    qbuf,
    kvext,
    keys,
    vals,
    gtail,
    ghalo,
    gext,
    filt,
    kvt,
    gain_ref,
    sink_ref,
    taps_ref,
    cgain_ref,
    inner,
    outer,
    taps,
    stat_own,
    stat_all,
    mx,
    mtransit,
    mixall,
    local_sem,
    w_send,
    w_recv,
    t_send,
    t_recv,
    o_send,
    o_recv,
    m_send,
    m_recv,
    halo_send,
    halo_recv,
    stat_send,
    stat_recv,
):
    s = lax.axis_index("sp")
    t = lax.axis_index("tp")
    z, y = s // 4, lax.rem(s, 4)
    x, core = t // 2, lax.rem(t, 2)

    def al(v, m):
        return pl.multiple_of(v, m)

    def wrap(v, o):
        return lax.rem(v + (o + 4), 4)

    def sp_at(dz, dy):
        return wrap(z, dz) * 4 + wrap(y, dy)

    def tp_at(dx, mine=True):
        return wrap(x, dx) * 2 + (core if mine else 1 - core)

    partner = (s, tp_at(0, False))
    barrier = pltpu.get_barrier_semaphore()
    peers = [(sp_at(dz, dy), t) for dz, dy in ((0, 1), (0, -1), (1, 0), (-1, 0))]
    peers += [(s, tp_at(1)), (s, tp_at(-1)), partner]
    for peer in peers:
        pl.semaphore_signal(barrier, inc=1, device_id=peer, device_id_type=MESH)

    role_half = pl.ds(al(lax.rem(y, 2) * 128, 128), 128)
    loads = {}
    for name, src, dst in (
        ("tok", tokens_hbm, tok),
        ("gain", gain_hbm, gain_ref),
        ("wk", wk_hbm, kvt.at[0:64, :]),
        ("wv", wv_hbm, kvt.at[64:128, :]),
        ("q0", wq_hbm.at[:, 0:128], wst.at[0, :, 0:128]),
        ("q1", wq_hbm.at[:, 128:256], wst.at[1, :, 0:128]),
        ("glu0", wglu_hbm.at[:, 0:128], wst.at[2, :, 0:128]),
        ("glu1", wglu_hbm.at[:, 128:256], wst.at[3, :, 0:128]),
        ("gate0", wgate_hbm.at[:, 0:128], wst.at[2, :, 128:256]),
        ("gate1", wgate_hbm.at[:, 128:256], wst.at[3, :, 128:256]),
        ("oa", oa_hbm, wo.at[pl.ds(al(s * ROWS, ROWS), 128), :]),
        ("oc", oc_hbm, wo.at[pl.ds(al(s * ROWS + 128, 128), 128), :]),
        ("taps", taps_hbm.at[:, role_half], taps_ref),
        ("cgain", cgain_hbm.at[:, role_half], cgain_ref),
        ("sink", sink_hbm, sink_ref),
        ("inner", inner_hbm, inner),
        ("outer", outer_hbm.at[pl.ds(z * 4, 4)], outer),
    ):
        copy = pltpu.make_async_copy(src, dst, local_sem.at[len(loads)])
        copy.start()
        loads[name] = copy

    def loaded(*names):
        for name in names:
            loads[name].wait()

    loaded("wk", "wv")
    kv_t = kvt[...].astype(F32).T.astype(BF16)
    wst[0, :, 128:256] = kv_t
    wst[1, :, 128:256] = kv_t
    loaded("tok", "gain")

    def norm_rows(i, carry):
        v = tok[pl.ds(al(i * 16, 16), 16), :].astype(F32)
        scale = lax.rsqrt(jnp.mean(v * v, axis=1, keepdims=True) + 1e-06)
        nrm[pl.ds(al(y * ROWS + i * 16, 16), 16), :] = (v * scale * gain_ref[...]).astype(BF16)
        return carry

    lax.fori_loop(0, ROWS // 16, norm_rows, 0)
    loaded("q0", "q1", "glu0", "glu1", "gate0", "gate1")
    pl.semaphore_wait(barrier, len(peers))

    w_net = Net(w_send, w_recv, partner)
    t_net = Net(t_send, t_recv, partner)
    o_net = Net(o_send, o_recv, partner)
    m_net = Net(m_send, m_recv, partner)

    def y_dev(d):
        return (sp_at(0, d), t)

    def z_dev(d):
        return (sp_at(d, 0), t)

    def x_dev(d):
        return (s, tp_at(d))

    def part_of(part, n):
        return {"full": (0, n), "lo": (0, n // 2), "hi": (n // 2, n // 2)}[part]

    def win_ref(o, off, part, mine=True):
        lo, n = part_of(part, ROWS)
        return win.at[pl.ds(al(sp_at(off, o) * ROWS + lo, 128), n), :]

    def tok_rows(o, part):
        lo, n = part_of(part, ROWS)
        return pl.ds(al(wrap(y, o) * ROWS + lo, 128), n)

    def tokx_ref(o, off, part, mine=True):
        return nrm.at[tok_rows(o, part), pl.ds(al(tp_at(off, mine) * XCOLS, 128), XCOLS)]

    def tokd_ref(o, off, part, mine=True):
        c = core if mine else 1 - core
        return nrm.at[tok_rows(o, part), pl.ds(al(8 * XCOLS + c * DCOLS, 128), DCOLS)]

    def along_y(ref):
        return lambda o, off, part, mine=True: ref(off, 0, part, mine)

    tx_y = Ring(t_net, "txy", along_y(tokx_ref), y_dev)
    td_y = Ring(t_net, "tdy", along_y(tokd_ref), y_dev)
    tx_x = Ring(t_net, "txx", tokx_ref, x_dev)
    td_p = Ring(t_net, "tdp", tokd_ref, x_dev)
    w_z = Ring(w_net, "wz", win_ref, z_dev)

    def out_ref_of(h):
        base, size = ((0, OUT_SPLIT), (OUT_SPLIT, ROWS - OUT_SPLIT))[h]

        def first(o, off, part, mine=True):
            lo, n = part_of(part, size)
            src = sp_at(0, off) if h == 0 else sp_at(off, 0)
            return wo.at[pl.ds(al(src * ROWS + (base + lo), 16), n), :]

        def second(o, off, part, mine=True):
            lo, n = part_of(part, size)
            src = sp_at(off, o) if h == 0 else sp_at(o, off)
            return wo.at[pl.ds(al(src * ROWS + (base + lo), 16), n), :]

        return first, second

    o_first, o_second = [], []
    for h in (0, 1):
        f, g = out_ref_of(h)
        o_first.append(Ring(o_net, ("of", h), f, (y_dev, z_dev)[h]))
        o_second.append(Ring(o_net, ("os", h), g, (z_dev, y_dev)[h]))

    tx_y.first(OWN)
    for d in (1, -1):
        lo, n = part_of(side(d), ROWS)
        w_net.send(
            ("tr", d), wst.at[wrap(y, 2), pl.ds(lo, n), :], transit.at[(1 - d) // 2], y_dev(d)
        )
    for d in (1, -1):
        w_net.send(("w", d), wst.at[wrap(y, d)], win_ref(0, 0, "full"), y_dev(d))
    for d in (1, -1):
        w_net.send(("wz", "T", 0, "full", d), wst.at[y], win_ref(0, 0, "full"), z_dev(d))
    win[pl.ds(al(s * ROWS, ROWS), ROWS), :] = wst[y]
    loaded("oa", "oc")
    o_first[1].first(OWN)

    tx_y.first_wait(OWN)
    tx_y.second((0,))
    tx_x.first(SIDES)
    tx_x.give(spread(SIDES, (0,)))
    for d in (1, -1):
        lo, n = part_of(side(d), ROWS)
        buf = transit.at[(1 - d) // 2]
        w_net.wait(("tr", d), buf)
        w_net.send(("trf", d), buf, win_ref(-d, 0, side(d)), y_dev(d))
    td_y.first(OWN)
    for d in (1, -1):
        w_net.wait(("w", d), win_ref(-d, 0, "full"))
    w_z.first(SIDES)
    w_z.first_wait(OWN)
    w_z.second((0,))
    tx_y.second_wait((0,))
    tx_x.first(FAR)
    tx_x.give(spread(FAR, (0,)))
    for d in (1, -1):
        w_net.wait(("trf", d), win_ref(2, 0, side(d)))
    w_z.first(FAR)
    tx_x.first_wait(SIDES)
    tx_x.second((-1, 1))
    tx_x.give(spread(SIDES, (1, -1)))
    w_z.first_wait(SIDES)
    w_z.second((-1, 1))
    td_y.first_wait(OWN)
    td_y.second((0,))
    td_p.give(((-1, 0, "full"), (1, 0, "full")))
    o_first[0].first(OWN)
    w_z.first_wait(FAR)
    w_z.second((2,))
    o_second[0].first(OWN)
    tx_x.first_wait(FAR)
    tx_x.second((2,))
    tx_x.give(spread(FAR, (1, -1)))

    loaded("taps", "cgain", "sink", "inner", "outer")
    taps[...] = taps_ref[...].astype(F32)

    w_z.second_wait((0, -1, 1, 2))

    def project(o):
        rows = pl.ds(al(wrap(y, o) * ROWS, ROWS), ROWS)
        acc[rows, :] = jnp.dot(nrm[rows, :], win[...], preferred_element_type=F32)

    project(0)
    tx_x.second_wait((-1, 1))
    tx_x.give(((-1, 2, "lo"), (-1, 2, "hi"), (1, 2, "lo"), (1, 2, "hi")))
    o_first[1].first_wait(OWN)
    o_first[1].second((0,))
    td_y.second_wait((0,))
    td_p.give(((2, 0, "lo"), (2, 0, "hi")))
    o_second[1].first(OWN)
    tx_x.give_wait(spread(SIDES, (0, 1, -1)))
    tx_x.give_wait(((-1, 2, "lo"), (-1, 2, "hi"), (1, 2, "lo"), (1, 2, "hi")))
    td_p.give_wait(((-1, 0, "full"), (1, 0, "full")))
    project(-1)
    project(1)
    tx_x.second_wait((2,))
    tx_x.give(((2, 2, "lo"), (2, 2, "hi")))
    tx_x.give_wait(spread(FAR, (0, 1, -1)))
    tx_x.give_wait(((2, 2, "lo"), (2, 2, "hi")))
    td_p.give_wait(((2, 0, "lo"), (2, 0, "hi")))
    project(2)

    def halo_copy(i, src, dst):
        return pltpu.make_async_remote_copy(
            src_ref=src,
            dst_ref=dst,
            send_sem=halo_send.at[i],
            recv_sem=halo_recv.at[i],
            device_id=z_dev(1),
            device_id_type=MESH,
        )

    lane = lax.broadcasted_iota(jnp.int32, (ROWS, 128), 1)

    def attention():
        first = lax.rem(lane, 64) < 32
        low = lane < 64

        def rotate(v, cosine, sine):
            other = jnp.where(first, pltpu.roll(v, 96, 1), pltpu.roll(v, 32, 1))
            return v * cosine + other * sine

        def fill(b, carry):
            rows = pl.ds(al(b * ROWS, ROWS), ROWS)
            ext = pl.ds(al(b * ROWS + WINDOW, WINDOW), ROWS)
            edge = outer[b]
            co, so = edge[:, 0:128], edge[:, 128:256]
            cosine = co * inner[:, 0:128] - so * inner[:, 128:256]
            sine = so * inner[:, 0:128] + co * inner[:, 128:256]
            sine = jnp.where(first, -sine, sine)
            qbuf[rows, :] = rotate(acc[rows, 0:128], cosine, sine).astype(BF16)
            kv = rotate(
                acc[rows, 128:256], jnp.where(low, cosine, 1.0), jnp.where(low, sine, 0.0)
            )
            kv = kv.astype(BF16)
            kvext[ext, :] = kv
            kv = kv.astype(F32)
            swapped = pltpu.roll(kv, 64, 1)
            keys[ext, :] = jnp.where(low, kv, swapped).astype(BF16)
            vals[ext, :] = jnp.where(low, swapped, kv).astype(BF16)
            return carry

        fill(3, 0)
        halo = halo_copy(0, kvext.at[pl.ds(GROUP, WINDOW), :], kvext.at[pl.ds(0, WINDOW), :])
        halo.start()
        lax.fori_loop(0, 3, fill, 0)

        low_w = low[:WINDOW, :]
        zero = jnp.zeros((WINDOW, 128), BF16)
        second = lax.broadcasted_iota(jnp.int32, (2 * WINDOW, 1), 0) >= WINDOW
        sink_a = jnp.where(y == 0, sink_ref[0:1, 0:1], sink_ref[0:1, 2:3])
        sink_b = jnp.where(y == 0, sink_ref[0:1, 1:2], sink_ref[0:1, 3:4])
        sink = jnp.where(second, sink_b, sink_a)
        row_i = lax.rem(lax.broadcasted_iota(jnp.int32, (2 * WINDOW, 2 * WINDOW), 0), WINDOW)
        col_j = lax.broadcasted_iota(jnp.int32, (2 * WINDOW, 2 * WINDOW), 1)
        distance = row_i + WINDOW - col_j
        near = (distance >= 0) & (distance < WINDOW)

        def attend(b):
            at = al(b * WINDOW, WINDOW)
            q = qbuf[pl.ds(at, WINDOW), :]
            stacked = jnp.concatenate([jnp.where(low_w, q, zero), jnp.where(low_w, zero, q)], axis=0)
            scores = lax.dot_general(
                stacked,
                keys[pl.ds(at, 2 * WINDOW), :],
                (((1,), (1,)), ((), ())),
                preferred_element_type=F32,
            )
            key_pos = z * GROUP + (b - 1) * WINDOW + col_j
            scores = jnp.where(near & (key_pos >= 0), scores * 0.125, -1e30)
            top = jnp.maximum(jnp.max(scores, axis=1, keepdims=True), sink)
            e = jnp.exp(scores - top)
            denom = jnp.sum(e, axis=1, keepdims=True) + jnp.exp(sink - top)
            probs = (e / denom).astype(BF16)
            att = jnp.dot(probs, vals[pl.ds(at, 2 * WINDOW), :], preferred_element_type=F32)
            mx[pl.ds(at, WINDOW), :] = jnp.where(low_w, att[:WINDOW, :], att[WINDOW:, :]).astype(BF16)

        def attend_pair(i, carry):
            attend(2 * i + 2)
            attend(2 * i + 1)
            return carry

        lax.fori_loop(0, 3, attend_pair, 0)
        attend(7)
        halo.wait_recv()
        edge = kvext[0:WINDOW, :].astype(F32)
        swapped = pltpu.roll(edge, 64, 1)
        keys[0:WINDOW, :] = jnp.where(low_w, edge, swapped).astype(BF16)
        vals[0:WINDOW, :] = jnp.where(low_w, swapped, edge).astype(BF16)
        attend(0)
        halo.wait_send()

    def convolution():
        def gate_rows(b, carry):
            rows = pl.ds(al(b * ROWS, ROWS), ROWS)
            g = acc[rows, 0:128] * (1.0 / (1.0 + jnp.exp(-acc[rows, 128:256])))
            gext[pl.ds(al(b * ROWS + 32, 32), ROWS), :] = g.astype(BF16).astype(F32)
            return carry

        gate_rows(3, 0)
        gtail[...] = gext[GROUP : GROUP + 32, :].astype(BF16)
        halo = halo_copy(1, gtail, ghalo)
        halo.start()
        lax.fori_loop(0, 3, gate_rows, 0)

        def filter_rows(r):
            f = jnp.zeros((64, 128), F32)
            for k in range(KSIZE):
                f = f + taps[k : k + 1, :] * gext[r + 2 + k : r + 66 + k, :]
            filt[r : r + 64, :] = f

        for r in range(64, GROUP, 64):
            filter_rows(r)
        halo.wait_recv()
        gext[0:32, :] = jnp.where(z > 0, ghalo[...].astype(F32), 0.0)
        filter_rows(0)

        stat = jnp.zeros((ROWS, 128), F32)
        for b in range(4):
            f = filt[b * ROWS : (b + 1) * ROWS, :]
            stat = jnp.where(lane == 2 * b, jnp.sum(f, axis=1, keepdims=True), stat)
            stat = jnp.where(lane == 2 * b + 1, jnp.sum(f * f, axis=1, keepdims=True), stat)
        stat_own[...] = stat.T[:8, :]
        copies = []
        for dy in (0, 1):
            for i in range(8):
                if dy == 0 and i == 0:
                    continue
                k = dy * 8 + i - 1
                copy = pltpu.make_async_remote_copy(
                    src_ref=stat_own,
                    dst_ref=stat_all.at[k],
                    send_sem=stat_send.at[k],
                    recv_sem=stat_recv.at[k],
                    device_id=(z * 4 + (y if dy == 0 else 5 - y), lax.rem(t + i, 8)),
                    device_id_type=MESH,
                )
                copy.start()
                copies.append(copy)
        whole = stat_own[...]
        for k, copy in enumerate(copies):
            copy.wait_recv()
            whole = whole + stat_all[k]
        whole = jnp.concatenate([whole, jnp.zeros((120, ROWS), F32)], axis=0).T
        for b in range(4):
            rows = slice(b * ROWS, (b + 1) * ROWS)
            mean_value = whole[:, 2 * b : 2 * b + 1] * (1.0 / CONV)
            variance = whole[:, 2 * b + 1 : 2 * b + 2] * (1.0 / CONV) - mean_value * mean_value
            scaled = (filt[rows, :] - mean_value) * lax.rsqrt(variance + 1e-05) * cgain_ref[...]
            mx[rows, :] = (scaled / (1.0 + jnp.exp(-scaled))).astype(BF16)
        for copy in copies:
            copy.wait_send()
        halo.wait_send()

    pl.when(y < 2)(attention)
    pl.when(y >= 2)(convolution)

    def mix_cols(o, off, mine=True):
        yy = wrap(y, o)
        block = 2 * tp_at(off, mine) + lax.rem(yy, 2)
        return pl.ds(al(block * 256 + (yy // 2) * 128, 128), 128)

    def mix_ref(o, off, part, mine=True):
        lo, n = part_of(part, ROWS)
        return mixall.at[pl.ds(lo, n), mix_cols(o, off, mine)]

    m_x = Ring(m_net, "mx", mix_ref, x_dev)
    for d in (1, -1):
        lo, n = part_of(side(d), ROWS)
        src = mx.at[pl.ds(al(wrap(y, 2) * ROWS + lo, 128), n), :]
        m_net.send(("tr", d), src, mtransit.at[(1 - d) // 2], y_dev(d))
    for d in (1, -1):
        src = mx.at[pl.ds(al(wrap(y, d) * ROWS, 128), ROWS), :]
        m_net.send(("m", d), src, mix_ref(0, 0, "full"), y_dev(d))
    mixall[:, mix_cols(0, 0)] = mx[pl.ds(al(y * ROWS, ROWS), ROWS), :]
    m_x.first(OWN)
    m_x.give(spread(OWN, (0,)))

    o_first[0].first_wait(OWN)
    o_first[0].second((0,))
    for d in (1, -1):
        buf = mtransit.at[(1 - d) // 2]
        m_net.wait(("tr", d), buf)
        m_net.send(("trf", d), buf, mix_ref(-d, 0, side(d)), y_dev(d))
    for d in (1, -1):
        m_net.wait(("m", d), mix_ref(-d, 0, "full"))
    m_x.first(SIDES)
    m_x.give(spread(SIDES, (0,)))

    for h in (0, 1):
        o_second[h].first_wait(OWN)
        o_second[h].second((0,))
        o_second[h].first(SIDES)
    for h in (0, 1):
        o_first[h].second_wait((0,))
        o_second[h].first(FAR)
    m_x.first_wait(OWN)
    m_x.second((0,))
    m_x.give(spread(OWN, (1, -1)))
    for d in (1, -1):
        m_net.wait(("trf", d), mix_ref(2, 0, side(d)))
    m_x.first(FAR)
    m_x.give(spread(FAR, (0,)))
    m_x.first_wait(SIDES)
    m_x.second((-1, 1))
    m_x.give(spread(SIDES, (1, -1)))
    for h in (0, 1):
        o_second[h].first_wait(SIDES)
        o_second[h].second((-1, 1))
    m_x.first_wait(FAR)
    m_x.second((2,))
    m_x.give(spread(FAR, (1, -1)))
    for h in (0, 1):
        o_second[h].first_wait(FAR)
        o_second[h].second((2,))
    m_x.second_wait((0, -1, 1, 2))
    last = tuple((o, 2, part) for o in (0, -1, 1, 2) for part in ("lo", "hi"))
    m_x.give(last)
    m_x.give_wait(spread(OWN + SIDES + FAR, (0, 1, -1)))
    m_x.give_wait(last)
    for h in (0, 1):
        o_second[h].second_wait((0, -1, 1, 2))

    for c in range(0, OUTW, 256):
        out_ref[:, c : c + 256] = jnp.dot(
            mixall[...], wo[:, c : c + 256], preferred_element_type=F32
        ).astype(BF16)

    for net in (w_net, t_net, o_net, m_net):
        net.drain()


def per_device(
    tokens,
    norm_gain,
    w_query,
    w_key,
    w_value,
    w_glu,
    w_gate,
    sink_logit,
    conv_taps,
    conv_gain,
    out_attn,
    out_conv,
):
    hbm = pl.BlockSpec(memory_space=pltpu.HBM)
    vmem = pl.BlockSpec(memory_space=pltpu.VMEM)
    dma = pltpu.SemaphoreType.DMA
    inner, outer = rope_tables()
    tables = (jnp.asarray(inner), jnp.asarray(outer[:, None, :]))
    return pl.pallas_call(
        kernel,
        name="mixer_layer",
        out_shape=jax.ShapeDtypeStruct((ROWS, OUTW), BF16),
        in_specs=[hbm] * 14,
        out_specs=vmem,
        scratch_shapes=[
            pltpu.VMEM((4, ROWS, WIDTH), BF16),
            pltpu.VMEM((2, 128, WIDTH), BF16),
            pltpu.VMEM((D, WIDTH), BF16),
            pltpu.VMEM((D, OUTW), BF16),
            pltpu.VMEM((ROWS, D), BF16),
            pltpu.VMEM((GROUP, D), BF16),
            pltpu.VMEM((GROUP, WIDTH), F32),
            pltpu.VMEM((GROUP, 128), BF16),
            pltpu.VMEM((GROUP + WINDOW, 128), BF16),
            pltpu.VMEM((GROUP + WINDOW, 128), BF16),
            pltpu.VMEM((GROUP + WINDOW, 128), BF16),
            pltpu.VMEM((32, 128), BF16),
            pltpu.VMEM((32, 128), BF16),
            pltpu.VMEM((GROUP + 32, 128), F32),
            pltpu.VMEM((GROUP, 128), F32),
            pltpu.VMEM((128, ROWS), BF16),
            pltpu.VMEM((1, D), F32),
            pltpu.VMEM((1, 4), F32),
            pltpu.VMEM((KSIZE, 128), BF16),
            pltpu.VMEM((1, 128), F32),
            pltpu.VMEM((ROWS, 256), F32),
            pltpu.VMEM((4, 1, 256), F32),
            pltpu.VMEM((KSIZE, 128), F32),
            pltpu.VMEM((8, ROWS), F32),
            pltpu.VMEM((15, 8, ROWS), F32),
            pltpu.VMEM((GROUP, 128), BF16),
            pltpu.VMEM((2, 128, 128), BF16),
            pltpu.VMEM((ROWS, D), BF16),
            dma((17,)),
            dma((SEMS,)),
            dma((SEMS,)),
            dma((SEMS,)),
            dma((SEMS,)),
            dma((SEMS,)),
            dma((SEMS,)),
            dma((SEMS,)),
            dma((SEMS,)),
            dma((2,)),
            dma((2,)),
            dma((15,)),
            dma((15,)),
        ],
        compiler_params=pltpu.CompilerParams(
            collective_id=0, has_side_effects=True, vmem_limit_bytes=67043328
        ),
    )(
        tokens,
        norm_gain[None, :],
        w_query,
        w_key.T,
        w_value.T,
        w_glu,
        w_gate,
        sink_logit[None, :],
        conv_taps,
        conv_gain[None, :],
        out_attn,
        out_conv,
        *tables,
    )


def solution(mesh):
    return jax.shard_map(
        per_device,
        mesh=mesh,
        in_specs=(
            P("sp", None),
            P(),
            P("sp", "tp"),
            P("sp", "tp"),
            P("sp", "tp"),
            P("sp", "tp"),
            P("sp", "tp"),
            P("tp"),
            P(None, "tp"),
            P("tp"),
            P("sp", "tp"),
            P("sp", "tp"),
        ),
        out_specs=P("sp", "tp"),
        check_vma=False,
    )
```

```python
import jax
import jax.numpy as jnp
import numpy as np
from jax import lax
from jax.experimental import pallas as pl
from jax.experimental.pallas import tpu as pltpu
from jax.sharding import PartitionSpec as P

MESH = pl.DeviceIdType.MESH
F32 = jnp.float32
BF16 = jnp.bfloat16

ROWS = 256
GROUP = 1024
D = 4096
HEAD = 64
CONV = 2048
KSIZE = 31
WINDOW = 128
WIDTH = 256
OUTW = 512
XCOLS = 384
DCOLS = 512
OUT_SPLIT = 160
SEMS = 20


def rope_tables():
    freq = (10000.0 ** (-np.arange(32, dtype=np.float64) * 2.0 / HEAD)).astype(np.float32)
    lanes = np.tile(freq.astype(np.float64), 4)[None, :]
    inner = np.arange(ROWS, dtype=np.float64)[:, None] * lanes
    outer = np.arange(16, dtype=np.float64)[:, None] * ROWS * lanes
    return tuple(
        np.concatenate([np.cos(a), np.sin(a)], axis=1).astype(np.float32) for a in (inner, outer)
    )


class Net:
    def __init__(self, send_sem, recv_sem, meter, partner):
        self.send_sem, self.recv_sem, self.meter, self.partner = send_sem, recv_sem, meter, partner
        self.index, self.size, self.total = {}, {}, 0

    def send(self, group, src, dst, device):
        k = self.index.setdefault(group, len(self.index))
        assert k < SEMS
        count = src.dtype.itemsize
        for n in src.shape:
            count *= n
        self.size[group] = self.size.get(group, 0) + count
        self.total += count
        pltpu.make_async_remote_copy(
            src_ref=src,
            dst_ref=dst,
            send_sem=self.send_sem.at[0],
            recv_sem=self.recv_sem.at[k],
            device_id=device,
            device_id_type=MESH,
        ).start()

    def await_bytes(self, sem, count):
        tiles = count // 2048
        across = max(n for n in range(1, 33) if tiles % n == 0)
        down = tiles // across
        assert tiles * 2048 == count and down <= 128
        counted = self.meter.at[0 : down * 8, 0 : across * 128]
        pltpu.make_async_copy(counted, counted, sem).wait()

    def wait(self, group):
        self.await_bytes(self.recv_sem.at[self.index[group]], self.size[group])

    def drain(self):
        self.await_bytes(self.send_sem.at[0], self.total)


def side(d):
    return "lo" if d == 1 else "hi"


class Ring:
    def __init__(self, net, name, ref, device):
        self.net, self.name, self.ref, self.device = net, name, ref, device

    def first(self, items):
        for o, part in items:
            for d in (1, -1):
                r = self.ref(o, 0, part)
                self.net.send((self.name, "T", items), r, r, self.device(d))

    def first_wait(self, items):
        self.net.wait((self.name, "T", items))

    def second(self, pieces):
        for o in pieces:
            for d in (1, -1):
                r = self.ref(o, -d, side(d))
                self.net.send((self.name, "F", pieces), r, r, self.device(d))

    def second_wait(self, pieces):
        self.net.wait((self.name, "F", pieces))

    def give(self, items):
        for o, off, part in items:
            r = self.ref(o, off, part)
            self.net.send((self.name, "P", items), r, r, self.net.partner)

    def give_wait(self, items):
        self.net.wait((self.name, "P", items))


OWN = ((0, "full"),)
SIDES = ((-1, "full"), (1, "full"))
FAR = ((2, "lo"), (2, "hi"))


def spread(items, offs):
    return tuple((o, off, part) for o, part in items for off in offs)


HALVES = ("lo", "hi")
OWN0, SIDES0, FAR0 = spread(OWN, (0,)), spread(SIDES, (0,)), spread(FAR, (0,))
OWN2 = tuple((0, 2, part) for part in HALVES)
SIDES2 = tuple((o, 2, part) for o in (-1, 1) for part in HALVES)
FAR2 = tuple((2, 2, part) for part in HALVES)


def kernel(
    tokens_hbm,
    gain_hbm,
    wq_hbm,
    wk_hbm,
    wv_hbm,
    wglu_hbm,
    wgate_hbm,
    sink_hbm,
    taps_hbm,
    cgain_hbm,
    oa_hbm,
    oc_hbm,
    inner_hbm,
    outer_hbm,
    out_ref,
    wst,
    transit,
    win,
    wo,
    tok,
    nrm,
    acc,
    qbuf,
    kvext,
    keys,
    vals,
    gtail,
    ghalo,
    gext,
    kvt,
    gain_ref,
    sink_ref,
    taps_ref,
    cgain_ref,
    gall,
    gfull,
    inner,
    outer,
    taps,
    mx,
    mtransit,
    mixall,
    convn,
    local_sem,
    w_send,
    w_recv,
    t_send,
    t_recv,
    o_send,
    o_recv,
    m_send,
    m_recv,
    g_send,
    g_recv,
    halo_send,
    halo_recv,
):
    s = lax.axis_index("sp")
    t = lax.axis_index("tp")
    z, y = s // 4, lax.rem(s, 4)
    x, core = t // 2, lax.rem(t, 2)

    def al(v, m):
        return pl.multiple_of(v, m)

    def wrap(v, o):
        return lax.rem(v + (o + 4), 4)

    def sp_at(dz, dy):
        return wrap(z, dz) * 4 + wrap(y, dy)

    def tp_at(dx, mine=True):
        return wrap(x, dx) * 2 + (core if mine else 1 - core)

    partner = (s, tp_at(0, False))
    barrier = pltpu.get_barrier_semaphore()
    peers = [(sp_at(dz, dy), t) for dz, dy in ((0, 1), (0, -1), (1, 0), (-1, 0))]
    peers += [(s, tp_at(1)), (s, tp_at(-1)), partner]
    for peer in peers:
        pl.semaphore_signal(barrier, inc=1, device_id=peer, device_id_type=MESH)

    role_half = pl.ds(al(lax.rem(y, 2) * 128, 128), 128)
    loads = {}
    for name, src, dst in (
        ("tok", tokens_hbm, tok),
        ("gain", gain_hbm, gain_ref),
        ("wk", wk_hbm, kvt.at[0:64, :]),
        ("wv", wv_hbm, kvt.at[64:128, :]),
        ("q0", wq_hbm.at[:, 0:128], wst.at[0, :, 0:128]),
        ("q1", wq_hbm.at[:, 128:256], wst.at[1, :, 0:128]),
        ("glu0", wglu_hbm.at[:, 0:128], wst.at[2, :, 0:128]),
        ("glu1", wglu_hbm.at[:, 128:256], wst.at[3, :, 0:128]),
        ("gate0", wgate_hbm.at[:, 0:128], wst.at[2, :, 128:256]),
        ("gate1", wgate_hbm.at[:, 128:256], wst.at[3, :, 128:256]),
        ("oa", oa_hbm, wo.at[s, 0:128, :]),
        ("oc", oc_hbm, wo.at[s, 128:256, :]),
        ("taps", taps_hbm.at[:, role_half], taps_ref),
        ("cgain", cgain_hbm, cgain_ref),
        ("sink", sink_hbm, sink_ref),
        ("inner", inner_hbm, inner),
        ("outer", outer_hbm.at[pl.ds(z * 4, 4)], outer),
    ):
        copy = pltpu.make_async_copy(src, dst, local_sem.at[len(loads)])
        copy.start()
        loads[name] = copy

    def loaded(*names):
        for name in names:
            loads[name].wait()

    loaded("wk", "wv")
    kv_t = kvt[...].astype(F32).T.astype(BF16)
    wst[0, :, 128:256] = kv_t
    wst[1, :, 128:256] = kv_t
    loaded("tok", "gain")

    def norm_rows(i, carry):
        v = tok[pl.ds(al(i * 16, 16), 16), :].astype(F32)
        scale = lax.rsqrt(jnp.mean(v * v, axis=1, keepdims=True) + 1e-06)
        nrm[pl.ds(al(y * ROWS + i * 16, 16), 16), :] = (v * scale * gain_ref[...]).astype(BF16)
        return carry

    lax.fori_loop(0, ROWS // 16, norm_rows, 0)
    loaded("q0", "q1", "glu0", "glu1", "gate0", "gate1")
    pl.semaphore_wait(barrier, len(peers))

    w_net = Net(w_send, w_recv, nrm, partner)
    t_net = Net(t_send, t_recv, nrm, partner)
    o_net = Net(o_send, o_recv, nrm, partner)
    m_net = Net(m_send, m_recv, nrm, partner)
    g_net = Net(g_send, g_recv, nrm, partner)

    def y_dev(d):
        return (sp_at(0, d), t)

    def z_dev(d):
        return (sp_at(d, 0), t)

    def x_dev(d):
        return (s, tp_at(d))

    def part_of(part, n):
        return {"full": (0, n), "lo": (0, n // 2), "hi": (n // 2, n // 2)}[part]

    def win_ref(o, off, part, mine=True):
        lo, n = part_of(part, ROWS)
        return win.at[pl.ds(al(sp_at(off, o) * ROWS + lo, 128), n), :]

    def tok_rows(o, part):
        lo, n = part_of(part, ROWS)
        return pl.ds(al(wrap(y, o) * ROWS + lo, 128), n)

    def tokx_ref(o, off, part, mine=True):
        return nrm.at[tok_rows(o, part), pl.ds(al(tp_at(off, mine) * XCOLS, 128), XCOLS)]

    def tokd_ref(o, off, part, mine=True):
        c = core if mine else 1 - core
        return nrm.at[tok_rows(o, part), pl.ds(al(8 * XCOLS + c * DCOLS, 128), DCOLS)]

    def along_y(ref):
        return lambda o, off, part, mine=True: ref(off, 0, part, mine)

    tx_y = Ring(t_net, "txy", along_y(tokx_ref), y_dev)
    td_y = Ring(t_net, "tdy", along_y(tokd_ref), y_dev)
    tx_x = Ring(t_net, "txx", tokx_ref, x_dev)
    td_p = Ring(t_net, "tdp", tokd_ref, x_dev)
    w_z = Ring(w_net, "wz", win_ref, z_dev)

    def out_ref_of(h):
        base, size = ((0, OUT_SPLIT), (OUT_SPLIT, ROWS - OUT_SPLIT))[h]

        def first(o, off, part, mine=True):
            lo, n = part_of(part, size)
            src = sp_at(0, off) if h == 0 else sp_at(off, 0)
            return wo.at[src, pl.ds(base + lo, n), :]

        def second(o, off, part, mine=True):
            lo, n = part_of(part, size)
            src = sp_at(off, o) if h == 0 else sp_at(o, off)
            return wo.at[src, pl.ds(base + lo, n), :]

        return first, second

    o_first, o_second = [], []
    for h in (0, 1):
        f, g = out_ref_of(h)
        o_first.append(Ring(o_net, ("of", h), f, (y_dev, z_dev)[h]))
        o_second.append(Ring(o_net, ("os", h), g, (z_dev, y_dev)[h]))

    tx_y.first(OWN)
    for d in (1, -1):
        lo, n = part_of(side(d), ROWS)
        w_net.send("tr", wst.at[wrap(y, 2), pl.ds(lo, n), :], transit.at[(1 - d) // 2], y_dev(d))
    for d in (1, -1):
        w_net.send("w", wst.at[wrap(y, d)], win_ref(0, 0, "full"), y_dev(d))
    for d in (1, -1):
        w_net.send("wz", wst.at[y], win_ref(0, 0, "full"), z_dev(d))
    win[pl.ds(al(s * ROWS, ROWS), ROWS), :] = wst[y]
    loaded("oa", "oc")
    o_first[1].first(OWN)
    o_second[0].first(OWN)
    loaded("taps", "cgain", "sink", "inner", "outer")
    taps[...] = taps_ref[...].astype(F32)
    gall[t] = jnp.broadcast_to(cgain_ref[...], (8, 256))

    tx_y.first_wait(OWN)
    tx_y.second((0,))
    tx_x.first(SIDES)
    tx_x.give(SIDES0)
    w_net.wait("tr")
    for d in (1, -1):
        w_net.send("trf", transit.at[(1 - d) // 2], win_ref(-d, 0, side(d)), y_dev(d))
    td_y.first(OWN)
    w_net.wait("w")
    w_z.first(SIDES)
    w_net.wait("wz")
    w_z.second((0,))
    tx_y.second_wait((0,))
    tx_x.first(FAR)
    tx_x.give(FAR0)
    w_net.wait("trf")
    w_z.first(FAR)
    tx_x.first_wait(SIDES)
    tx_x.second((-1, 1))
    tx_x.give(spread(SIDES, (1, -1)))
    w_z.first_wait(SIDES)
    w_z.second((-1, 1))
    td_y.first_wait(OWN)
    td_y.second((0,))
    td_p.give(SIDES0)
    o_first[0].first(OWN)
    tx_x.first_wait(FAR)
    tx_x.second((2,))
    tx_x.give(spread(FAR, (1, -1)))
    o_first[1].first_wait(OWN)
    o_first[1].second((0,))
    o_second[1].first(OWN)
    o_second[1].first(SIDES)
    w_z.first_wait(FAR)
    w_z.second((2,))
    tx_x.second_wait((-1, 1))
    tx_x.give(SIDES2)
    o_first[0].first_wait(OWN)
    o_first[0].second((0,))
    o_second[0].first_wait(OWN)
    o_second[0].second((0,))
    o_second[0].first(SIDES)
    td_y.second_wait((0,))
    td_p.give(FAR0)
    tx_x.second_wait((2,))
    tx_x.give(FAR2)

    def project(o):
        rows = pl.ds(al(wrap(y, o) * ROWS, ROWS), ROWS)
        acc[rows, :] = jnp.dot(nrm[rows, :], win[...], preferred_element_type=F32)

    w_z.second_wait((0,))
    w_z.second_wait((-1, 1))
    w_z.second_wait((2,))
    project(0)
    tx_x.give_wait(SIDES0)
    tx_x.give_wait(spread(SIDES, (1, -1)))
    tx_x.give_wait(SIDES2)
    td_p.give_wait(SIDES0)
    project(-1)
    project(1)
    o_first[1].second_wait((0,))
    o_second[1].first(FAR)
    o_second[1].first_wait(OWN)
    o_second[1].second((0,))
    tx_x.give_wait(FAR0)
    tx_x.give_wait(spread(FAR, (1, -1)))
    tx_x.give_wait(FAR2)
    td_p.give_wait(FAR0)
    project(2)
    o_first[0].second_wait((0,))
    o_second[0].first(FAR)
    for i in range(1, 8):
        g_net.send("gain", gall.at[t], gall.at[t], (s, lax.rem(t + i, 8)))

    def halo_copy(i, src, dst):
        return pltpu.make_async_remote_copy(
            src_ref=src,
            dst_ref=dst,
            send_sem=halo_send.at[i],
            recv_sem=halo_recv.at[i],
            device_id=z_dev(1),
            device_id_type=MESH,
        )

    lane = lax.broadcasted_iota(jnp.int32, (ROWS, 128), 1)

    def attention():
        first = lax.rem(lane, 64) < 32
        low = lane < 64

        def rotate(v, cosine, sine):
            other = jnp.where(first, pltpu.roll(v, 96, 1), pltpu.roll(v, 32, 1))
            return v * cosine + other * sine

        def fill(b, carry):
            rows = pl.ds(al(b * ROWS, ROWS), ROWS)
            ext = pl.ds(al(b * ROWS + WINDOW, WINDOW), ROWS)
            edge = outer[b]
            co, so = edge[:, 0:128], edge[:, 128:256]
            cosine = co * inner[:, 0:128] - so * inner[:, 128:256]
            sine = so * inner[:, 0:128] + co * inner[:, 128:256]
            sine = jnp.where(first, -sine, sine)
            qbuf[rows, :] = rotate(acc[rows, 0:128], cosine, sine).astype(BF16)
            kv = rotate(
                acc[rows, 128:256], jnp.where(low, cosine, 1.0), jnp.where(low, sine, 0.0)
            )
            kv = kv.astype(BF16)
            kvext[ext, :] = kv
            kv = kv.astype(F32)
            swapped = pltpu.roll(kv, 64, 1)
            keys[ext, :] = jnp.where(low, kv, swapped).astype(BF16)
            vals[ext, :] = jnp.where(low, swapped, kv).astype(BF16)
            return carry

        fill(3, 0)
        halo = halo_copy(0, kvext.at[pl.ds(GROUP, WINDOW), :], kvext.at[pl.ds(0, WINDOW), :])
        halo.start()
        lax.fori_loop(0, 3, fill, 0)

        low_w = low[:WINDOW, :]
        zero = jnp.zeros((WINDOW, 128), BF16)
        second = lax.broadcasted_iota(jnp.int32, (2 * WINDOW, 1), 0) >= WINDOW
        sink_a = jnp.where(y == 0, sink_ref[0:1, 0:1], sink_ref[0:1, 2:3])
        sink_b = jnp.where(y == 0, sink_ref[0:1, 1:2], sink_ref[0:1, 3:4])
        sink = jnp.where(second, sink_b, sink_a)
        row_i = lax.rem(lax.broadcasted_iota(jnp.int32, (2 * WINDOW, 2 * WINDOW), 0), WINDOW)
        col_j = lax.broadcasted_iota(jnp.int32, (2 * WINDOW, 2 * WINDOW), 1)
        distance = row_i + WINDOW - col_j
        near = (distance >= 0) & (distance < WINDOW)

        def attend(b):
            at = al(b * WINDOW, WINDOW)
            q = qbuf[pl.ds(at, WINDOW), :]
            stacked = jnp.concatenate([jnp.where(low_w, q, zero), jnp.where(low_w, zero, q)], axis=0)
            scores = lax.dot_general(
                stacked,
                keys[pl.ds(at, 2 * WINDOW), :],
                (((1,), (1,)), ((), ())),
                preferred_element_type=F32,
            )
            key_pos = z * GROUP + (b - 1) * WINDOW + col_j
            scores = jnp.where(near & (key_pos >= 0), scores * 0.125, -1e30)
            top = jnp.maximum(jnp.max(scores, axis=1, keepdims=True), sink)
            e = jnp.exp(scores - top)
            denom = jnp.sum(e, axis=1, keepdims=True) + jnp.exp(sink - top)
            probs = (e / denom).astype(BF16)
            att = jnp.dot(probs, vals[pl.ds(at, 2 * WINDOW), :], preferred_element_type=F32)
            mx[pl.ds(at, WINDOW), :] = jnp.where(low_w, att[:WINDOW, :], att[WINDOW:, :]).astype(BF16)

        def attend_pair(i, carry):
            attend(2 * i + 2)
            attend(2 * i + 1)
            return carry

        lax.fori_loop(0, 3, attend_pair, 0)
        attend(7)
        halo.wait_recv()
        edge = kvext[0:WINDOW, :].astype(F32)
        swapped = pltpu.roll(edge, 64, 1)
        keys[0:WINDOW, :] = jnp.where(low_w, edge, swapped).astype(BF16)
        vals[0:WINDOW, :] = jnp.where(low_w, swapped, edge).astype(BF16)
        attend(0)
        halo.wait_send()

    def convolution():
        def gate_rows(b, carry):
            rows = pl.ds(al(b * ROWS, ROWS), ROWS)
            g = acc[rows, 0:128] * (1.0 / (1.0 + jnp.exp(-acc[rows, 128:256])))
            gext[pl.ds(al(b * ROWS + 32, 32), ROWS), :] = g.astype(BF16).astype(F32)
            return carry

        gate_rows(3, 0)
        gtail[...] = gext[GROUP : GROUP + 32, :].astype(BF16)
        halo = halo_copy(1, gtail, ghalo)
        halo.start()
        lax.fori_loop(0, 3, gate_rows, 0)

        def filter_rows(r):
            f = jnp.zeros((64, 128), F32)
            for k in range(KSIZE):
                f = f + taps[k : k + 1, :] * gext[r + 2 + k : r + 66 + k, :]
            mx[r : r + 64, :] = f.astype(BF16)

        for r in range(64, GROUP, 64):
            filter_rows(r)
        halo.wait_recv()
        gext[0:32, :] = jnp.where(z > 0, ghalo[...].astype(F32), 0.0)
        filter_rows(0)

        halo.wait_send()

    pl.when(y < 2)(attention)
    pl.when(y >= 2)(convolution)

    def mix_ref(o, off, part, mine=True):
        lo, n = part_of(part, ROWS)
        yy = wrap(y, o)
        cols = pl.ds(al(tp_at(off, mine) * 256 + lax.rem(yy, 2) * 128, 128), 128)
        return mixall.at[yy // 2, pl.ds(lo, n), cols]

    m_x = Ring(m_net, "mx", mix_ref, x_dev)
    for d in (1, -1):
        lo, n = part_of(side(d), ROWS)
        src = mx.at[pl.ds(al(wrap(y, 2) * ROWS + lo, 128), n), :]
        m_net.send("tr", src, mtransit.at[(1 - d) // 2], y_dev(d))
    for d in (1, -1):
        src = mx.at[pl.ds(al(wrap(y, d) * ROWS, 128), ROWS), :]
        m_net.send("m", src, mix_ref(0, 0, "full"), y_dev(d))
    own_cols = pl.ds(al(t * 256 + lax.rem(y, 2) * 128, 128), 128)
    mixall[y // 2, :, own_cols] = mx[pl.ds(al(y * ROWS, ROWS), ROWS), :]
    m_x.first(OWN)
    m_x.give(OWN0)
    m_net.wait("tr")
    for d in (1, -1):
        m_net.send("trf", mtransit.at[(1 - d) // 2], mix_ref(-d, 0, side(d)), y_dev(d))
    o_second[0].first_wait(SIDES)
    o_second[0].second((-1, 1))
    m_net.wait("m")
    m_x.first(SIDES)
    m_x.give(SIDES0)
    o_second[1].first_wait(SIDES)
    o_second[1].second((-1, 1))
    m_x.first_wait(OWN)
    m_x.second((0,))
    m_x.give(spread(OWN, (1, -1)))
    m_net.wait("trf")
    m_x.first(FAR)
    m_x.give(FAR0)
    m_x.first_wait(SIDES)
    m_x.second((-1, 1))
    m_x.give(spread(SIDES, (1, -1)))
    o_second[1].first_wait(FAR)
    o_second[1].second((2,))
    o_second[0].first_wait(FAR)
    o_second[0].second((2,))
    m_x.second_wait((0,))
    m_x.give(OWN2)
    m_x.first_wait(FAR)
    m_x.second((2,))
    m_x.give(spread(FAR, (1, -1)))
    m_x.second_wait((-1, 1))
    m_x.give(SIDES2)
    g_net.wait("gain")
    for i in range(8):
        gfull[:, i * 256 : (i + 1) * 256] = gall[i, 0:1, :]
    m_x.second_wait((2,))
    m_x.give(FAR2)
    for items in (OWN0, spread(OWN, (1, -1)), OWN2, SIDES0, spread(SIDES, (1, -1)), SIDES2):
        m_x.give_wait(items)
    for items in (FAR0, spread(FAR, (1, -1)), FAR2):
        m_x.give_wait(items)

    def channel_norm(i, carry):
        rows = pl.ds(al(i * 16, 16), 16)
        f = mixall[1, rows, :].astype(F32)
        mean_value = jnp.sum(f, axis=1, keepdims=True) * (1.0 / CONV)
        variance = jnp.sum(f * f, axis=1, keepdims=True) * (1.0 / CONV) - mean_value * mean_value
        scaled = (f - mean_value) * lax.rsqrt(variance + 1e-05) * gfull[...]
        convn[rows, :] = (scaled / (1.0 + jnp.exp(-scaled))).astype(BF16)
        return carry

    lax.fori_loop(0, ROWS // 16, channel_norm, 0)
    for ring in o_second:
        for pieces in ((0,), (-1, 1), (2,)):
            ring.second_wait(pieces)

    for c in range(0, OUTW, 256):
        w_attn = wo[:, 0:128, c : c + 256].reshape(2048, 256)
        w_conv = wo[:, 128:256, c : c + 256].reshape(2048, 256)
        v = jnp.dot(mixall[0], w_attn, preferred_element_type=F32)
        v = v + jnp.dot(convn[...], w_conv, preferred_element_type=F32)
        out_ref[:, c : c + 256] = v.astype(BF16)

    for net in (w_net, t_net, o_net, m_net, g_net):
        net.drain()


def per_device(
    tokens,
    norm_gain,
    w_query,
    w_key,
    w_value,
    w_glu,
    w_gate,
    sink_logit,
    conv_taps,
    conv_gain,
    out_attn,
    out_conv,
):
    hbm = pl.BlockSpec(memory_space=pltpu.HBM)
    vmem = pl.BlockSpec(memory_space=pltpu.VMEM)
    dma = pltpu.SemaphoreType.DMA
    inner, outer = rope_tables()
    tables = (jnp.asarray(inner), jnp.asarray(outer[:, None, :]))
    return pl.pallas_call(
        kernel,
        name="mixer_layer",
        out_shape=jax.ShapeDtypeStruct((ROWS, OUTW), BF16),
        in_specs=[hbm] * 14,
        out_specs=vmem,
        scratch_shapes=[
            pltpu.VMEM((4, ROWS, WIDTH), BF16),
            pltpu.VMEM((2, 128, WIDTH), BF16),
            pltpu.VMEM((D, WIDTH), BF16),
            pltpu.VMEM((16, ROWS, OUTW), BF16),
            pltpu.VMEM((ROWS, D), BF16),
            pltpu.VMEM((GROUP, D), BF16),
            pltpu.VMEM((GROUP, WIDTH), F32),
            pltpu.VMEM((GROUP, 128), BF16),
            pltpu.VMEM((GROUP + WINDOW, 128), BF16),
            pltpu.VMEM((GROUP + WINDOW, 128), BF16),
            pltpu.VMEM((GROUP + WINDOW, 128), BF16),
            pltpu.VMEM((32, 128), BF16),
            pltpu.VMEM((32, 128), BF16),
            pltpu.VMEM((GROUP + 32, 128), F32),
            pltpu.VMEM((128, ROWS), BF16),
            pltpu.VMEM((1, D), F32),
            pltpu.VMEM((1, 4), F32),
            pltpu.VMEM((KSIZE, 128), BF16),
            pltpu.VMEM((1, 256), F32),
            pltpu.VMEM((8, 8, 256), F32),
            pltpu.VMEM((1, 2048), F32),
            pltpu.VMEM((ROWS, 256), F32),
            pltpu.VMEM((4, 1, 256), F32),
            pltpu.VMEM((KSIZE, 128), F32),
            pltpu.VMEM((GROUP, 128), BF16),
            pltpu.VMEM((2, 128, 128), BF16),
            pltpu.VMEM((2, ROWS, 2048), BF16),
            pltpu.VMEM((ROWS, 2048), BF16),
            dma((17,)),
            dma((1,)),
            dma((SEMS,)),
            dma((1,)),
            dma((SEMS,)),
            dma((1,)),
            dma((SEMS,)),
            dma((1,)),
            dma((SEMS,)),
            dma((1,)),
            dma((1,)),
            dma((2,)),
            dma((2,)),
        ],
        compiler_params=pltpu.CompilerParams(
            collective_id=0, has_side_effects=True, vmem_limit_bytes=67043328
        ),
    )(
        tokens,
        norm_gain[None, :],
        w_query,
        w_key.T,
        w_value.T,
        w_glu,
        w_gate,
        sink_logit[None, :],
        conv_taps,
        conv_gain[None, :],
        out_attn,
        out_conv,
        *tables,
    )


def solution(mesh):
    return jax.shard_map(
        per_device,
        mesh=mesh,
        in_specs=(
            P("sp", None),
            P(),
            P("sp", "tp"),
            P("sp", "tp"),
            P("sp", "tp"),
            P("sp", "tp"),
            P("sp", "tp"),
            P("tp"),
            P(None, "tp"),
            P("tp"),
            P("sp", "tp"),
            P("sp", "tp"),
        ),
        out_specs=P("sp", "tp"),
        check_vma=False,
    )
```

```python
import jax
import jax.numpy as jnp
import numpy as np
from jax import lax
from jax.experimental import pallas as pl
from jax.experimental.pallas import tpu as pltpu
from jax.sharding import PartitionSpec as P

MESH = pl.DeviceIdType.MESH
F32 = jnp.float32
BF16 = jnp.bfloat16

ROWS = 256
GROUP = 1024
D = 4096
HEAD = 64
CONV = 2048
KSIZE = 31
WINDOW = 128
WIDTH = 256
OUTW = 512
XCOLS = 384
DCOLS = 512
OUT_SPLIT = 160
SEMS = 26


def rope_tables():
    freq = (10000.0 ** (-np.arange(32, dtype=np.float64) * 2.0 / HEAD)).astype(np.float32)
    lanes = np.tile(freq.astype(np.float64), 4)[None, :]
    inner = np.arange(ROWS, dtype=np.float64)[:, None] * lanes
    outer = np.arange(16, dtype=np.float64)[:, None] * ROWS * lanes
    return tuple(
        np.concatenate([np.cos(a), np.sin(a)], axis=1).astype(np.float32) for a in (inner, outer)
    )


class Net:
    def __init__(self, send_sem, recv_sem, meter, partner):
        self.send_sem, self.recv_sem, self.meter, self.partner = send_sem, recv_sem, meter, partner
        self.index, self.size, self.total = {}, {}, 0

    def send(self, group, src, dst, device):
        k = self.index.setdefault(group, len(self.index))
        assert k < SEMS
        count = src.dtype.itemsize
        for n in src.shape:
            count *= n
        self.size[group] = self.size.get(group, 0) + count
        self.total += count
        pltpu.make_async_remote_copy(
            src_ref=src,
            dst_ref=dst,
            send_sem=self.send_sem.at[0],
            recv_sem=self.recv_sem.at[k],
            device_id=device,
            device_id_type=MESH,
        ).start()

    def await_bytes(self, sem, count):
        tiles = count // 2048
        across = max(n for n in range(1, 33) if tiles % n == 0)
        down = tiles // across
        assert tiles * 2048 == count and down <= 128
        counted = self.meter.at[0 : down * 8, 0 : across * 128]
        pltpu.make_async_copy(counted, counted, sem).wait()

    def wait(self, group):
        self.await_bytes(self.recv_sem.at[self.index[group]], self.size[group])

    def drain(self):
        self.await_bytes(self.send_sem.at[0], self.total)


def side(d):
    return "lo" if d == 1 else "hi"


class Ring:
    def __init__(self, net, name, ref, device):
        self.net, self.name, self.ref, self.device = net, name, ref, device

    def first(self, *groups):
        for sends in groups:
            for o, part, d in sends:
                r = self.ref(o, 0, part)
                self.net.send((self.name, "T", sends), r, r, self.device(d))

    def first_wait(self, *groups):
        for sends in groups:
            self.net.wait((self.name, "T", sends))

    def second(self, *groups):
        for sends in groups:
            for o, d in sends:
                r = self.ref(o, -d, side(d))
                self.net.send((self.name, "F", sends), r, r, self.device(d))

    def second_wait(self, *groups):
        for sends in groups:
            self.net.wait((self.name, "F", sends))

    def give(self, *groups):
        for items in groups:
            for o, off in items:
                r = self.ref(o, off, "full")
                self.net.send((self.name, "P", items), r, r, self.net.partner)

    def give_wait(self, *groups):
        for items in groups:
            self.net.wait((self.name, "P", items))


def both(*items):
    return tuple((o, part, d) for o, part in items for d in (1, -1))


OWN_A = ((0, "lo", 1), (0, "hi", -1))
OWN_B = ((0, "hi", 1), (0, "lo", -1))
SIDES_A = both((-1, "lo"), (1, "hi"))
SIDES_B = both((-1, "hi"), (1, "lo"))
FAR = both((2, "lo"), (2, "hi"))
OWN_F = ((0, 1), (0, -1))
SIDES_AF = ((-1, 1), (1, -1))
SIDES_BF = ((-1, -1), (1, 1))
FAR_F = ((2, 1), (2, -1))
OWN0, OWN1, OWN2 = ((0, 0),), ((0, 1), (0, -1)), ((0, 2),)
SIDES0, SIDES1, SIDES2 = ((-1, 0), (1, 0)), ((-1, 1), (-1, -1), (1, 1), (1, -1)), ((-1, 2), (1, 2))
FAR0, FAR1, FAR2 = ((2, 0),), ((2, 1), (2, -1)), ((2, 2),)


def kernel(
    tokens_hbm,
    gain_hbm,
    wq_hbm,
    wk_hbm,
    wv_hbm,
    wglu_hbm,
    wgate_hbm,
    sink_hbm,
    taps_hbm,
    cgain_hbm,
    oa_hbm,
    oc_hbm,
    inner_hbm,
    outer_hbm,
    out_ref,
    wst,
    transit,
    win,
    wo,
    tok,
    nrm,
    acc,
    qbuf,
    kvext,
    keys,
    vals,
    gtail,
    ghalo,
    gext,
    kvt,
    gain_ref,
    sink_ref,
    taps_ref,
    cgain_ref,
    gall,
    gfull,
    inner,
    outer,
    taps,
    mx,
    mtransit,
    mixall,
    convn,
    local_sem,
    w_send,
    w_recv,
    t_send,
    t_recv,
    o_send,
    o_recv,
    m_send,
    m_recv,
    g_send,
    g_recv,
    halo_send,
    halo_recv,
):
    s = lax.axis_index("sp")
    t = lax.axis_index("tp")
    z, y = s // 4, lax.rem(s, 4)
    x, core = t // 2, lax.rem(t, 2)

    def al(v, m):
        return pl.multiple_of(v, m)

    def wrap(v, o):
        return lax.rem(v + (o + 4), 4)

    def sp_at(dz, dy):
        return wrap(z, dz) * 4 + wrap(y, dy)

    def tp_at(dx, mine=True):
        return wrap(x, dx) * 2 + (core if mine else 1 - core)

    partner = (s, tp_at(0, False))
    barrier = pltpu.get_barrier_semaphore()
    peers = [(sp_at(dz, dy), t) for dz, dy in ((0, 1), (0, -1), (1, 0), (-1, 0))]
    peers += [(s, tp_at(1)), (s, tp_at(-1)), partner]
    for peer in peers:
        pl.semaphore_signal(barrier, inc=1, device_id=peer, device_id_type=MESH)

    role_half = pl.ds(al(lax.rem(y, 2) * 128, 128), 128)
    loads = {}
    for name, src, dst in (
        ("tok", tokens_hbm, tok),
        ("gain", gain_hbm, gain_ref),
        ("wk", wk_hbm, kvt.at[0:64, :]),
        ("wv", wv_hbm, kvt.at[64:128, :]),
        ("q0", wq_hbm.at[:, 0:128], wst.at[0, :, 0:128]),
        ("q1", wq_hbm.at[:, 128:256], wst.at[1, :, 0:128]),
        ("glu0", wglu_hbm.at[:, 0:128], wst.at[2, :, 0:128]),
        ("glu1", wglu_hbm.at[:, 128:256], wst.at[3, :, 0:128]),
        ("gate0", wgate_hbm.at[:, 0:128], wst.at[2, :, 128:256]),
        ("gate1", wgate_hbm.at[:, 128:256], wst.at[3, :, 128:256]),
        ("oa", oa_hbm, wo.at[s, 0:128, :]),
        ("oc", oc_hbm, wo.at[s, 128:256, :]),
        ("taps", taps_hbm.at[:, role_half], taps_ref),
        ("cgain", cgain_hbm, cgain_ref),
        ("sink", sink_hbm, sink_ref),
        ("inner", inner_hbm, inner),
        ("outer", outer_hbm.at[pl.ds(z * 4, 4)], outer),
    ):
        copy = pltpu.make_async_copy(src, dst, local_sem.at[len(loads)])
        copy.start()
        loads[name] = copy

    def loaded(*names):
        for name in names:
            loads[name].wait()

    loaded("wk", "wv")
    kv_t = kvt[...].astype(F32).T.astype(BF16)
    wst[0, :, 128:256] = kv_t
    wst[1, :, 128:256] = kv_t
    loaded("tok", "gain")

    def norm_rows(i, carry):
        v = tok[pl.ds(al(i * 16, 16), 16), :].astype(F32)
        scale = lax.rsqrt(jnp.mean(v * v, axis=1, keepdims=True) + 1e-06)
        nrm[pl.ds(al(y * ROWS + i * 16, 16), 16), :] = (v * scale * gain_ref[...]).astype(BF16)
        return carry

    lax.fori_loop(0, ROWS // 16, norm_rows, 0)
    loaded("q0", "q1", "glu0", "glu1", "gate0", "gate1")
    pl.semaphore_wait(barrier, len(peers))

    w_net = Net(w_send, w_recv, nrm, partner)
    t_net = Net(t_send, t_recv, nrm, partner)
    o_net = Net(o_send, o_recv, nrm, partner)
    m_net = Net(m_send, m_recv, nrm, partner)
    g_net = Net(g_send, g_recv, nrm, partner)

    def y_dev(d):
        return (sp_at(0, d), t)

    def z_dev(d):
        return (sp_at(d, 0), t)

    def x_dev(d):
        return (s, tp_at(d))

    def part_of(part, n):
        return {"full": (0, n), "lo": (0, n // 2), "hi": (n // 2, n // 2)}[part]

    def win_ref(o, off, part, mine=True):
        lo, n = part_of(part, ROWS)
        return win.at[pl.ds(al(sp_at(off, o) * ROWS + lo, 128), n), :]

    def tok_rows(o, part):
        lo, n = part_of(part, ROWS)
        return pl.ds(al(wrap(y, o) * ROWS + lo, 128), n)

    def tokx_ref(o, off, part, mine=True):
        return nrm.at[tok_rows(o, part), pl.ds(al(tp_at(off, mine) * XCOLS, 128), XCOLS)]

    def tokd_ref(o, off, part, mine=True):
        c = core if mine else 1 - core
        return nrm.at[tok_rows(o, part), pl.ds(al(8 * XCOLS + c * DCOLS, 128), DCOLS)]

    def along_y(ref):
        return lambda o, off, part, mine=True: ref(off, 0, part, mine)

    tx_y = Ring(t_net, "txy", along_y(tokx_ref), y_dev)
    td_y = Ring(t_net, "tdy", along_y(tokd_ref), y_dev)
    tx_x = Ring(t_net, "txx", tokx_ref, x_dev)
    td_p = Ring(t_net, "tdp", tokd_ref, x_dev)
    w_z = Ring(w_net, "wz", win_ref, z_dev)

    def out_ref_of(h):
        base, size = ((0, OUT_SPLIT), (OUT_SPLIT, ROWS - OUT_SPLIT))[h]

        def first(o, off, part, mine=True):
            lo, n = part_of(part, size)
            src = sp_at(0, off) if h == 0 else sp_at(off, 0)
            return wo.at[src, pl.ds(base + lo, n), :]

        def second(o, off, part, mine=True):
            lo, n = part_of(part, size)
            src = sp_at(off, o) if h == 0 else sp_at(o, off)
            return wo.at[src, pl.ds(base + lo, n), :]

        return first, second

    o_first, o_second = [], []
    for h in (0, 1):
        f, g = out_ref_of(h)
        o_first.append(Ring(o_net, ("of", h), f, (y_dev, z_dev)[h]))
        o_second.append(Ring(o_net, ("os", h), g, (z_dev, y_dev)[h]))

    def w_first(name, parts):
        for d, part in zip((1, -1), parts):
            lo, n = part_of(part, ROWS)
            src = wst.at[wrap(y, d), pl.ds(lo, n), :]
            w_net.send(name, src, win_ref(0, 0, part), y_dev(d))

    tx_y.first(OWN_A)
    for d in (1, -1):
        lo, n = part_of(side(d), ROWS)
        w_net.send("tr", wst.at[wrap(y, 2), pl.ds(lo, n), :], transit.at[(1 - d) // 2], y_dev(d))
    tx_y.first(OWN_B)
    for name, sends in (("wz_a", OWN_A), ("wz_b", OWN_B)):
        for o, part, d in sends:
            lo, n = part_of(part, ROWS)
            w_net.send(name, wst.at[y, pl.ds(lo, n), :], win_ref(0, 0, part), z_dev(d))
    win[pl.ds(al(s * ROWS, ROWS), ROWS), :] = wst[y]
    loaded("oa", "oc")
    o_first[1].first(OWN_A, OWN_B)
    o_second[0].first(OWN_A, OWN_B)

    tx_y.first_wait(OWN_A)
    tx_y.second(OWN_F)
    tx_x.first(SIDES_A)
    w_first("w_a", ("lo", "hi"))
    w_first("w_b", ("hi", "lo"))
    w_net.wait("tr")
    for d in (1, -1):
        w_net.send("trf", transit.at[(1 - d) // 2], win_ref(-d, 0, side(d)), y_dev(d))
    td_y.first(OWN_A, OWN_B)
    tx_y.first_wait(OWN_B)
    tx_x.first(SIDES_B)
    tx_x.give(SIDES0)
    loaded("taps", "cgain", "sink", "inner", "outer")
    taps[...] = taps_ref[...].astype(F32)
    gall[t] = jnp.broadcast_to(cgain_ref[...], (8, 256))
    w_net.wait("wz_a")
    w_z.second(OWN_F)
    tx_y.second_wait(OWN_F)
    tx_x.first_wait(SIDES_A)
    tx_x.second(SIDES_AF)
    tx_x.first(FAR)
    tx_x.give(FAR0)
    w_net.wait("w_a")
    w_z.first(SIDES_A)
    w_net.wait("w_b")
    w_z.first(SIDES_B)
    w_net.wait("trf")
    w_z.first(FAR)
    tx_x.first_wait(SIDES_B)
    tx_x.second(SIDES_BF)
    tx_x.give(SIDES1)
    w_net.wait("wz_b")
    td_y.first_wait(OWN_A)
    td_y.second(OWN_F)
    o_first[0].first(OWN_A, OWN_B)
    w_z.first_wait(SIDES_A)
    w_z.second(SIDES_AF)
    o_first[1].first_wait(OWN_A)
    o_first[1].second(OWN_F)
    w_z.first_wait(SIDES_B)
    w_z.second(SIDES_BF)
    tx_x.first_wait(FAR)
    tx_x.second(FAR_F)
    tx_x.give(FAR1)
    td_y.first_wait(OWN_B)
    td_p.give(SIDES0)
    o_first[1].first_wait(OWN_B)
    o_second[1].first(OWN_A, OWN_B, SIDES_A, SIDES_B)
    w_z.first_wait(FAR)
    w_z.second(FAR_F)
    o_second[0].first_wait(OWN_A)
    o_second[0].second(OWN_F)
    o_second[0].first_wait(OWN_B)
    tx_x.second_wait(SIDES_AF, SIDES_BF)
    tx_x.give(SIDES2)
    td_y.second_wait(OWN_F)
    td_p.give(FAR0)
    o_first[0].first_wait(OWN_A)
    o_first[0].second(OWN_F)
    o_second[0].first(SIDES_A)
    tx_x.second_wait(FAR_F)
    tx_x.give(FAR2)
    o_first[0].first_wait(OWN_B)
    o_second[0].first(SIDES_B)

    def project(o):
        rows = pl.ds(al(wrap(y, o) * ROWS, ROWS), ROWS)
        acc[rows, :] = jnp.dot(nrm[rows, :], win[...], preferred_element_type=F32)

    w_z.second_wait(OWN_F, SIDES_AF, SIDES_BF, FAR_F)
    project(0)
    tx_x.give_wait(SIDES0, SIDES1, SIDES2)
    td_p.give_wait(SIDES0)
    project(-1)
    project(1)
    tx_x.give_wait(FAR0, FAR1, FAR2)
    td_p.give_wait(FAR0)
    project(2)
    o_first[1].second_wait(OWN_F)
    o_second[1].first(FAR)
    o_second[1].first_wait(OWN_A)
    o_second[1].second(OWN_F)
    o_second[1].first_wait(OWN_B)
    o_first[0].second_wait(OWN_F)
    o_second[0].first(FAR)
    for i in range(1, 8):
        g_net.send("gain", gall.at[t], gall.at[t], (s, lax.rem(t + i, 8)))

    def halo_copy(i, src, dst):
        return pltpu.make_async_remote_copy(
            src_ref=src,
            dst_ref=dst,
            send_sem=halo_send.at[i],
            recv_sem=halo_recv.at[i],
            device_id=z_dev(1),
            device_id_type=MESH,
        )

    lane = lax.broadcasted_iota(jnp.int32, (ROWS, 128), 1)

    def attention():
        first = lax.rem(lane, 64) < 32
        low = lane < 64

        def rotate(v, cosine, sine):
            other = jnp.where(first, pltpu.roll(v, 96, 1), pltpu.roll(v, 32, 1))
            return v * cosine + other * sine

        def fill(b, carry):
            rows = pl.ds(al(b * ROWS, ROWS), ROWS)
            ext = pl.ds(al(b * ROWS + WINDOW, WINDOW), ROWS)
            edge = outer[b]
            co, so = edge[:, 0:128], edge[:, 128:256]
            cosine = co * inner[:, 0:128] - so * inner[:, 128:256]
            sine = so * inner[:, 0:128] + co * inner[:, 128:256]
            sine = jnp.where(first, -sine, sine)
            qbuf[rows, :] = rotate(acc[rows, 0:128], cosine, sine).astype(BF16)
            kv = rotate(
                acc[rows, 128:256], jnp.where(low, cosine, 1.0), jnp.where(low, sine, 0.0)
            )
            kv = kv.astype(BF16)
            kvext[ext, :] = kv
            kv = kv.astype(F32)
            swapped = pltpu.roll(kv, 64, 1)
            keys[ext, :] = jnp.where(low, kv, swapped).astype(BF16)
            vals[ext, :] = jnp.where(low, swapped, kv).astype(BF16)
            return carry

        fill(3, 0)
        halo = halo_copy(0, kvext.at[pl.ds(GROUP, WINDOW), :], kvext.at[pl.ds(0, WINDOW), :])
        halo.start()
        lax.fori_loop(0, 3, fill, 0)

        low_w = low[:WINDOW, :]
        zero = jnp.zeros((WINDOW, 128), BF16)
        second = lax.broadcasted_iota(jnp.int32, (2 * WINDOW, 1), 0) >= WINDOW
        sink_a = jnp.where(y == 0, sink_ref[0:1, 0:1], sink_ref[0:1, 2:3])
        sink_b = jnp.where(y == 0, sink_ref[0:1, 1:2], sink_ref[0:1, 3:4])
        sink = jnp.where(second, sink_b, sink_a)
        row_i = lax.rem(lax.broadcasted_iota(jnp.int32, (2 * WINDOW, 2 * WINDOW), 0), WINDOW)
        col_j = lax.broadcasted_iota(jnp.int32, (2 * WINDOW, 2 * WINDOW), 1)
        distance = row_i + WINDOW - col_j
        near = (distance >= 0) & (distance < WINDOW)

        def attend(b):
            at = al(b * WINDOW, WINDOW)
            q = qbuf[pl.ds(at, WINDOW), :]
            stacked = jnp.concatenate([jnp.where(low_w, q, zero), jnp.where(low_w, zero, q)], axis=0)
            scores = lax.dot_general(
                stacked,
                keys[pl.ds(at, 2 * WINDOW), :],
                (((1,), (1,)), ((), ())),
                preferred_element_type=F32,
            )
            key_pos = z * GROUP + (b - 1) * WINDOW + col_j
            scores = jnp.where(near & (key_pos >= 0), scores * 0.125, -1e30)
            top = jnp.maximum(jnp.max(scores, axis=1, keepdims=True), sink)
            e = jnp.exp(scores - top)
            denom = jnp.sum(e, axis=1, keepdims=True) + jnp.exp(sink - top)
            probs = (e / denom).astype(BF16)
            att = jnp.dot(probs, vals[pl.ds(at, 2 * WINDOW), :], preferred_element_type=F32)
            mx[pl.ds(at, WINDOW), :] = jnp.where(low_w, att[:WINDOW, :], att[WINDOW:, :]).astype(BF16)

        def attend_pair(i, carry):
            attend(2 * i + 2)
            attend(2 * i + 1)
            return carry

        lax.fori_loop(0, 3, attend_pair, 0)
        attend(7)
        halo.wait_recv()
        edge = kvext[0:WINDOW, :].astype(F32)
        swapped = pltpu.roll(edge, 64, 1)
        keys[0:WINDOW, :] = jnp.where(low_w, edge, swapped).astype(BF16)
        vals[0:WINDOW, :] = jnp.where(low_w, swapped, edge).astype(BF16)
        attend(0)
        halo.wait_send()

    def convolution():
        def gate_rows(b, carry):
            rows = pl.ds(al(b * ROWS, ROWS), ROWS)
            g = acc[rows, 0:128] * (1.0 / (1.0 + jnp.exp(-acc[rows, 128:256])))
            gext[pl.ds(al(b * ROWS + 32, 32), ROWS), :] = g.astype(BF16).astype(F32)
            return carry

        gate_rows(3, 0)
        gtail[...] = gext[GROUP : GROUP + 32, :].astype(BF16)
        halo = halo_copy(1, gtail, ghalo)
        halo.start()
        lax.fori_loop(0, 3, gate_rows, 0)

        def filter_rows(r):
            f = jnp.zeros((64, 128), F32)
            for k in range(KSIZE):
                f = f + taps[k : k + 1, :] * gext[r + 2 + k : r + 66 + k, :]
            mx[r : r + 64, :] = f.astype(BF16)

        for r in range(64, GROUP, 64):
            filter_rows(r)
        halo.wait_recv()
        gext[0:32, :] = jnp.where(z > 0, ghalo[...].astype(F32), 0.0)
        filter_rows(0)

        halo.wait_send()

    pl.when(y < 2)(attention)
    pl.when(y >= 2)(convolution)

    def mix_ref(o, off, part, mine=True):
        lo, n = part_of(part, ROWS)
        yy = wrap(y, o)
        cols = pl.ds(al(tp_at(off, mine) * 256 + lax.rem(yy, 2) * 128, 128), 128)
        return mixall.at[yy // 2, pl.ds(lo, n), cols]

    m_x = Ring(m_net, "mx", mix_ref, x_dev)
    own_cols = pl.ds(al(t * 256 + lax.rem(y, 2) * 128, 128), 128)
    mixall[y // 2, :, own_cols] = mx[pl.ds(al(y * ROWS, ROWS), ROWS), :]

    def m_rows(o, part):
        lo, n = part_of(part, ROWS)
        return mx.at[pl.ds(al(wrap(y, o) * ROWS + lo, 128), n), :]

    for d in (1, -1):
        m_net.send("tr", m_rows(2, side(d)), mtransit.at[(1 - d) // 2], y_dev(d))
    for name, parts in (("m_a", ("lo", "hi")), ("m_b", ("hi", "lo"))):
        for d, part in zip((1, -1), parts):
            m_net.send(name, m_rows(d, part), mix_ref(0, 0, part), y_dev(d))
    m_x.first(OWN_A, OWN_B)
    m_x.give(OWN0)
    m_net.wait("tr")
    for d in (1, -1):
        m_net.send("trf", mtransit.at[(1 - d) // 2], mix_ref(-d, 0, side(d)), y_dev(d))
    m_net.wait("m_a")
    m_x.first(SIDES_A)
    m_net.wait("m_b")
    m_x.first(SIDES_B)
    m_x.give(SIDES0)
    o_second[0].first_wait(SIDES_A)
    o_second[0].second(SIDES_AF)
    o_second[1].first_wait(SIDES_A)
    o_second[1].second(SIDES_AF)
    m_x.first_wait(OWN_A)
    m_x.second(OWN_F)
    m_x.first_wait(OWN_B)
    m_x.give(OWN1)
    m_net.wait("trf")
    m_x.first(FAR)
    m_x.give(FAR0)
    o_second[0].first_wait(SIDES_B)
    o_second[0].second(SIDES_BF)
    o_second[1].first_wait(SIDES_B)
    o_second[1].second(SIDES_BF)
    m_x.first_wait(SIDES_A)
    m_x.second(SIDES_AF)
    m_x.first_wait(SIDES_B)
    m_x.second(SIDES_BF)
    m_x.give(SIDES1)
    m_x.second_wait(OWN_F)
    m_x.give(OWN2)
    o_second[1].first_wait(FAR)
    o_second[1].second(FAR_F)
    m_x.first_wait(FAR)
    m_x.second(FAR_F)
    m_x.give(FAR1)
    o_second[0].first_wait(FAR)
    o_second[0].second(FAR_F)
    m_x.second_wait(SIDES_AF, SIDES_BF)
    m_x.give(SIDES2)
    g_net.wait("gain")
    for i in range(8):
        gfull[:, i * 256 : (i + 1) * 256] = gall[i, 0:1, :]
    m_x.second_wait(FAR_F)
    m_x.give(FAR2)
    m_x.give_wait(OWN0, OWN1, OWN2, SIDES0, SIDES1, SIDES2, FAR0, FAR1, FAR2)

    def channel_norm(i, carry):
        rows = pl.ds(al(i * 16, 16), 16)
        f = mixall[1, rows, :].astype(F32)
        mean_value = jnp.sum(f, axis=1, keepdims=True) * (1.0 / CONV)
        variance = jnp.sum(f * f, axis=1, keepdims=True) * (1.0 / CONV) - mean_value * mean_value
        scaled = (f - mean_value) * lax.rsqrt(variance + 1e-05) * gfull[...]
        convn[rows, :] = (scaled / (1.0 + jnp.exp(-scaled))).astype(BF16)
        return carry

    lax.fori_loop(0, ROWS // 16, channel_norm, 0)
    for ring in o_second:
        ring.second_wait(OWN_F, SIDES_AF, SIDES_BF, FAR_F)

    for c in range(0, OUTW, 256):
        w_attn = wo[:, 0:128, c : c + 256].reshape(2048, 256)
        w_conv = wo[:, 128:256, c : c + 256].reshape(2048, 256)
        v = jnp.dot(mixall[0], w_attn, preferred_element_type=F32)
        v = v + jnp.dot(convn[...], w_conv, preferred_element_type=F32)
        out_ref[:, c : c + 256] = v.astype(BF16)

    for net in (w_net, t_net, o_net, m_net, g_net):
        net.drain()


def per_device(
    tokens,
    norm_gain,
    w_query,
    w_key,
    w_value,
    w_glu,
    w_gate,
    sink_logit,
    conv_taps,
    conv_gain,
    out_attn,
    out_conv,
):
    hbm = pl.BlockSpec(memory_space=pltpu.HBM)
    vmem = pl.BlockSpec(memory_space=pltpu.VMEM)
    dma = pltpu.SemaphoreType.DMA
    inner, outer = rope_tables()
    tables = (jnp.asarray(inner), jnp.asarray(outer[:, None, :]))
    return pl.pallas_call(
        kernel,
        name="mixer_layer",
        out_shape=jax.ShapeDtypeStruct((ROWS, OUTW), BF16),
        in_specs=[hbm] * 14,
        out_specs=vmem,
        scratch_shapes=[
            pltpu.VMEM((4, ROWS, WIDTH), BF16),
            pltpu.VMEM((2, 128, WIDTH), BF16),
            pltpu.VMEM((D, WIDTH), BF16),
            pltpu.VMEM((16, ROWS, OUTW), BF16),
            pltpu.VMEM((ROWS, D), BF16),
            pltpu.VMEM((GROUP, D), BF16),
            pltpu.VMEM((GROUP, WIDTH), F32),
            pltpu.VMEM((GROUP, 128), BF16),
            pltpu.VMEM((GROUP + WINDOW, 128), BF16),
            pltpu.VMEM((GROUP + WINDOW, 128), BF16),
            pltpu.VMEM((GROUP + WINDOW, 128), BF16),
            pltpu.VMEM((32, 128), BF16),
            pltpu.VMEM((32, 128), BF16),
            pltpu.VMEM((GROUP + 32, 128), F32),
            pltpu.VMEM((128, ROWS), BF16),
            pltpu.VMEM((1, D), F32),
            pltpu.VMEM((1, 4), F32),
            pltpu.VMEM((KSIZE, 128), BF16),
            pltpu.VMEM((1, 256), F32),
            pltpu.VMEM((8, 8, 256), F32),
            pltpu.VMEM((1, 2048), F32),
            pltpu.VMEM((ROWS, 256), F32),
            pltpu.VMEM((4, 1, 256), F32),
            pltpu.VMEM((KSIZE, 128), F32),
            pltpu.VMEM((GROUP, 128), BF16),
            pltpu.VMEM((2, 128, 128), BF16),
            pltpu.VMEM((2, ROWS, 2048), BF16),
            pltpu.VMEM((ROWS, 2048), BF16),
            dma((17,)),
            dma((1,)),
            dma((SEMS,)),
            dma((1,)),
            dma((SEMS,)),
            dma((1,)),
            dma((SEMS,)),
            dma((1,)),
            dma((SEMS,)),
            dma((1,)),
            dma((1,)),
            dma((2,)),
            dma((2,)),
        ],
        compiler_params=pltpu.CompilerParams(
            collective_id=0, has_side_effects=True, vmem_limit_bytes=67043328
        ),
    )(
        tokens,
        norm_gain[None, :],
        w_query,
        w_key.T,
        w_value.T,
        w_glu,
        w_gate,
        sink_logit[None, :],
        conv_taps,
        conv_gain[None, :],
        out_attn,
        out_conv,
        *tables,
    )


def solution(mesh):
    return jax.shard_map(
        per_device,
        mesh=mesh,
        in_specs=(
            P("sp", None),
            P(),
            P("sp", "tp"),
            P("sp", "tp"),
            P("sp", "tp"),
            P("sp", "tp"),
            P("sp", "tp"),
            P("tp"),
            P(None, "tp"),
            P("tp"),
            P("sp", "tp"),
            P("sp", "tp"),
        ),
        out_specs=P("sp", "tp"),
        check_vma=False,
    )
```

```python
import jax
import jax.numpy as jnp
import numpy as np
from jax import lax
from jax.experimental import pallas as pl
from jax.experimental.pallas import tpu as pltpu
from jax.sharding import PartitionSpec as P

MESH = pl.DeviceIdType.MESH
F32 = jnp.float32
BF16 = jnp.bfloat16

ROWS = 256
GROUP = 1024
D = 4096
HEAD = 64
CONV = 2048
KSIZE = 31
WINDOW = 128
WIDTH = 256
OUTW = 512
XCOLS = 384
DCOLS = 512
OUT_SPLIT = 160
SEMS = 26


def rope_tables():
    freq = (10000.0 ** (-np.arange(32, dtype=np.float64) * 2.0 / HEAD)).astype(np.float32)
    lanes = np.tile(freq.astype(np.float64), 4)[None, :]
    inner = np.arange(ROWS, dtype=np.float64)[:, None] * lanes
    outer = np.arange(16, dtype=np.float64)[:, None] * ROWS * lanes
    return tuple(
        np.concatenate([np.cos(a), np.sin(a)], axis=1).astype(np.float32) for a in (inner, outer)
    )


class Net:
    def __init__(self, send_sem, recv_sem, meter, partner):
        self.send_sem, self.recv_sem, self.meter, self.partner = send_sem, recv_sem, meter, partner
        self.index, self.size, self.total = {}, {}, 0

    def send(self, group, src, dst, device):
        k = self.index.setdefault(group, len(self.index))
        assert k < SEMS
        count = src.dtype.itemsize
        for n in src.shape:
            count *= n
        self.size[group] = self.size.get(group, 0) + count
        self.total += count
        pltpu.make_async_remote_copy(
            src_ref=src,
            dst_ref=dst,
            send_sem=self.send_sem.at[0],
            recv_sem=self.recv_sem.at[k],
            device_id=device,
            device_id_type=MESH,
        ).start()

    def await_bytes(self, sem, count):
        tiles = count // 2048
        across = max(n for n in range(1, 33) if tiles % n == 0)
        down = tiles // across
        assert tiles * 2048 == count and down <= 128
        counted = self.meter.at[0 : down * 8, 0 : across * 128]
        pltpu.make_async_copy(counted, counted, sem).wait()

    def wait(self, group):
        self.await_bytes(self.recv_sem.at[self.index[group]], self.size[group])

    def drain(self):
        self.await_bytes(self.send_sem.at[0], self.total)


def side(d):
    return "lo" if d == 1 else "hi"


class Ring:
    def __init__(self, net, name, ref, device):
        self.net, self.name, self.ref, self.device = net, name, ref, device

    def first(self, *groups):
        for sends in groups:
            for o, part, d in sends:
                r = self.ref(o, 0, part)
                self.net.send((self.name, "T", sends), r, r, self.device(d))

    def first_wait(self, *groups):
        for sends in groups:
            self.net.wait((self.name, "T", sends))

    def second(self, *groups):
        for sends in groups:
            for o, d in sends:
                r = self.ref(o, -d, side(d))
                self.net.send((self.name, "F", sends), r, r, self.device(d))

    def second_wait(self, *groups):
        for sends in groups:
            self.net.wait((self.name, "F", sends))

    def give(self, *groups):
        for items in groups:
            for o, off in items:
                r = self.ref(o, off, "full")
                self.net.send((self.name, "P", items), r, r, self.net.partner)

    def give_wait(self, *groups):
        for items in groups:
            self.net.wait((self.name, "P", items))


def both(*items):
    return tuple((o, part, d) for o, part in items for d in (1, -1))


OWN_A = ((0, "lo", 1), (0, "hi", -1))
OWN_B = ((0, "hi", 1), (0, "lo", -1))
SIDES_A = both((-1, "lo"), (1, "hi"))
SIDES_B = both((-1, "hi"), (1, "lo"))
FAR = both((2, "lo"), (2, "hi"))
OWN_F = ((0, 1), (0, -1))
SIDES_AF = ((-1, 1), (1, -1))
SIDES_BF = ((-1, -1), (1, 1))
FAR_F = ((2, 1), (2, -1))
OWN0, OWN1, OWN2 = ((0, 0),), ((0, 1), (0, -1)), ((0, 2),)
SIDES0, SIDES1, SIDES2 = ((-1, 0), (1, 0)), ((-1, 1), (-1, -1), (1, 1), (1, -1)), ((-1, 2), (1, 2))
FAR0, FAR1, FAR2 = ((2, 0),), ((2, 1), (2, -1)), ((2, 2),)


def kernel(
    tokens_hbm,
    gain_hbm,
    wq_hbm,
    wk_hbm,
    wv_hbm,
    wglu_hbm,
    wgate_hbm,
    sink_hbm,
    taps_hbm,
    cgain_hbm,
    oa_hbm,
    oc_hbm,
    inner_hbm,
    outer_hbm,
    out_ref,
    wst,
    transit,
    win,
    wo,
    tok,
    nrmx,
    nrmd,
    meter,
    acc,
    qbuf,
    kvext,
    keys,
    vals,
    gtail,
    ghalo,
    gext,
    kvt,
    gain_ref,
    sink_ref,
    taps_ref,
    cgain_ref,
    gall,
    gfull,
    inner,
    outer,
    taps,
    mx,
    mixall,
    convn,
    local_sem,
    w_send,
    w_recv,
    t_send,
    t_recv,
    o_send,
    o_recv,
    m_send,
    m_recv,
    g_send,
    g_recv,
    halo_send,
    halo_recv,
):
    s = lax.axis_index("sp")
    t = lax.axis_index("tp")
    z, y = s // 4, lax.rem(s, 4)
    x, core = t // 2, lax.rem(t, 2)

    def al(v, m):
        return pl.multiple_of(v, m)

    def wrap(v, o):
        return lax.rem(v + (o + 4), 4)

    def sp_at(dz, dy):
        return wrap(z, dz) * 4 + wrap(y, dy)

    def tp_at(dx, mine=True):
        return wrap(x, dx) * 2 + (core if mine else 1 - core)

    partner = (s, tp_at(0, False))
    barrier = pltpu.get_barrier_semaphore()
    peers = [(sp_at(dz, dy), t) for dz, dy in ((0, 1), (0, -1), (1, 0), (-1, 0))]
    peers += [(s, tp_at(1)), (s, tp_at(-1)), partner]
    for peer in peers:
        pl.semaphore_signal(barrier, inc=1, device_id=peer, device_id_type=MESH)

    role_half = pl.ds(al(lax.rem(y, 2) * 128, 128), 128)
    loads = {}
    for name, src, dst in (
        ("tok", tokens_hbm, tok),
        ("gain", gain_hbm, gain_ref),
        ("wk", wk_hbm, kvt.at[0:64, :]),
        ("wv", wv_hbm, kvt.at[64:128, :]),
        ("q0", wq_hbm.at[:, 0:128], wst.at[2, :, 0:128]),
        ("q1", wq_hbm.at[:, 128:256], wst.at[3, :, 0:128]),
        ("glu0", wglu_hbm.at[:, 0:128], wst.at[0, :, 0:128]),
        ("glu1", wglu_hbm.at[:, 128:256], wst.at[1, :, 0:128]),
        ("gate0", wgate_hbm.at[:, 0:128], wst.at[0, :, 128:256]),
        ("gate1", wgate_hbm.at[:, 128:256], wst.at[1, :, 128:256]),
        ("oa", oa_hbm, wo.at[s, 0:128, :]),
        ("oc", oc_hbm, wo.at[s, 128:256, :]),
        ("taps", taps_hbm.at[:, role_half], taps_ref),
        ("cgain", cgain_hbm, cgain_ref),
        ("sink", sink_hbm, sink_ref),
        ("inner", inner_hbm, inner),
        ("outer", outer_hbm.at[pl.ds(z * 4, 4)], outer),
    ):
        copy = pltpu.make_async_copy(src, dst, local_sem.at[len(loads)])
        copy.start()
        loads[name] = copy

    def loaded(*names):
        for name in names:
            loads[name].wait()

    loaded("wk", "wv")
    kv_t = kvt[...].astype(F32).T.astype(BF16)
    wst[2, :, 128:256] = kv_t
    wst[3, :, 128:256] = kv_t
    loaded("tok", "gain")

    def norm_rows(i, carry):
        v = tok[pl.ds(al(i * 16, 16), 16), :].astype(F32)
        scale = lax.rsqrt(jnp.mean(v * v, axis=1, keepdims=True) + 1e-06)
        v = (v * scale * gain_ref[...]).astype(BF16)
        rows = pl.ds(al(y * ROWS + i * 16, 16), 16)
        for c in range(8):
            nrmx[c, rows, :] = v[:, c * XCOLS : (c + 1) * XCOLS]
        for c in range(2):
            nrmd[c, rows, :] = v[:, 8 * XCOLS + c * DCOLS : 8 * XCOLS + (c + 1) * DCOLS]
        return carry

    lax.fori_loop(0, ROWS // 16, norm_rows, 0)
    loaded("q0", "q1", "glu0", "glu1", "gate0", "gate1")
    pl.semaphore_wait(barrier, len(peers))

    w_net = Net(w_send, w_recv, meter, partner)
    t_net = Net(t_send, t_recv, meter, partner)
    o_net = Net(o_send, o_recv, meter, partner)
    m_net = Net(m_send, m_recv, meter, partner)
    g_net = Net(g_send, g_recv, meter, partner)

    def y_dev(d):
        return (sp_at(0, d), t)

    def z_dev(d):
        return (sp_at(d, 0), t)

    def x_dev(d):
        return (s, tp_at(d))

    def part_of(part, n):
        return {"full": (0, n), "lo": (0, n // 2), "hi": (n // 2, n // 2)}[part]

    def win_ref(o, off, part, mine=True):
        lo, n = part_of(part, ROWS)
        return win.at[pl.ds(al(sp_at(off, o) * ROWS + lo, 128), n), :]

    def tok_rows(o, part):
        lo, n = part_of(part, ROWS)
        return pl.ds(al(wrap(y, o) * ROWS + lo, 128), n)

    def tokx_ref(o, off, part, mine=True):
        return nrmx.at[tp_at(off, mine), tok_rows(o, part), :]

    def tokd_ref(o, off, part, mine=True):
        return nrmd.at[core if mine else 1 - core, tok_rows(o, part), :]

    def along_y(ref):
        return lambda o, off, part, mine=True: ref(off, 0, part, mine)

    tx_y = Ring(t_net, "txy", along_y(tokx_ref), y_dev)
    td_y = Ring(t_net, "tdy", along_y(tokd_ref), y_dev)
    tx_x = Ring(t_net, "txx", tokx_ref, x_dev)
    td_p = Ring(t_net, "tdp", tokd_ref, x_dev)
    w_z = Ring(w_net, "wz", win_ref, z_dev)

    def out_ref_of(h):
        base, size = ((0, OUT_SPLIT), (OUT_SPLIT, ROWS - OUT_SPLIT))[h]

        def first(o, off, part, mine=True):
            lo, n = part_of(part, size)
            src = sp_at(0, off) if h == 0 else sp_at(off, 0)
            return wo.at[src, pl.ds(base + lo, n), :]

        def second(o, off, part, mine=True):
            lo, n = part_of(part, size)
            src = sp_at(off, o) if h == 0 else sp_at(o, off)
            return wo.at[src, pl.ds(base + lo, n), :]

        return first, second

    o_first, o_second = [], []
    for h in (0, 1):
        f, g = out_ref_of(h)
        o_first.append(Ring(o_net, ("of", h), f, (y_dev, z_dev)[h]))
        o_second.append(Ring(o_net, ("os", h), g, (z_dev, y_dev)[h]))

    def w_first(name, parts):
        for d, part in zip((1, -1), parts):
            lo, n = part_of(part, ROWS)
            src = wst.at[wrap(y, d), pl.ds(lo, n), :]
            w_net.send(name, src, win_ref(0, 0, part), y_dev(d))

    tx_y.first(OWN_A)
    for d in (1, -1):
        lo, n = part_of(side(d), ROWS)
        w_net.send("tr", wst.at[wrap(y, 2), pl.ds(lo, n), :], transit.at[(1 - d) // 2], y_dev(d))
    tx_y.first(OWN_B)
    for name, sends in (("wz_a", OWN_A), ("wz_b", OWN_B)):
        for o, part, d in sends:
            lo, n = part_of(part, ROWS)
            w_net.send(name, wst.at[y, pl.ds(lo, n), :], win_ref(0, 0, part), z_dev(d))
    win[pl.ds(al(s * ROWS, ROWS), ROWS), :] = wst[y]
    loaded("oa", "oc")
    o_first[1].first(OWN_A, OWN_B)
    o_second[0].first(OWN_A, OWN_B)

    tx_y.first_wait(OWN_A)
    tx_y.second(OWN_F)
    tx_x.first(SIDES_A)
    w_first("w_a", ("lo", "hi"))
    w_first("w_b", ("hi", "lo"))
    w_net.wait("tr")
    for d in (1, -1):
        w_net.send("trf", transit.at[(1 - d) // 2], win_ref(-d, 0, side(d)), y_dev(d))
    td_y.first(OWN_A, OWN_B)
    tx_y.first_wait(OWN_B)
    tx_x.first(SIDES_B)
    tx_x.give(SIDES0)
    loaded("taps", "cgain", "sink", "inner", "outer")
    taps[...] = taps_ref[...].astype(F32)
    gall[t] = jnp.broadcast_to(cgain_ref[...], (8, 256))
    w_net.wait("wz_a")
    w_z.second(OWN_F)
    tx_y.second_wait(OWN_F)
    tx_x.first_wait(SIDES_A)
    tx_x.second(SIDES_AF)
    tx_x.first(FAR)
    tx_x.give(FAR0)
    w_net.wait("w_a")
    w_z.first(SIDES_A)
    w_net.wait("w_b")
    w_z.first(SIDES_B)
    w_net.wait("trf")
    w_z.first(FAR)
    tx_x.first_wait(SIDES_B)
    tx_x.second(SIDES_BF)
    tx_x.give(SIDES1)
    w_net.wait("wz_b")
    td_y.first_wait(OWN_A)
    td_y.second(OWN_F)
    o_first[0].first(OWN_A, OWN_B)
    w_z.first_wait(SIDES_A)
    w_z.second(SIDES_AF)
    o_first[1].first_wait(OWN_A)
    o_first[1].second(OWN_F)
    w_z.first_wait(SIDES_B)
    w_z.second(SIDES_BF)
    tx_x.first_wait(FAR)
    tx_x.second(FAR_F)
    tx_x.give(FAR1)
    td_y.first_wait(OWN_B)
    td_p.give(SIDES0)
    o_first[1].first_wait(OWN_B)
    o_second[1].first(OWN_A, OWN_B, SIDES_A, SIDES_B)
    w_z.first_wait(FAR)
    w_z.second(FAR_F)
    o_second[0].first_wait(OWN_A)
    o_second[0].second(OWN_F)
    o_second[0].first_wait(OWN_B)
    tx_x.second_wait(SIDES_AF, SIDES_BF)
    tx_x.give(SIDES2)
    td_y.second_wait(OWN_F)
    td_p.give(FAR0)
    o_first[0].first_wait(OWN_A)
    o_first[0].second(OWN_F)
    o_second[0].first(SIDES_A)

    def project(o):
        rows = pl.ds(al(wrap(y, o) * ROWS, ROWS), ROWS)
        parts = [nrmx[c, rows, :] for c in range(8)] + [nrmd[c, rows, :] for c in range(2)]
        whole = jnp.concatenate(parts, axis=1)
        acc[rows, :] = jnp.dot(whole, win[...], preferred_element_type=F32)

    def halo_copy(src, dst):
        return pltpu.make_async_remote_copy(
            src_ref=src,
            dst_ref=dst,
            send_sem=halo_send.at[0],
            recv_sem=halo_recv.at[0],
            device_id=z_dev(1),
            device_id_type=MESH,
        )

    lane = lax.broadcasted_iota(jnp.int32, (ROWS, 128), 1)
    first = lax.rem(lane, 64) < 32
    low = lane < 64
    low_w = low[:WINDOW, :]
    kv_halo = halo_copy(kvext.at[pl.ds(GROUP, WINDOW), :], kvext.at[pl.ds(0, WINDOW), :])
    gate_halo = halo_copy(gtail, ghalo)

    def rotate(v, cosine, sine):
        other = jnp.where(first, pltpu.roll(v, 96, 1), pltpu.roll(v, 32, 1))
        return v * cosine + other * sine

    def fill(b):
        rows = slice(b * ROWS, (b + 1) * ROWS)
        ext = slice(b * ROWS + WINDOW, (b + 1) * ROWS + WINDOW)
        edge = outer[b]
        co, so = edge[:, 0:128], edge[:, 128:256]
        cosine = co * inner[:, 0:128] - so * inner[:, 128:256]
        sine = so * inner[:, 0:128] + co * inner[:, 128:256]
        sine = jnp.where(first, -sine, sine)
        q = rotate(acc[rows, 0:128], cosine, sine).astype(BF16).astype(F32)
        qbuf[rows, :] = (q * 0.125).astype(BF16)
        kv = rotate(acc[rows, 128:256], jnp.where(low, cosine, 1.0), jnp.where(low, sine, 0.0))
        kv = kv.astype(BF16)
        kvext[ext, :] = kv
        kv = kv.astype(F32)
        swapped = pltpu.roll(kv, 64, 1)
        keys[ext, :] = jnp.where(low, kv, swapped).astype(BF16)
        vals[ext, :] = jnp.where(low, swapped, kv).astype(BF16)

    def attend(role, b):
        zero = jnp.zeros((WINDOW, 128), BF16)
        second = lax.broadcasted_iota(jnp.int32, (2 * WINDOW, 1), 0) >= WINDOW
        i = 2 * (role - 2)
        sink = jnp.where(second, sink_ref[0:1, i + 1 : i + 2], sink_ref[0:1, i : i + 1])
        row_i = lax.rem(lax.broadcasted_iota(jnp.int32, (2 * WINDOW, 2 * WINDOW), 0), WINDOW)
        col_j = lax.broadcasted_iota(jnp.int32, (2 * WINDOW, 2 * WINDOW), 1)
        distance = row_i + WINDOW - col_j
        near = (distance >= 0) & (distance < WINDOW)
        if b == 0:
            near = near & (z * GROUP - WINDOW + col_j >= 0)
        q = qbuf[b * WINDOW : (b + 1) * WINDOW, :]
        stacked = jnp.concatenate([jnp.where(low_w, q, zero), jnp.where(low_w, zero, q)], axis=0)
        scores = lax.dot_general(
            stacked,
            keys[b * WINDOW : (b + 2) * WINDOW, :],
            (((1,), (1,)), ((), ())),
            preferred_element_type=F32,
        )
        scores = jnp.where(near, scores, -1e30)
        top = jnp.maximum(jnp.max(scores, axis=1, keepdims=True), sink)
        e = jnp.exp(scores - top)
        denom = jnp.sum(e, axis=1, keepdims=True) + jnp.exp(sink - top)
        probs = (e * (1.0 / denom)).astype(BF16)
        att = jnp.dot(probs, vals[b * WINDOW : (b + 2) * WINDOW, :], preferred_element_type=F32)
        mx[b * WINDOW : (b + 1) * WINDOW, :] = jnp.where(
            low_w, att[:WINDOW, :], att[WINDOW:, :]
        ).astype(BF16)

    def late_windows(far):
        return [(2 * far + i) % 8 for i in range(3)]

    def attend_first(role):
        kv_halo.wait_recv()
        edge = kvext[0:WINDOW, :].astype(F32)
        swapped = pltpu.roll(edge, 64, 1)
        keys[0:WINDOW, :] = jnp.where(low_w, edge, swapped).astype(BF16)
        vals[0:WINDOW, :] = jnp.where(low_w, swapped, edge).astype(BF16)
        attend(role, 0)
        kv_halo.wait_send()

    def attend_early(role):
        far = (role + 2) % 4
        fill(3)
        kv_halo.start()
        for b in range(3):
            if b != far:
                fill(b)
        for b in range(7, 0, -1):
            if b not in late_windows(far):
                attend(role, b)
        if 0 not in late_windows(far):
            attend_first(role)

    def attend_late(role):
        far = (role + 2) % 4
        fill(far)
        for b in range(7, 0, -1):
            if b in late_windows(far):
                attend(role, b)
        if 0 in late_windows(far):
            attend_first(role)

    def gate_rows(b):
        rows = slice(b * ROWS, (b + 1) * ROWS)
        g = acc[rows, 0:128] * (0.5 + 0.5 * jnp.tanh(0.5 * acc[rows, 128:256]))
        gext[b * ROWS + 32 : (b + 1) * ROWS + 32, :] = g.astype(BF16).astype(F32)

    def send_tail():
        gtail[...] = gext[GROUP : GROUP + 32, :].astype(BF16)
        gate_halo.start()

    def filter_rows(r):
        f = jnp.zeros((64, 128), F32)
        for k in range(KSIZE):
            f = f + taps[k : k + 1, :] * gext[r + 2 + k : r + 66 + k, :]
        mx[r : r + 64, :] = f.astype(BF16)

    def late_rows(far):
        return [(far * ROWS + i * 64) % GROUP for i in range(5)]

    def filter_first():
        gate_halo.wait_recv()
        gext[0:32, :] = jnp.where(z > 0, ghalo[...].astype(F32), 0.0)
        filter_rows(0)
        gate_halo.wait_send()

    def filter_early(role):
        far = (role + 2) % 4
        for b in (3, 0, 1, 2):
            if b != far:
                gate_rows(b)
                if b == 3:
                    send_tail()
        for r in range(64, GROUP, 64):
            if r not in late_rows(far):
                filter_rows(r)
        if 0 not in late_rows(far):
            filter_first()

    def filter_late(role):
        far = (role + 2) % 4
        gate_rows(far)
        if far == 3:
            send_tail()
        for r in range(64, GROUP, 64):
            if r in late_rows(far):
                filter_rows(r)
        if 0 in late_rows(far):
            filter_first()

    def by_role(conv, attention):
        for role in range(4):
            pl.when(y == role)(lambda role=role: (conv if role < 2 else attention)(role))

    def mix_ref(o, off, part, mine=True):
        lo, n = part_of(part, ROWS)
        yy = wrap(y, o)
        cols = pl.ds(al(tp_at(off, mine) * 256 + lax.rem(yy, 2) * 128, 128), 128)
        return mixall.at[yy // 2, pl.ds(lo, n), cols]

    m_x = Ring(m_net, "mx", mix_ref, x_dev)
    own_cols = pl.ds(al(t * 256 + lax.rem(y, 2) * 128, 128), 128)

    def m_send(name, o, part):
        lo, n = part_of(part, ROWS)
        src = mx.at[pl.ds(al(wrap(y, o) * ROWS + lo, 128), n), :]
        m_net.send(name, src, mix_ref(0, 0, part), y_dev(o))

    w_z.second_wait(OWN_F, SIDES_AF, SIDES_BF, FAR_F)
    project(0)
    tx_x.give_wait(SIDES0, SIDES1, SIDES2)
    td_p.give_wait(SIDES0)
    project(-1)
    project(1)
    tx_x.second_wait(FAR_F)
    tx_x.give(FAR2)
    o_first[0].first_wait(OWN_B)
    o_second[0].first(SIDES_B)
    by_role(filter_early, attend_early)
    m_send("m_a", 1, "lo")
    m_send("m_a", -1, "hi")
    tx_x.give_wait(FAR0, FAR1, FAR2)
    td_p.give_wait(FAR0)
    project(2)
    mixall[y // 2, :, own_cols] = mx[pl.ds(al(y * ROWS, ROWS), ROWS), :]
    m_x.first(OWN_A, OWN_B)
    m_x.give(OWN0)
    o_first[1].second_wait(OWN_F)
    o_second[1].first(FAR)
    o_second[1].first_wait(OWN_A)
    o_second[1].second(OWN_F)
    o_second[1].first_wait(OWN_B)
    o_first[0].second_wait(OWN_F)
    o_second[0].first(FAR)
    for i in range(1, 8):
        g_net.send("gain", gall.at[t], gall.at[t], (s, lax.rem(t + i, 8)))
    by_role(filter_late, attend_late)
    m_send("m_far", 2, "full")
    m_send("m_b", -1, "lo")
    m_send("m_b", 1, "hi")
    m_net.wait("m_a")
    m_x.first(SIDES_A)
    m_x.first_wait(OWN_A)
    m_x.second(OWN_F)
    m_x.first_wait(OWN_B)
    m_x.give(OWN1)
    o_second[0].first_wait(SIDES_A)
    o_second[0].second(SIDES_AF)
    o_second[1].first_wait(SIDES_A)
    o_second[1].second(SIDES_AF)
    o_second[0].first_wait(SIDES_B)
    o_second[0].second(SIDES_BF)
    o_second[1].first_wait(SIDES_B)
    o_second[1].second(SIDES_BF)
    m_net.wait("m_b")
    m_x.first(SIDES_B)
    m_x.give(SIDES0)
    m_net.wait("m_far")
    m_net.send("m_far_x", mix_ref(2, 0, "full"), mix_ref(2, 0, "full"), x_dev(2))
    m_x.first(FAR)
    m_x.give(FAR0)
    m_x.second_wait(OWN_F)
    m_x.give(OWN2)
    m_x.first_wait(SIDES_A)
    m_x.second(SIDES_AF)
    o_second[1].first_wait(FAR)
    o_second[1].second(FAR_F)
    m_x.first_wait(SIDES_B)
    m_x.second(SIDES_BF)
    m_x.give(SIDES1)
    o_second[0].first_wait(FAR)
    o_second[0].second(FAR_F)
    m_x.first_wait(FAR)
    m_x.give(FAR1)
    m_net.wait("m_far_x")
    m_x.give(FAR2)
    g_net.wait("gain")
    for i in range(8):
        gfull[:, i * 256 : (i + 1) * 256] = gall[i, 0:1, :]
    m_x.second_wait(SIDES_AF, SIDES_BF)
    m_x.give(SIDES2)
    m_x.give_wait(OWN0, OWN1, OWN2, SIDES0, SIDES1, SIDES2, FAR0, FAR1, FAR2)

    def channel_norm(i, carry):
        rows = pl.ds(al(i * 32, 32), 32)
        f = mixall[0, rows, :].astype(F32)
        mean_value = jnp.sum(f, axis=1, keepdims=True) * (1.0 / CONV)
        variance = jnp.sum(f * f, axis=1, keepdims=True) * (1.0 / CONV) - mean_value * mean_value
        scaled = (f - mean_value) * lax.rsqrt(variance + 1e-05) * gfull[...]
        convn[rows, :] = (scaled * (0.5 + 0.5 * jnp.tanh(0.5 * scaled))).astype(BF16)
        return carry

    lax.fori_loop(0, ROWS // 32, channel_norm, 0)
    for ring in o_second:
        ring.second_wait(OWN_F, SIDES_AF, SIDES_BF, FAR_F)

    for c in range(0, OUTW, 256):
        w_attn = wo[:, 0:128, c : c + 256].reshape(2048, 256)
        w_conv = wo[:, 128:256, c : c + 256].reshape(2048, 256)
        v = jnp.dot(mixall[1], w_attn, preferred_element_type=F32)
        v = v + jnp.dot(convn[...], w_conv, preferred_element_type=F32)
        out_ref[:, c : c + 256] = v.astype(BF16)

    for net in (w_net, t_net, o_net, m_net, g_net):
        net.drain()


def per_device(
    tokens,
    norm_gain,
    w_query,
    w_key,
    w_value,
    w_glu,
    w_gate,
    sink_logit,
    conv_taps,
    conv_gain,
    out_attn,
    out_conv,
):
    hbm = pl.BlockSpec(memory_space=pltpu.HBM)
    vmem = pl.BlockSpec(memory_space=pltpu.VMEM)
    dma = pltpu.SemaphoreType.DMA
    inner, outer = rope_tables()
    tables = (jnp.asarray(inner), jnp.asarray(outer[:, None, :]))
    return pl.pallas_call(
        kernel,
        name="mixer_layer",
        out_shape=jax.ShapeDtypeStruct((ROWS, OUTW), BF16),
        in_specs=[hbm] * 14,
        out_specs=vmem,
        scratch_shapes=[
            pltpu.VMEM((4, ROWS, WIDTH), BF16),
            pltpu.VMEM((2, 128, WIDTH), BF16),
            pltpu.VMEM((D, WIDTH), BF16),
            pltpu.VMEM((16, ROWS, OUTW), BF16),
            pltpu.VMEM((ROWS, D), BF16),
            pltpu.VMEM((8, GROUP, XCOLS), BF16),
            pltpu.VMEM((2, GROUP, DCOLS), BF16),
            pltpu.VMEM((GROUP, D), BF16),
            pltpu.VMEM((GROUP, WIDTH), F32),
            pltpu.VMEM((GROUP, 128), BF16),
            pltpu.VMEM((GROUP + WINDOW, 128), BF16),
            pltpu.VMEM((GROUP + WINDOW, 128), BF16),
            pltpu.VMEM((GROUP + WINDOW, 128), BF16),
            pltpu.VMEM((32, 128), BF16),
            pltpu.VMEM((32, 128), BF16),
            pltpu.VMEM((GROUP + 32, 128), F32),
            pltpu.VMEM((128, ROWS), BF16),
            pltpu.VMEM((1, D), F32),
            pltpu.VMEM((1, 4), F32),
            pltpu.VMEM((KSIZE, 128), BF16),
            pltpu.VMEM((1, 256), F32),
            pltpu.VMEM((8, 8, 256), F32),
            pltpu.VMEM((1, 2048), F32),
            pltpu.VMEM((ROWS, 256), F32),
            pltpu.VMEM((4, 1, 256), F32),
            pltpu.VMEM((KSIZE, 128), F32),
            pltpu.VMEM((GROUP, 128), BF16),
            pltpu.VMEM((2, ROWS, 2048), BF16),
            pltpu.VMEM((ROWS, 2048), BF16),
            dma((17,)),
            dma((1,)),
            dma((SEMS,)),
            dma((1,)),
            dma((SEMS,)),
            dma((1,)),
            dma((SEMS,)),
            dma((1,)),
            dma((SEMS,)),
            dma((1,)),
            dma((1,)),
            dma((1,)),
            dma((1,)),
        ],
        compiler_params=pltpu.CompilerParams(
            collective_id=0, has_side_effects=True, vmem_limit_bytes=67043328
        ),
    )(
        tokens,
        norm_gain[None, :],
        w_query,
        w_key.T,
        w_value.T,
        w_glu,
        w_gate,
        sink_logit[None, :],
        conv_taps,
        conv_gain[None, :],
        out_attn,
        out_conv,
        *tables,
    )


def solution(mesh):
    return jax.shard_map(
        per_device,
        mesh=mesh,
        in_specs=(
            P("sp", None),
            P(),
            P("sp", "tp"),
            P("sp", "tp"),
            P("sp", "tp"),
            P("sp", "tp"),
            P("sp", "tp"),
            P("tp"),
            P(None, "tp"),
            P("tp"),
            P("sp", "tp"),
            P("sp", "tp"),
        ),
        out_specs=P("sp", "tp"),
        check_vma=False,
    )
```

```python
import jax
import jax.numpy as jnp
import numpy as np
from jax import lax
from jax.experimental import pallas as pl
from jax.experimental.pallas import tpu as pltpu
from jax.sharding import PartitionSpec as P

MESH = pl.DeviceIdType.MESH
F32 = jnp.float32
BF16 = jnp.bfloat16

ROWS = 256
GROUP = 1024
D = 4096
HEAD = 64
CONV = 2048
KSIZE = 31
WINDOW = 128
WIDTH = 256
OUTW = 512
XCOLS = 384
DCOLS = 512
OUT_SPLIT = 160
SEMS = 26


def rope_tables():
    freq = (10000.0 ** (-np.arange(32, dtype=np.float64) * 2.0 / HEAD)).astype(np.float32)
    lanes = np.tile(freq.astype(np.float64), 4)[None, :]
    inner = np.arange(ROWS, dtype=np.float64)[:, None] * lanes
    outer = np.arange(16, dtype=np.float64)[:, None] * ROWS * lanes
    return tuple(
        np.concatenate([np.cos(a), np.sin(a)], axis=1).astype(np.float32) for a in (inner, outer)
    )


class Net:
    def __init__(self, send_sem, recv_sem, meter, partner):
        self.send_sem, self.recv_sem, self.meter, self.partner = send_sem, recv_sem, meter, partner
        self.index, self.size, self.total = {}, {}, 0

    def send(self, group, src, dst, device):
        k = self.index.setdefault(group, len(self.index))
        assert k < SEMS
        count = src.dtype.itemsize
        for n in src.shape:
            count *= n
        self.size[group] = self.size.get(group, 0) + count
        self.total += count
        pltpu.make_async_remote_copy(
            src_ref=src,
            dst_ref=dst,
            send_sem=self.send_sem.at[0],
            recv_sem=self.recv_sem.at[k],
            device_id=device,
            device_id_type=MESH,
        ).start()

    def await_bytes(self, sem, count):
        tiles = count // 2048
        across = max(n for n in range(1, 33) if tiles % n == 0)
        down = tiles // across
        assert tiles * 2048 == count and down <= 128
        counted = self.meter.at[0 : down * 8, 0 : across * 128]
        pltpu.make_async_copy(counted, counted, sem).wait()

    def wait(self, group):
        self.await_bytes(self.recv_sem.at[self.index[group]], self.size[group])

    def drain(self):
        self.await_bytes(self.send_sem.at[0], self.total)


def side(d):
    return "lo" if d == 1 else "hi"


class Ring:
    def __init__(self, net, name, ref, device):
        self.net, self.name, self.ref, self.device = net, name, ref, device

    def first(self, *groups):
        for sends in groups:
            for o, part, d in sends:
                r = self.ref(o, 0, part)
                self.net.send((self.name, "T", sends), r, r, self.device(d))

    def first_wait(self, *groups):
        for sends in groups:
            self.net.wait((self.name, "T", sends))

    def second(self, *groups):
        for sends in groups:
            for o, d in sends:
                r = self.ref(o, -d, side(d))
                self.net.send((self.name, "F", sends), r, r, self.device(d))

    def second_wait(self, *groups):
        for sends in groups:
            self.net.wait((self.name, "F", sends))

    def give(self, *groups):
        for items in groups:
            for o, off in items:
                r = self.ref(o, off, "full")
                self.net.send((self.name, "P", items), r, r, self.net.partner)

    def give_wait(self, *groups):
        for items in groups:
            self.net.wait((self.name, "P", items))


def both(*items):
    return tuple((o, part, d) for o, part in items for d in (1, -1))


OWN_A = ((0, "lo", 1), (0, "hi", -1))
OWN_B = ((0, "hi", 1), (0, "lo", -1))
SIDES_A = both((-1, "lo"), (1, "hi"))
SIDES_B = both((-1, "hi"), (1, "lo"))
FAR = both((2, "lo"), (2, "hi"))
OWN_F = ((0, 1), (0, -1))
SIDES_AF = ((-1, 1), (1, -1))
SIDES_BF = ((-1, -1), (1, 1))
FAR_F = ((2, 1), (2, -1))
OWN0, OWN1, OWN2 = ((0, 0),), ((0, 1), (0, -1)), ((0, 2),)
SIDES0, SIDES1, SIDES2 = ((-1, 0), (1, 0)), ((-1, 1), (-1, -1), (1, 1), (1, -1)), ((-1, 2), (1, 2))
FAR0, FAR1, FAR2 = ((2, 0),), ((2, 1), (2, -1)), ((2, 2),)


def kernel(
    tokens_hbm,
    gain_hbm,
    wq_hbm,
    wk_hbm,
    wv_hbm,
    wglu_hbm,
    wgate_hbm,
    sink_hbm,
    taps_hbm,
    cgain_hbm,
    oa_hbm,
    oc_hbm,
    inner_hbm,
    outer_hbm,
    out_ref,
    wst,
    transit,
    win,
    wo,
    tok,
    nrmx,
    nrmd,
    meter,
    acc,
    qbuf,
    kvext,
    keys,
    vals,
    gtail,
    ghalo,
    gext,
    kvt,
    gain_ref,
    sink_ref,
    taps_ref,
    cgain_ref,
    gall,
    gfull,
    inner,
    outer,
    taps,
    mx,
    mixall,
    convn,
    local_sem,
    w_send,
    w_recv,
    t_send,
    t_recv,
    o_send,
    o_recv,
    m_send,
    m_recv,
    g_send,
    g_recv,
    halo_send,
    halo_recv,
):
    s = lax.axis_index("sp")
    t = lax.axis_index("tp")
    z, y = s // 4, lax.rem(s, 4)
    x, core = t // 2, lax.rem(t, 2)

    def al(v, m):
        return pl.multiple_of(v, m)

    def wrap(v, o):
        return lax.rem(v + (o + 4), 4)

    def sp_at(dz, dy):
        return wrap(z, dz) * 4 + wrap(y, dy)

    def tp_at(dx, mine=True):
        return wrap(x, dx) * 2 + (core if mine else 1 - core)

    partner = (s, tp_at(0, False))
    barrier = pltpu.get_barrier_semaphore()
    peers = [(sp_at(dz, dy), t) for dz, dy in ((0, 1), (0, -1), (1, 0), (-1, 0))]
    peers += [(s, tp_at(1)), (s, tp_at(-1)), partner]
    for peer in peers:
        pl.semaphore_signal(barrier, inc=1, device_id=peer, device_id_type=MESH)

    role_half = pl.ds(al(lax.rem(y, 2) * 128, 128), 128)
    loads = {}
    for name, src, dst in (
        ("tok", tokens_hbm, tok),
        ("gain", gain_hbm, gain_ref),
        ("wk", wk_hbm, kvt.at[0:64, :]),
        ("wv", wv_hbm, kvt.at[64:128, :]),
        ("q0", wq_hbm.at[:, 0:128], wst.at[2, :, 0:128]),
        ("q1", wq_hbm.at[:, 128:256], wst.at[3, :, 0:128]),
        ("glu0", wglu_hbm.at[:, 0:128], wst.at[0, :, 0:128]),
        ("glu1", wglu_hbm.at[:, 128:256], wst.at[1, :, 0:128]),
        ("gate0", wgate_hbm.at[:, 0:128], wst.at[0, :, 128:256]),
        ("gate1", wgate_hbm.at[:, 128:256], wst.at[1, :, 128:256]),
        ("oa", oa_hbm, wo.at[s, 0:128, :]),
        ("oc", oc_hbm, wo.at[s, 128:256, :]),
        ("taps", taps_hbm.at[:, role_half], taps_ref),
        ("cgain", cgain_hbm, cgain_ref),
        ("sink", sink_hbm, sink_ref),
        ("inner", inner_hbm, inner),
        ("outer", outer_hbm.at[pl.ds(z * 4, 4)], outer),
    ):
        copy = pltpu.make_async_copy(src, dst, local_sem.at[len(loads)])
        copy.start()
        loads[name] = copy

    def loaded(*names):
        for name in names:
            loads[name].wait()

    loaded("wk", "wv")
    kv_t = kvt[...].astype(F32).T.astype(BF16)
    wst[2, :, 128:256] = kv_t
    wst[3, :, 128:256] = kv_t
    loaded("tok", "gain")

    def norm_rows(i, carry):
        v = tok[pl.ds(al(i * 16, 16), 16), :].astype(F32)
        scale = lax.rsqrt(jnp.mean(v * v, axis=1, keepdims=True) + 1e-06)
        v = (v * scale * gain_ref[...]).astype(BF16)
        rows = pl.ds(al(y * ROWS + i * 16, 16), 16)
        for c in range(8):
            nrmx[c, rows, :] = v[:, c * XCOLS : (c + 1) * XCOLS]
        for c in range(2):
            nrmd[c, rows, :] = v[:, 8 * XCOLS + c * DCOLS : 8 * XCOLS + (c + 1) * DCOLS]
        return carry

    lax.fori_loop(0, ROWS // 16, norm_rows, 0)
    loaded("q0", "q1", "glu0", "glu1", "gate0", "gate1")
    pl.semaphore_wait(barrier, len(peers))

    w_net = Net(w_send, w_recv, meter, partner)
    t_net = Net(t_send, t_recv, meter, partner)
    o_net = Net(o_send, o_recv, meter, partner)
    m_net = Net(m_send, m_recv, meter, partner)
    g_net = Net(g_send, g_recv, meter, partner)

    def y_dev(d):
        return (sp_at(0, d), t)

    def z_dev(d):
        return (sp_at(d, 0), t)

    def x_dev(d):
        return (s, tp_at(d))

    def part_of(part, n):
        return {"full": (0, n), "lo": (0, n // 2), "hi": (n // 2, n // 2)}[part]

    def win_ref(o, off, part, mine=True):
        lo, n = part_of(part, ROWS)
        return win.at[pl.ds(al(sp_at(off, o) * ROWS + lo, 128), n), :]

    def tok_rows(o, part):
        lo, n = part_of(part, ROWS)
        return pl.ds(al(wrap(y, o) * ROWS + lo, 128), n)

    def tokx_ref(o, off, part, mine=True):
        return nrmx.at[tp_at(off, mine), tok_rows(o, part), :]

    def tokd_ref(o, off, part, mine=True):
        return nrmd.at[core if mine else 1 - core, tok_rows(o, part), :]

    def along_y(ref):
        return lambda o, off, part, mine=True: ref(off, 0, part, mine)

    tx_y = Ring(t_net, "txy", along_y(tokx_ref), y_dev)
    td_y = Ring(t_net, "tdy", along_y(tokd_ref), y_dev)
    tx_x = Ring(t_net, "txx", tokx_ref, x_dev)
    td_p = Ring(t_net, "tdp", tokd_ref, x_dev)
    w_z = Ring(w_net, "wz", win_ref, z_dev)

    def out_ref_of(h):
        base, size = ((0, OUT_SPLIT), (OUT_SPLIT, ROWS - OUT_SPLIT))[h]

        def first(o, off, part, mine=True):
            lo, n = part_of(part, size)
            src = sp_at(0, off) if h == 0 else sp_at(off, 0)
            return wo.at[src, pl.ds(base + lo, n), :]

        def second(o, off, part, mine=True):
            lo, n = part_of(part, size)
            src = sp_at(off, o) if h == 0 else sp_at(o, off)
            return wo.at[src, pl.ds(base + lo, n), :]

        return first, second

    o_first, o_second = [], []
    for h in (0, 1):
        f, g = out_ref_of(h)
        o_first.append(Ring(o_net, ("of", h), f, (y_dev, z_dev)[h]))
        o_second.append(Ring(o_net, ("os", h), g, (z_dev, y_dev)[h]))

    def w_first(name, parts):
        for d, part in zip((1, -1), parts):
            lo, n = part_of(part, ROWS)
            src = wst.at[wrap(y, d), pl.ds(lo, n), :]
            w_net.send(name, src, win_ref(0, 0, part), y_dev(d))

    tx_y.first(OWN_A)
    w_first("w_a", ("lo", "hi"))
    tx_y.first(OWN_B)
    w_first("w_b", ("hi", "lo"))
    for d in (1, -1):
        lo, n = part_of(side(d), ROWS)
        w_net.send("tr", wst.at[wrap(y, 2), pl.ds(lo, n), :], transit.at[(1 - d) // 2], y_dev(d))
    for name, sends in (("wz_a", OWN_A), ("wz_b", OWN_B)):
        for o, part, d in sends:
            lo, n = part_of(part, ROWS)
            w_net.send(name, wst.at[y, pl.ds(lo, n), :], win_ref(0, 0, part), z_dev(d))
    win[pl.ds(al(s * ROWS, ROWS), ROWS), :] = wst[y]
    loaded("oa", "oc")
    o_first[1].first(OWN_A, OWN_B)

    tx_y.first_wait(OWN_A)
    tx_y.second(OWN_F)
    tx_x.first(SIDES_A)
    w_net.wait("w_a")
    w_z.first(SIDES_A)
    tx_y.first_wait(OWN_B)
    tx_x.first(SIDES_B)
    tx_x.give(SIDES0)
    w_net.wait("w_b")
    w_z.first(SIDES_B)
    w_net.wait("wz_a")
    w_z.second(OWN_F)
    o_second[0].first(OWN_A, OWN_B)
    w_net.wait("tr")
    for d in (1, -1):
        w_net.send("trf", transit.at[(1 - d) // 2], win_ref(-d, 0, side(d)), y_dev(d))
    td_y.first(OWN_A, OWN_B)
    tx_y.second_wait(OWN_F)
    tx_x.first(FAR)
    tx_x.give(FAR0)
    tx_x.first_wait(SIDES_A)
    tx_x.second(SIDES_AF)
    w_net.wait("trf")
    w_z.first(FAR)
    w_z.first_wait(SIDES_A)
    w_z.second(SIDES_AF)
    w_z.first_wait(SIDES_B)
    w_z.second(SIDES_BF)
    tx_x.first_wait(SIDES_B)
    tx_x.second(SIDES_BF)
    tx_x.give(SIDES1)
    w_net.wait("wz_b")
    loaded("taps", "cgain", "sink", "inner", "outer")
    taps[...] = taps_ref[...].astype(F32)
    gall[t] = jnp.broadcast_to(cgain_ref[...], (8, 256))
    td_y.first_wait(OWN_A)
    td_y.second(OWN_F)
    o_first[0].first(OWN_A, OWN_B)
    w_z.first_wait(FAR)
    w_z.second(FAR_F)
    tx_x.first_wait(FAR)
    tx_x.second(FAR_F)
    tx_x.give(FAR1)
    td_y.first_wait(OWN_B)
    td_p.give(SIDES0)
    o_first[1].first_wait(OWN_A)
    o_first[1].second(OWN_F)
    o_first[1].first_wait(OWN_B)
    o_second[1].first(OWN_A, OWN_B, SIDES_A, SIDES_B)
    o_second[0].first_wait(OWN_A)
    o_second[0].second(OWN_F)
    o_second[0].first_wait(OWN_B)
    td_y.second_wait(OWN_F)
    td_p.give(FAR0)
    tx_x.second_wait(SIDES_AF, SIDES_BF)
    tx_x.give(SIDES2)

    def project(o):
        rows = pl.ds(al(wrap(y, o) * ROWS, ROWS), ROWS)
        parts = [nrmx[c, rows, :] for c in range(8)] + [nrmd[c, rows, :] for c in range(2)]
        whole = jnp.concatenate(parts, axis=1)
        acc[rows, :] = jnp.dot(whole, win[...], preferred_element_type=F32)

    def halo_copy(src, dst):
        return pltpu.make_async_remote_copy(
            src_ref=src,
            dst_ref=dst,
            send_sem=halo_send.at[0],
            recv_sem=halo_recv.at[0],
            device_id=z_dev(1),
            device_id_type=MESH,
        )

    lane = lax.broadcasted_iota(jnp.int32, (ROWS, 128), 1)
    first = lax.rem(lane, 64) < 32
    low = lane < 64
    low_w = low[:WINDOW, :]
    kv_halo = halo_copy(kvext.at[pl.ds(GROUP, WINDOW), :], kvext.at[pl.ds(0, WINDOW), :])
    gate_halo = halo_copy(gtail, ghalo)

    def rotate(v, cosine, sine):
        other = jnp.where(first, pltpu.roll(v, 96, 1), pltpu.roll(v, 32, 1))
        return v * cosine + other * sine

    def fill(b):
        rows = pl.ds(al(b * ROWS, ROWS), ROWS)
        ext = pl.ds(al(b * ROWS + WINDOW, WINDOW), ROWS)
        edge = outer[b]
        co, so = edge[:, 0:128], edge[:, 128:256]
        cosine = co * inner[:, 0:128] - so * inner[:, 128:256]
        sine = so * inner[:, 0:128] + co * inner[:, 128:256]
        sine = jnp.where(first, -sine, sine)
        q = rotate(acc[rows, 0:128], cosine, sine).astype(BF16).astype(F32)
        qbuf[rows, :] = (q * 0.125).astype(BF16)
        kv = rotate(acc[rows, 128:256], jnp.where(low, cosine, 1.0), jnp.where(low, sine, 0.0))
        kv = kv.astype(BF16)
        kvext[ext, :] = kv
        kv = kv.astype(F32)
        swapped = pltpu.roll(kv, 64, 1)
        keys[ext, :] = jnp.where(low, kv, swapped).astype(BF16)
        vals[ext, :] = jnp.where(low, swapped, kv).astype(BF16)

    def attend(b):
        zero = jnp.zeros((WINDOW, 128), BF16)
        second = lax.broadcasted_iota(jnp.int32, (2 * WINDOW, 1), 0) >= WINDOW
        sink_a = jnp.where(y == 2, sink_ref[0:1, 0:1], sink_ref[0:1, 2:3])
        sink_b = jnp.where(y == 2, sink_ref[0:1, 1:2], sink_ref[0:1, 3:4])
        sink = jnp.where(second, sink_b, sink_a)
        row_i = lax.rem(lax.broadcasted_iota(jnp.int32, (2 * WINDOW, 2 * WINDOW), 0), WINDOW)
        col_j = lax.broadcasted_iota(jnp.int32, (2 * WINDOW, 2 * WINDOW), 1)
        distance = row_i + WINDOW - col_j
        near = (distance >= 0) & (distance < WINDOW)
        near = near & (z * GROUP + (b - 1) * WINDOW + col_j >= 0)
        at = al(b * WINDOW, WINDOW)
        q = qbuf[pl.ds(at, WINDOW), :]
        stacked = jnp.concatenate([jnp.where(low_w, q, zero), jnp.where(low_w, zero, q)], axis=0)
        scores = lax.dot_general(
            stacked,
            keys[pl.ds(at, 2 * WINDOW), :],
            (((1,), (1,)), ((), ())),
            preferred_element_type=F32,
        )
        scores = jnp.where(near, scores, -1e30)
        top = jnp.maximum(jnp.max(scores, axis=1, keepdims=True), sink)
        e = jnp.exp(scores - top)
        denom = jnp.sum(e, axis=1, keepdims=True) + jnp.exp(sink - top)
        probs = (e * (1.0 / denom)).astype(BF16)
        att = jnp.dot(probs, vals[pl.ds(at, 2 * WINDOW), :], preferred_element_type=F32)
        mx[pl.ds(at, WINDOW), :] = jnp.where(low_w, att[:WINDOW, :], att[WINDOW:, :]).astype(BF16)

    def take_halo():
        kv_halo.wait_recv()
        edge = kvext[0:WINDOW, :].astype(F32)
        swapped = pltpu.roll(edge, 64, 1)
        keys[0:WINDOW, :] = jnp.where(low_w, edge, swapped).astype(BF16)
        vals[0:WINDOW, :] = jnp.where(low_w, swapped, edge).astype(BF16)
        kv_halo.wait_send()

    def attend_early():
        fill(3)
        kv_halo.start()

        def fill_others(i, carry):
            fill(jnp.where(i == 0, 3 - y, 0) + 2 * i)
            return carry

        lax.fori_loop(0, 2, fill_others, 0)

        def pair(i, carry):
            attend(jnp.where(y == 2, 3 + 2 * i, 1 + 5 * i))
            attend(jnp.where(y == 2, 4 + 2 * i, 5 + 2 * i))
            return carry

        lax.fori_loop(0, 2, pair, 0)
        pl.when(y == 3)(take_halo)
        attend(jnp.where(y == 2, 7, 0))

    def attend_late():
        fill(y - 2)
        attend(y)
        attend(jnp.where(y == 2, 1, 4))
        pl.when(y == 2)(take_halo)
        attend(jnp.where(y == 2, 0, 2))

    def gate_rows(b):
        rows = slice(b * ROWS, (b + 1) * ROWS)
        g = acc[rows, 0:128] * (0.5 + 0.5 * jnp.tanh(0.5 * acc[rows, 128:256]))
        gext[b * ROWS + 32 : (b + 1) * ROWS + 32, :] = g.astype(BF16).astype(F32)

    def send_tail():
        gtail[...] = gext[GROUP : GROUP + 32, :].astype(BF16)
        gate_halo.start()

    def filter_rows(r):
        f = jnp.zeros((64, 128), F32)
        for k in range(KSIZE):
            f = f + taps[k : k + 1, :] * gext[r + 2 + k : r + 66 + k, :]
        mx[r : r + 64, :] = f.astype(BF16)

    def late_rows(far):
        return [(far * ROWS + i * 64) % GROUP for i in range(5)]

    def filter_first():
        gate_halo.wait_recv()
        gext[0:32, :] = jnp.where(z > 0, ghalo[...].astype(F32), 0.0)
        filter_rows(0)
        gate_halo.wait_send()

    def filter_early(role):
        far = (role + 2) % 4
        for b in (3, 0, 1, 2):
            if b != far:
                gate_rows(b)
                if b == 3:
                    send_tail()
        for r in range(64, GROUP, 64):
            if r not in late_rows(far):
                filter_rows(r)
        if 0 not in late_rows(far):
            filter_first()

    def filter_late(role):
        far = (role + 2) % 4
        gate_rows(far)
        if far == 3:
            send_tail()
        for r in range(64, GROUP, 64):
            if r in late_rows(far):
                filter_rows(r)
        if 0 in late_rows(far):
            filter_first()

    def by_role(conv, attention):
        for role in range(2):
            pl.when(y == role)(lambda role=role: conv(role))
        pl.when(y >= 2)(attention)

    def mix_ref(o, off, part, mine=True):
        lo, n = part_of(part, ROWS)
        yy = wrap(y, o)
        cols = pl.ds(al(tp_at(off, mine) * 256 + lax.rem(yy, 2) * 128, 128), 128)
        return mixall.at[yy // 2, pl.ds(lo, n), cols]

    m_x = Ring(m_net, "mx", mix_ref, x_dev)
    own_cols = pl.ds(al(t * 256 + lax.rem(y, 2) * 128, 128), 128)

    def m_send(name, o, part):
        lo, n = part_of(part, ROWS)
        src = mx.at[pl.ds(al(wrap(y, o) * ROWS + lo, 128), n), :]
        m_net.send(name, src, mix_ref(0, 0, part), y_dev(o))

    w_z.second_wait(OWN_F, SIDES_AF, SIDES_BF, FAR_F)
    project(0)
    o_first[0].first_wait(OWN_A)
    o_first[0].second(OWN_F)
    o_second[0].first(SIDES_A)
    tx_x.second_wait(FAR_F)
    tx_x.give(FAR2)
    tx_x.give_wait(SIDES0, SIDES1, SIDES2)
    td_p.give_wait(SIDES0)
    project(-1)
    project(1)
    o_first[0].first_wait(OWN_B)
    o_second[0].first(SIDES_B)
    by_role(filter_early, attend_early)
    m_send("m_a", 1, "lo")
    m_send("m_a", -1, "hi")
    tx_x.give_wait(FAR0, FAR1, FAR2)
    td_p.give_wait(FAR0)
    project(2)
    mixall[y // 2, :, own_cols] = mx[pl.ds(al(y * ROWS, ROWS), ROWS), :]
    m_x.first(OWN_A, OWN_B)
    m_x.give(OWN0)
    o_first[1].second_wait(OWN_F)
    o_second[1].first(FAR)
    o_second[1].first_wait(OWN_A)
    o_second[1].second(OWN_F)
    o_second[1].first_wait(OWN_B)
    o_first[0].second_wait(OWN_F)
    o_second[0].first(FAR)
    for i in range(1, 8):
        g_net.send("gain", gall.at[t], gall.at[t], (s, lax.rem(t + i, 8)))
    by_role(filter_late, attend_late)
    m_send("m_far", 2, "full")
    m_send("m_b", -1, "lo")
    m_send("m_b", 1, "hi")
    m_net.wait("m_a")
    m_x.first(SIDES_A)
    m_x.first_wait(OWN_A)
    m_x.second(OWN_F)
    m_x.first_wait(OWN_B)
    m_x.give(OWN1)
    for ring in o_second:
        ring.first_wait(SIDES_A)
        ring.second(SIDES_AF)
        ring.first_wait(SIDES_B)
        ring.second(SIDES_BF)
    m_net.wait("m_b")
    m_x.first(SIDES_B)
    m_x.give(SIDES0)
    m_net.wait("m_far")
    m_net.send("m_far_x", mix_ref(2, 0, "full"), mix_ref(2, 0, "full"), x_dev(2))
    m_x.first(FAR)
    m_x.give(FAR0)
    m_x.second_wait(OWN_F)
    m_x.give(OWN2)
    m_x.first_wait(SIDES_A)
    m_x.second(SIDES_AF)
    o_second[1].first_wait(FAR)
    o_second[1].second(FAR_F)
    m_x.first_wait(SIDES_B)
    m_x.second(SIDES_BF)
    m_x.give(SIDES1)
    o_second[0].first_wait(FAR)
    o_second[0].second(FAR_F)
    m_x.first_wait(FAR)
    m_x.give(FAR1)
    m_net.wait("m_far_x")
    m_x.give(FAR2)
    g_net.wait("gain")
    for i in range(8):
        gfull[:, i * 256 : (i + 1) * 256] = gall[i, 0:1, :]
    m_x.second_wait(SIDES_AF, SIDES_BF)
    m_x.give(SIDES2)
    m_x.give_wait(OWN0, OWN1, OWN2, SIDES0, SIDES1, SIDES2, FAR0, FAR1, FAR2)

    def channel_norm(i, carry):
        rows = pl.ds(al(i * 32, 32), 32)
        f = mixall[0, rows, :].astype(F32)
        mean_value = jnp.sum(f, axis=1, keepdims=True) * (1.0 / CONV)
        variance = jnp.sum(f * f, axis=1, keepdims=True) * (1.0 / CONV) - mean_value * mean_value
        scaled = (f - mean_value) * lax.rsqrt(variance + 1e-05) * gfull[...]
        convn[rows, :] = (scaled * (0.5 + 0.5 * jnp.tanh(0.5 * scaled))).astype(BF16)
        return carry

    lax.fori_loop(0, ROWS // 32, channel_norm, 0)
    for ring in o_second:
        ring.second_wait(OWN_F, SIDES_AF, SIDES_BF, FAR_F)

    for c in range(0, OUTW, 256):
        w_attn = wo[:, 0:128, c : c + 256].reshape(2048, 256)
        w_conv = wo[:, 128:256, c : c + 256].reshape(2048, 256)
        v = jnp.dot(mixall[1], w_attn, preferred_element_type=F32)
        v = v + jnp.dot(convn[...], w_conv, preferred_element_type=F32)
        out_ref[:, c : c + 256] = v.astype(BF16)

    for net in (w_net, t_net, o_net, m_net, g_net):
        net.drain()


def per_device(
    tokens,
    norm_gain,
    w_query,
    w_key,
    w_value,
    w_glu,
    w_gate,
    sink_logit,
    conv_taps,
    conv_gain,
    out_attn,
    out_conv,
):
    hbm = pl.BlockSpec(memory_space=pltpu.HBM)
    vmem = pl.BlockSpec(memory_space=pltpu.VMEM)
    dma = pltpu.SemaphoreType.DMA
    inner, outer = rope_tables()
    tables = (jnp.asarray(inner), jnp.asarray(outer[:, None, :]))
    return pl.pallas_call(
        kernel,
        name="mixer_layer",
        out_shape=jax.ShapeDtypeStruct((ROWS, OUTW), BF16),
        in_specs=[hbm] * 14,
        out_specs=vmem,
        scratch_shapes=[
            pltpu.VMEM((4, ROWS, WIDTH), BF16),
            pltpu.VMEM((2, 128, WIDTH), BF16),
            pltpu.VMEM((D, WIDTH), BF16),
            pltpu.VMEM((16, ROWS, OUTW), BF16),
            pltpu.VMEM((ROWS, D), BF16),
            pltpu.VMEM((8, GROUP, XCOLS), BF16),
            pltpu.VMEM((2, GROUP, DCOLS), BF16),
            pltpu.VMEM((GROUP, D), BF16),
            pltpu.VMEM((GROUP, WIDTH), F32),
            pltpu.VMEM((GROUP, 128), BF16),
            pltpu.VMEM((GROUP + WINDOW, 128), BF16),
            pltpu.VMEM((GROUP + WINDOW, 128), BF16),
            pltpu.VMEM((GROUP + WINDOW, 128), BF16),
            pltpu.VMEM((32, 128), BF16),
            pltpu.VMEM((32, 128), BF16),
            pltpu.VMEM((GROUP + 32, 128), F32),
            pltpu.VMEM((128, ROWS), BF16),
            pltpu.VMEM((1, D), F32),
            pltpu.VMEM((1, 4), F32),
            pltpu.VMEM((KSIZE, 128), BF16),
            pltpu.VMEM((1, 256), F32),
            pltpu.VMEM((8, 8, 256), F32),
            pltpu.VMEM((1, 2048), F32),
            pltpu.VMEM((ROWS, 256), F32),
            pltpu.VMEM((4, 1, 256), F32),
            pltpu.VMEM((KSIZE, 128), F32),
            pltpu.VMEM((GROUP, 128), BF16),
            pltpu.VMEM((2, ROWS, 2048), BF16),
            pltpu.VMEM((ROWS, 2048), BF16),
            dma((17,)),
            dma((1,)),
            dma((SEMS,)),
            dma((1,)),
            dma((SEMS,)),
            dma((1,)),
            dma((SEMS,)),
            dma((1,)),
            dma((SEMS,)),
            dma((1,)),
            dma((1,)),
            dma((1,)),
            dma((1,)),
        ],
        compiler_params=pltpu.CompilerParams(
            collective_id=0, has_side_effects=True, vmem_limit_bytes=67043328
        ),
    )(
        tokens,
        norm_gain[None, :],
        w_query,
        w_key.T,
        w_value.T,
        w_glu,
        w_gate,
        sink_logit[None, :],
        conv_taps,
        conv_gain[None, :],
        out_attn,
        out_conv,
        *tables,
    )


def solution(mesh):
    return jax.shard_map(
        per_device,
        mesh=mesh,
        in_specs=(
            P("sp", None),
            P(),
            P("sp", "tp"),
            P("sp", "tp"),
            P("sp", "tp"),
            P("sp", "tp"),
            P("sp", "tp"),
            P("tp"),
            P(None, "tp"),
            P("tp"),
            P("sp", "tp"),
            P("sp", "tp"),
        ),
        out_specs=P("sp", "tp"),
        check_vma=False,
    )
```

```python
import jax
import jax.numpy as jnp
import numpy as np
from jax import lax
from jax.experimental import pallas as pl
from jax.experimental.pallas import tpu as pltpu
from jax.sharding import PartitionSpec as P

MESH = pl.DeviceIdType.MESH
F32 = jnp.float32
BF16 = jnp.bfloat16

ROWS = 256
GROUP = 1024
D = 4096
HEAD = 64
CONV = 2048
KSIZE = 31
WINDOW = 128
WIDTH = 256
OUTW = 512
XCOLS = 384
DCOLS = 512
OUT_SPLIT = 160
SEMS = {"w": 10, "t": 13, "o": 17, "m": 14}


def rope_tables():
    freq = (10000.0 ** (-np.arange(32, dtype=np.float64) * 2.0 / HEAD)).astype(np.float32)
    lanes = np.tile(freq.astype(np.float64), 4)[None, :]
    inner = np.arange(ROWS, dtype=np.float64)[:, None] * lanes
    outer = np.arange(16, dtype=np.float64)[:, None] * ROWS * lanes
    return tuple(
        np.concatenate([np.cos(a), np.sin(a)], axis=1).astype(np.float32) for a in (inner, outer)
    )


class Net:
    def __init__(self, send_sem, recv_sem, meter, partner):
        self.send_sem, self.recv_sem, self.meter, self.partner = send_sem, recv_sem, meter, partner
        self.index, self.size, self.total = {}, {}, 0
        self.joined, self.done = {}, set()

    def join(self, name, *groups):
        for group in groups:
            self.joined[group] = name

    def send(self, group, src, dst, device):
        group = self.joined.get(group, group)
        assert group not in self.done
        k = self.index.setdefault(group, len(self.index))
        assert k < self.recv_sem.shape[0]
        count = src.dtype.itemsize
        for n in src.shape:
            count *= n
        self.size[group] = self.size.get(group, 0) + count
        self.total += count
        pltpu.make_async_remote_copy(
            src_ref=src,
            dst_ref=dst,
            send_sem=self.send_sem.at[0],
            recv_sem=self.recv_sem.at[k],
            device_id=device,
            device_id_type=MESH,
        ).start()

    def await_bytes(self, sem, count):
        tiles = count // 2048
        across = max(n for n in range(1, 33) if tiles % n == 0)
        down = tiles // across
        assert tiles * 2048 == count and down <= 128
        counted = self.meter.at[0 : down * 8, 0 : across * 128]
        pltpu.make_async_copy(counted, counted, sem).wait()

    def wait(self, group):
        group = self.joined.get(group, group)
        if group in self.done:
            return
        self.done.add(group)
        self.await_bytes(self.recv_sem.at[self.index[group]], self.size[group])

    def drain(self):
        self.await_bytes(self.send_sem.at[0], self.total)


def side(d):
    return "lo" if d == 1 else "hi"


class Ring:
    def __init__(self, net, name, ref, device):
        self.net, self.name, self.ref, self.device = net, name, ref, device

    def first(self, *groups):
        for sends in groups:
            for o, part, d in sends:
                r = self.ref(o, 0, part)
                self.net.send((self.name, "T", sends), r, r, self.device(d))

    def first_wait(self, *groups):
        for sends in groups:
            self.net.wait((self.name, "T", sends))

    def second(self, *groups):
        for sends in groups:
            for o, d in sends:
                r = self.ref(o, -d, side(d))
                self.net.send((self.name, "F", sends), r, r, self.device(d))

    def second_wait(self, *groups):
        for sends in groups:
            self.net.wait((self.name, "F", sends))

    def give(self, *groups):
        for items in groups:
            for o, off in items:
                r = self.ref(o, off, "full")
                self.net.send((self.name, "P", items), r, r, self.net.partner)

    def give_wait(self, *groups):
        for items in groups:
            self.net.wait((self.name, "P", items))


def both(*items):
    return tuple((o, part, d) for o, part in items for d in (1, -1))


OWN_A = ((0, "lo", 1), (0, "hi", -1))
OWN_B = ((0, "hi", 1), (0, "lo", -1))
SIDES_A = both((-1, "lo"), (1, "hi"))
SIDES_B = both((-1, "hi"), (1, "lo"))
FAR = both((2, "lo"), (2, "hi"))
FAR_HI, FAR_LO = both((2, "hi")), both((2, "lo"))
FAR_HF = ((2, -1),)
OWN_F = ((0, 1), (0, -1))
SIDES_AF = ((-1, 1), (1, -1))
SIDES_BF = ((-1, -1), (1, 1))
FAR_F = ((2, 1), (2, -1))
OWN0, OWN1, OWN2 = ((0, 0),), ((0, 1), (0, -1)), ((0, 2),)
SIDES0, SIDES1, SIDES2 = ((-1, 0), (1, 0)), ((-1, 1), (-1, -1), (1, 1), (1, -1)), ((-1, 2), (1, 2))
FAR0, FAR1, FAR2 = ((2, 0),), ((2, 1), (2, -1)), ((2, 2),)


def kernel(
    tokens_hbm,
    gain_hbm,
    wq_hbm,
    wk_hbm,
    wv_hbm,
    wglu_hbm,
    wgate_hbm,
    sink_hbm,
    taps_hbm,
    cgain_hbm,
    oa_hbm,
    oc_hbm,
    inner_hbm,
    outer_hbm,
    out_ref,
    wst,
    transit,
    win,
    wo,
    tok,
    nrmx,
    nrmd,
    meter,
    acc,
    qbuf,
    kvext,
    keys,
    vals,
    gtail,
    ghalo,
    gext,
    kvt,
    gain_ref,
    sink_ref,
    taps_ref,
    cgain_ref,
    gall,
    gfull,
    inner,
    outer,
    taps,
    mx,
    mixall,
    convn,
    local_sem,
    w_send,
    w_recv,
    t_send,
    t_recv,
    o_send,
    o_recv,
    m_send,
    m_recv,
    g_send,
    g_recv,
    halo_send,
    halo_recv,
):
    s = lax.axis_index("sp")
    t = lax.axis_index("tp")
    z, y = s // 4, lax.rem(s, 4)
    x, core = t // 2, lax.rem(t, 2)

    def al(v, m):
        return pl.multiple_of(v, m)

    def wrap(v, o):
        return lax.rem(v + (o + 4), 4)

    def sp_at(dz, dy):
        return wrap(z, dz) * 4 + wrap(y, dy)

    def tp_at(dx, mine=True):
        return wrap(x, dx) * 2 + (core if mine else 1 - core)

    partner = (s, tp_at(0, False))
    barrier = pltpu.get_barrier_semaphore()
    peers = [(sp_at(dz, dy), t) for dz, dy in ((0, 1), (0, -1), (1, 0), (-1, 0))]
    peers += [(s, tp_at(1)), (s, tp_at(-1)), partner]
    for peer in peers:
        pl.semaphore_signal(barrier, inc=1, device_id=peer, device_id_type=MESH)

    role_half = pl.ds(al(lax.rem(y, 2) * 128, 128), 128)
    loads = {}
    for name, src, dst in (
        ("tok", tokens_hbm, tok),
        ("gain", gain_hbm, gain_ref),
        ("wk", wk_hbm, kvt.at[0:64, :]),
        ("wv", wv_hbm, kvt.at[64:128, :]),
        ("q0", wq_hbm.at[:, 0:128], wst.at[2, :, 0:128]),
        ("q1", wq_hbm.at[:, 128:256], wst.at[3, :, 0:128]),
        ("glu0", wglu_hbm.at[:, 0:128], wst.at[0, :, 0:128]),
        ("glu1", wglu_hbm.at[:, 128:256], wst.at[1, :, 0:128]),
        ("gate0", wgate_hbm.at[:, 0:128], wst.at[0, :, 128:256]),
        ("gate1", wgate_hbm.at[:, 128:256], wst.at[1, :, 128:256]),
        ("oa", oa_hbm, wo.at[s, 0:128, :]),
        ("oc", oc_hbm, wo.at[s, 128:256, :]),
        ("taps", taps_hbm.at[:, role_half], taps_ref),
        ("cgain", cgain_hbm, cgain_ref),
        ("sink", sink_hbm, sink_ref),
        ("inner", inner_hbm, inner),
        ("outer", outer_hbm.at[pl.ds(z * 4, 4)], outer),
    ):
        copy = pltpu.make_async_copy(src, dst, local_sem.at[len(loads)])
        copy.start()
        loads[name] = copy

    def loaded(*names):
        for name in names:
            loads[name].wait()

    loaded("wk", "wv")
    kv_t = kvt[...].astype(F32).T.astype(BF16)
    wst[2, :, 128:256] = kv_t
    wst[3, :, 128:256] = kv_t
    loaded("tok", "gain")

    def norm_rows(i, carry):
        v = tok[pl.ds(al(i * 16, 16), 16), :].astype(F32)
        scale = lax.rsqrt(jnp.mean(v * v, axis=1, keepdims=True) + 1e-06)
        v = (v * scale * gain_ref[...]).astype(BF16)
        rows = pl.ds(al(y * ROWS + i * 16, 16), 16)
        for c in range(8):
            nrmx[c, rows, :] = v[:, c * XCOLS : (c + 1) * XCOLS]
        for c in range(2):
            nrmd[c, rows, :] = v[:, 8 * XCOLS + c * DCOLS : 8 * XCOLS + (c + 1) * DCOLS]
        return carry

    lax.fori_loop(0, ROWS // 16, norm_rows, 0)
    loaded("q0", "q1", "glu0", "glu1", "gate0", "gate1")
    pl.semaphore_wait(barrier, len(peers))

    w_net = Net(w_send, w_recv, meter, partner)
    t_net = Net(t_send, t_recv, meter, partner)
    o_net = Net(o_send, o_recv, meter, partner)
    m_net = Net(m_send, m_recv, meter, partner)
    g_net = Net(g_send, g_recv, meter, partner)

    def y_dev(d):
        return (sp_at(0, d), t)

    def z_dev(d):
        return (sp_at(d, 0), t)

    def x_dev(d):
        return (s, tp_at(d))

    def part_of(part, n):
        return {"full": (0, n), "lo": (0, n // 2), "hi": (n // 2, n // 2)}[part]

    def win_ref(o, off, part, mine=True):
        lo, n = part_of(part, ROWS)
        return win.at[pl.ds(al(sp_at(off, o) * ROWS + lo, 128), n), :]

    def tok_rows(o, part):
        lo, n = part_of(part, ROWS)
        return pl.ds(al(wrap(y, o) * ROWS + lo, 128), n)

    def tokx_ref(o, off, part, mine=True):
        return nrmx.at[tp_at(off, mine), tok_rows(o, part), :]

    def tokd_ref(o, off, part, mine=True):
        return nrmd.at[core if mine else 1 - core, tok_rows(o, part), :]

    def along_y(ref):
        return lambda o, off, part, mine=True: ref(off, 0, part, mine)

    tx_y = Ring(t_net, "txy", along_y(tokx_ref), y_dev)
    td_y = Ring(t_net, "tdy", along_y(tokd_ref), y_dev)
    tx_x = Ring(t_net, "txx", tokx_ref, x_dev)
    td_p = Ring(t_net, "tdp", tokd_ref, x_dev)
    w_z = Ring(w_net, "wz", win_ref, z_dev)

    def out_ref_of(h):
        base, size = ((0, OUT_SPLIT), (OUT_SPLIT, ROWS - OUT_SPLIT))[h]

        def first(o, off, part, mine=True):
            lo, n = part_of(part, size)
            src = sp_at(0, off) if h == 0 else sp_at(off, 0)
            return wo.at[src, pl.ds(base + lo, n), :]

        def second(o, off, part, mine=True):
            lo, n = part_of(part, size)
            src = sp_at(off, o) if h == 0 else sp_at(o, off)
            return wo.at[src, pl.ds(base + lo, n), :]

        return first, second

    o_first, o_second = [], []
    for h in (0, 1):
        f, g = out_ref_of(h)
        o_first.append(Ring(o_net, ("of", h), f, (y_dev, z_dev)[h]))
        o_second.append(Ring(o_net, ("os", h), g, (z_dev, y_dev)[h]))

    def w_first(name, parts):
        for d, part in zip((1, -1), parts):
            lo, n = part_of(part, ROWS)
            src = wst.at[wrap(y, d), pl.ds(lo, n), :]
            w_net.send(name, src, win_ref(0, 0, part), y_dev(d))

    for items in (SIDES0, SIDES1, SIDES2):
        t_net.join("sides", ("txx", "P", items), ("tdp", "P", items))
        m_net.join("give", ("mx", "P", items))
    for items in (FAR0, FAR1, FAR2):
        t_net.join("far", ("txx", "P", items), ("tdp", "P", items))
        m_net.join("give", ("mx", "P", items))
    for items in (OWN0, OWN1, OWN2):
        m_net.join("give", ("mx", "P", items))
    for sends in (OWN_F, SIDES_AF, SIDES_BF, FAR_F):
        w_net.join("second", ("wz", "F", sends))
        o_net.join("second", (("os", 0), "F", sends), (("os", 1), "F", sends))
    for sends in (SIDES_AF, SIDES_BF):
        t_net.join("second", ("txx", "F", sends))
        m_net.join("second", ("mx", "F", sends))

    tx_y.first(OWN_A)
    w_first("w_a", ("lo", "hi"))
    tx_y.first(OWN_B)
    w_first("w_b", ("hi", "lo"))
    for d in (1, -1):
        lo, n = part_of(side(d), ROWS)
        w_net.send("tr", wst.at[wrap(y, 2), pl.ds(lo, n), :], transit.at[(1 - d) // 2], y_dev(d))
    for name, sends in (("wz_a", OWN_A), ("wz_b", OWN_B)):
        for o, part, d in sends:
            lo, n = part_of(part, ROWS)
            w_net.send(name, wst.at[y, pl.ds(lo, n), :], win_ref(0, 0, part), z_dev(d))
    win[pl.ds(al(s * ROWS, ROWS), ROWS), :] = wst[y]
    loaded("oa", "oc")
    o_first[1].first(OWN_A, OWN_B)

    tx_y.first_wait(OWN_A)
    tx_y.second(OWN_F)
    tx_x.first(SIDES_A)
    w_net.wait("w_a")
    w_z.first(SIDES_A)
    tx_y.first_wait(OWN_B)
    tx_x.first(SIDES_B)
    tx_x.give(SIDES0)
    w_net.wait("w_b")
    w_z.first(SIDES_B)
    w_net.wait("wz_a")
    w_z.second(OWN_F)
    o_second[0].first(OWN_A, OWN_B)
    w_net.wait("tr")
    for d in (1, -1):
        w_net.send("trf", transit.at[(1 - d) // 2], win_ref(-d, 0, side(d)), y_dev(d))
    td_y.first(OWN_A, OWN_B)
    tx_y.second_wait(OWN_F)
    tx_x.first(FAR)
    tx_x.give(FAR0)
    tx_x.first_wait(SIDES_A)
    tx_x.second(SIDES_AF)
    w_net.wait("trf")
    w_z.first(FAR)
    w_z.first_wait(SIDES_A)
    w_z.second(SIDES_AF)
    w_z.first_wait(SIDES_B)
    w_z.second(SIDES_BF)
    tx_x.first_wait(SIDES_B)
    tx_x.second(SIDES_BF)
    tx_x.give(SIDES1)
    w_net.wait("wz_b")
    loaded("taps", "cgain", "sink", "inner", "outer")
    taps[...] = taps_ref[...].astype(F32)
    gall[t] = jnp.broadcast_to(cgain_ref[...], (8, 256))
    td_y.first_wait(OWN_A)
    td_y.second(OWN_F)
    o_first[0].first(OWN_A, OWN_B)
    w_z.first_wait(FAR)
    w_z.second(FAR_F)
    tx_x.first_wait(FAR)
    tx_x.second(FAR_F)
    tx_x.give(FAR1)
    td_y.first_wait(OWN_B)
    td_p.give(SIDES0)
    o_first[1].first_wait(OWN_A)
    o_first[1].second(OWN_F)
    o_first[1].first_wait(OWN_B)
    o_second[1].first(OWN_A, OWN_B, SIDES_A, SIDES_B)
    o_second[0].first_wait(OWN_A)
    o_second[0].second(OWN_F)
    o_second[0].first_wait(OWN_B)
    td_y.second_wait(OWN_F)
    td_p.give(FAR0)
    tx_x.second_wait(SIDES_AF, SIDES_BF)
    tx_x.give(SIDES2)

    def project(o):
        rows = pl.ds(al(wrap(y, o) * ROWS, ROWS), ROWS)
        parts = [nrmx[c, rows, :] for c in range(8)] + [nrmd[c, rows, :] for c in range(2)]
        whole = jnp.concatenate(parts, axis=1)
        acc[rows, :] = jnp.dot(whole, win[...], preferred_element_type=F32)

    def halo_copy(src, dst):
        return pltpu.make_async_remote_copy(
            src_ref=src,
            dst_ref=dst,
            send_sem=halo_send.at[0],
            recv_sem=halo_recv.at[0],
            device_id=z_dev(1),
            device_id_type=MESH,
        )

    lane = lax.broadcasted_iota(jnp.int32, (ROWS, 128), 1)
    first = lax.rem(lane, 64) < 32
    low = lane < 64
    low_w = low[:WINDOW, :]
    kv_halo = halo_copy(kvext.at[pl.ds(GROUP, WINDOW), :], kvext.at[pl.ds(0, WINDOW), :])
    gate_halo = halo_copy(gtail, ghalo)

    def rotate(v, cosine, sine):
        other = jnp.where(first, pltpu.roll(v, 96, 1), pltpu.roll(v, 32, 1))
        return v * cosine + other * sine

    def fill(b):
        rows = pl.ds(al(b * ROWS, ROWS), ROWS)
        ext = pl.ds(al(b * ROWS + WINDOW, WINDOW), ROWS)
        edge = outer[b]
        co, so = edge[:, 0:128], edge[:, 128:256]
        cosine = co * inner[:, 0:128] - so * inner[:, 128:256]
        sine = so * inner[:, 0:128] + co * inner[:, 128:256]
        sine = jnp.where(first, -sine, sine)
        q = rotate(acc[rows, 0:128], cosine, sine).astype(BF16).astype(F32)
        qbuf[rows, :] = (q * 0.125).astype(BF16)
        kv = rotate(acc[rows, 128:256], jnp.where(low, cosine, 1.0), jnp.where(low, sine, 0.0))
        kv = kv.astype(BF16)
        kvext[ext, :] = kv
        kv = kv.astype(F32)
        swapped = pltpu.roll(kv, 64, 1)
        keys[ext, :] = jnp.where(low, kv, swapped).astype(BF16)
        vals[ext, :] = jnp.where(low, swapped, kv).astype(BF16)

    def attend(b):
        zero = jnp.zeros((WINDOW, 128), BF16)
        second = lax.broadcasted_iota(jnp.int32, (2 * WINDOW, 1), 0) >= WINDOW
        sink_a = jnp.where(y == 2, sink_ref[0:1, 0:1], sink_ref[0:1, 2:3])
        sink_b = jnp.where(y == 2, sink_ref[0:1, 1:2], sink_ref[0:1, 3:4])
        sink = jnp.where(second, sink_b, sink_a)
        row_i = lax.rem(lax.broadcasted_iota(jnp.int32, (2 * WINDOW, 2 * WINDOW), 0), WINDOW)
        col_j = lax.broadcasted_iota(jnp.int32, (2 * WINDOW, 2 * WINDOW), 1)
        distance = row_i + WINDOW - col_j
        near = (distance >= 0) & (distance < WINDOW)
        near = near & (z * GROUP + (b - 1) * WINDOW + col_j >= 0)
        at = al(b * WINDOW, WINDOW)
        q = qbuf[pl.ds(at, WINDOW), :]
        stacked = jnp.concatenate([jnp.where(low_w, q, zero), jnp.where(low_w, zero, q)], axis=0)
        scores = lax.dot_general(
            stacked,
            keys[pl.ds(at, 2 * WINDOW), :],
            (((1,), (1,)), ((), ())),
            preferred_element_type=F32,
        )
        scores = jnp.where(near, scores, -1e30)
        top = jnp.maximum(jnp.max(scores, axis=1, keepdims=True), sink)
        e = jnp.exp(scores - top)
        denom = jnp.sum(e, axis=1, keepdims=True) + jnp.exp(sink - top)
        probs = (e * (1.0 / denom)).astype(BF16)
        att = jnp.dot(probs, vals[pl.ds(at, 2 * WINDOW), :], preferred_element_type=F32)
        mx[pl.ds(at, WINDOW), :] = jnp.where(low_w, att[:WINDOW, :], att[WINDOW:, :]).astype(BF16)

    def take_halo():
        kv_halo.wait_recv()
        edge = kvext[0:WINDOW, :].astype(F32)
        swapped = pltpu.roll(edge, 64, 1)
        keys[0:WINDOW, :] = jnp.where(low_w, edge, swapped).astype(BF16)
        vals[0:WINDOW, :] = jnp.where(low_w, swapped, edge).astype(BF16)
        kv_halo.wait_send()

    def attend_early():
        fill(3)
        kv_halo.start()

        def fill_others(i, carry):
            fill(jnp.where(i == 0, 3 - y, 0) + 2 * i)
            return carry

        lax.fori_loop(0, 2, fill_others, 0)

        def pair(i, carry):
            attend(jnp.where(y == 2, 3 + 2 * i, 1 + 5 * i))
            attend(jnp.where(y == 2, 4 + 2 * i, 5 + 2 * i))
            return carry

        lax.fori_loop(0, 2, pair, 0)
        pl.when(y == 3)(take_halo)
        attend(jnp.where(y == 2, 7, 0))

    def attend_late():
        fill(y - 2)
        attend(y)
        attend(jnp.where(y == 2, 1, 4))
        pl.when(y == 2)(take_halo)
        attend(jnp.where(y == 2, 0, 2))

    def gate_rows(b):
        rows = slice(b * ROWS, (b + 1) * ROWS)
        g = acc[rows, 0:128] * (0.5 + 0.5 * jnp.tanh(0.5 * acc[rows, 128:256]))
        gext[b * ROWS + 32 : (b + 1) * ROWS + 32, :] = g.astype(BF16).astype(F32)

    def send_tail():
        gtail[...] = gext[GROUP : GROUP + 32, :].astype(BF16)
        gate_halo.start()

    def filter_rows(r):
        f = jnp.zeros((64, 128), F32)
        for k in range(KSIZE):
            f = f + taps[k : k + 1, :] * gext[r + 2 + k : r + 66 + k, :]
        mx[r : r + 64, :] = f.astype(BF16)

    def late_rows(far):
        return [(far * ROWS + i * 64) % GROUP for i in range(5)]

    def filter_first():
        gate_halo.wait_recv()
        gext[0:32, :] = jnp.where(z > 0, ghalo[...].astype(F32), 0.0)
        filter_rows(0)
        gate_halo.wait_send()

    def filter_early(role):
        far = (role + 2) % 4
        for b in (3, 0, 1, 2):
            if b != far:
                gate_rows(b)
                if b == 3:
                    send_tail()
        for r in range(64, GROUP, 64):
            if r not in late_rows(far):
                filter_rows(r)
        if 0 not in late_rows(far):
            filter_first()

    def filter_late(role):
        far = (role + 2) % 4
        gate_rows(far)
        if far == 3:
            send_tail()
        for r in range(64, GROUP, 64):
            if r in late_rows(far):
                filter_rows(r)
        if 0 in late_rows(far):
            filter_first()

    def by_role(conv, attention):
        for role in range(2):
            pl.when(y == role)(lambda role=role: conv(role))
        pl.when(y >= 2)(attention)

    def mix_ref(o, off, part, mine=True):
        lo, n = part_of(part, ROWS)
        yy = wrap(y, o)
        cols = pl.ds(al(tp_at(off, mine) * 256 + lax.rem(yy, 2) * 128, 128), 128)
        return mixall.at[yy // 2, pl.ds(lo, n), cols]

    m_x = Ring(m_net, "mx", mix_ref, x_dev)
    own_cols = pl.ds(al(t * 256 + lax.rem(y, 2) * 128, 128), 128)

    def m_send(name, o, part):
        lo, n = part_of(part, ROWS)
        src = mx.at[pl.ds(al(wrap(y, o) * ROWS + lo, 128), n), :]
        m_net.send(name, src, mix_ref(0, 0, part), y_dev(o))

    w_z.second_wait(OWN_F, SIDES_AF, SIDES_BF, FAR_F)
    project(0)
    o_first[0].first_wait(OWN_A)
    o_first[0].second(OWN_F)
    o_second[0].first(SIDES_A)
    tx_x.second_wait(FAR_F)
    tx_x.give(FAR2)
    tx_x.give_wait(SIDES0, SIDES1, SIDES2)
    td_p.give_wait(SIDES0)
    project(-1)
    project(1)
    o_first[0].first_wait(OWN_B)
    o_second[0].first(SIDES_B)
    by_role(filter_early, attend_early)
    m_send("m_a", 1, "lo")
    m_send("m_a", -1, "hi")
    tx_x.give_wait(FAR0, FAR1, FAR2)
    td_p.give_wait(FAR0)
    project(2)
    mixall[y // 2, :, own_cols] = mx[pl.ds(al(y * ROWS, ROWS), ROWS), :]
    m_x.first(OWN_A, OWN_B)
    m_x.give(OWN0)
    o_first[1].second_wait(OWN_F)
    o_second[1].first(FAR)
    o_second[1].first_wait(OWN_A)
    o_second[1].second(OWN_F)
    o_second[1].first_wait(OWN_B)
    o_first[0].second_wait(OWN_F)
    o_second[0].first(FAR)
    for i in range(1, 8):
        g_net.send("gain", gall.at[t], gall.at[t], (s, lax.rem(t + i, 8)))
    by_role(filter_late, attend_late)
    m_send("m_far", 2, "full")
    m_send("m_b", -1, "lo")
    m_send("m_b", 1, "hi")
    m_net.wait("m_a")
    m_x.first(SIDES_A)
    m_x.first_wait(OWN_A)
    m_x.second(OWN_F)
    m_x.first_wait(OWN_B)
    m_x.give(OWN1)
    m_net.wait("m_b")
    m_x.first(SIDES_B)
    m_x.give(SIDES0)
    m_net.wait("m_far")
    m_x.first(FAR_HI, FAR_LO)
    m_net.send("m_far_x", mix_ref(2, 0, "lo"), mix_ref(2, 0, "lo"), x_dev(2))
    m_x.give(FAR0)
    for ring in o_second:
        ring.first_wait(SIDES_A)
        ring.second(SIDES_AF)
        ring.first_wait(SIDES_B)
        ring.second(SIDES_BF)
    m_x.second_wait(OWN_F)
    m_x.give(OWN2)
    m_x.first_wait(SIDES_A)
    m_x.second(SIDES_AF)
    o_second[1].first_wait(FAR)
    o_second[1].second(FAR_F)
    m_x.first_wait(SIDES_B)
    m_x.second(SIDES_BF)
    m_x.give(SIDES1)
    o_second[0].first_wait(FAR)
    o_second[0].second(FAR_F)
    m_x.first_wait(FAR_HI)
    m_x.second(FAR_HF)
    m_x.first_wait(FAR_LO)
    m_x.give(FAR1)
    m_net.wait("m_far_x")
    m_x.second_wait(FAR_HF)
    m_x.give(FAR2)
    g_net.wait("gain")
    for i in range(8):
        gfull[:, i * 256 : (i + 1) * 256] = gall[i, 0:1, :]
    m_x.second_wait(SIDES_AF, SIDES_BF)
    m_x.give(SIDES2)
    m_x.give_wait(OWN0, OWN1, OWN2, SIDES0, SIDES1, SIDES2, FAR0, FAR1, FAR2)

    def channel_norm(i, carry):
        rows = pl.ds(al(i * 32, 32), 32)
        f = mixall[0, rows, :].astype(F32)
        mean_value = jnp.sum(f, axis=1, keepdims=True) * (1.0 / CONV)
        variance = jnp.sum(f * f, axis=1, keepdims=True) * (1.0 / CONV) - mean_value * mean_value
        scaled = (f - mean_value) * lax.rsqrt(variance + 1e-05) * gfull[...]
        convn[rows, :] = (scaled * (0.5 + 0.5 * jnp.tanh(0.5 * scaled))).astype(BF16)
        return carry

    lax.fori_loop(0, ROWS // 32, channel_norm, 0)
    for ring in o_second:
        ring.second_wait(OWN_F, SIDES_AF, SIDES_BF, FAR_F)

    for c in range(0, OUTW, 256):
        w_attn = wo[:, 0:128, c : c + 256].reshape(2048, 256)
        w_conv = wo[:, 128:256, c : c + 256].reshape(2048, 256)
        v = jnp.dot(mixall[1], w_attn, preferred_element_type=F32)
        v = v + jnp.dot(convn[...], w_conv, preferred_element_type=F32)
        out_ref[:, c : c + 256] = v.astype(BF16)

    for net in (w_net, t_net, o_net, m_net, g_net):
        net.drain()


def per_device(
    tokens,
    norm_gain,
    w_query,
    w_key,
    w_value,
    w_glu,
    w_gate,
    sink_logit,
    conv_taps,
    conv_gain,
    out_attn,
    out_conv,
):
    hbm = pl.BlockSpec(memory_space=pltpu.HBM)
    vmem = pl.BlockSpec(memory_space=pltpu.VMEM)
    dma = pltpu.SemaphoreType.DMA
    inner, outer = rope_tables()
    tables = (jnp.asarray(inner), jnp.asarray(outer[:, None, :]))
    return pl.pallas_call(
        kernel,
        name="mixer_layer",
        out_shape=jax.ShapeDtypeStruct((ROWS, OUTW), BF16),
        in_specs=[hbm] * 14,
        out_specs=vmem,
        scratch_shapes=[
            pltpu.VMEM((4, ROWS, WIDTH), BF16),
            pltpu.VMEM((2, 128, WIDTH), BF16),
            pltpu.VMEM((D, WIDTH), BF16),
            pltpu.VMEM((16, ROWS, OUTW), BF16),
            pltpu.VMEM((ROWS, D), BF16),
            pltpu.VMEM((8, GROUP, XCOLS), BF16),
            pltpu.VMEM((2, GROUP, DCOLS), BF16),
            pltpu.VMEM((GROUP, D), BF16),
            pltpu.VMEM((GROUP, WIDTH), F32),
            pltpu.VMEM((GROUP, 128), BF16),
            pltpu.VMEM((GROUP + WINDOW, 128), BF16),
            pltpu.VMEM((GROUP + WINDOW, 128), BF16),
            pltpu.VMEM((GROUP + WINDOW, 128), BF16),
            pltpu.VMEM((32, 128), BF16),
            pltpu.VMEM((32, 128), BF16),
            pltpu.VMEM((GROUP + 32, 128), F32),
            pltpu.VMEM((128, ROWS), BF16),
            pltpu.VMEM((1, D), F32),
            pltpu.VMEM((1, 4), F32),
            pltpu.VMEM((KSIZE, 128), BF16),
            pltpu.VMEM((1, 256), F32),
            pltpu.VMEM((8, 8, 256), F32),
            pltpu.VMEM((1, 2048), F32),
            pltpu.VMEM((ROWS, 256), F32),
            pltpu.VMEM((4, 1, 256), F32),
            pltpu.VMEM((KSIZE, 128), F32),
            pltpu.VMEM((GROUP, 128), BF16),
            pltpu.VMEM((2, ROWS, 2048), BF16),
            pltpu.VMEM((ROWS, 2048), BF16),
            dma((17,)),
            dma((1,)),
            dma((SEMS["w"],)),
            dma((1,)),
            dma((SEMS["t"],)),
            dma((1,)),
            dma((SEMS["o"],)),
            dma((1,)),
            dma((SEMS["m"],)),
            dma((1,)),
            dma((1,)),
            dma((1,)),
            dma((1,)),
        ],
        compiler_params=pltpu.CompilerParams(
            collective_id=0, has_side_effects=True, vmem_limit_bytes=67043328
        ),
    )(
        tokens,
        norm_gain[None, :],
        w_query,
        w_key.T,
        w_value.T,
        w_glu,
        w_gate,
        sink_logit[None, :],
        conv_taps,
        conv_gain[None, :],
        out_attn,
        out_conv,
        *tables,
    )


def solution(mesh):
    return jax.shard_map(
        per_device,
        mesh=mesh,
        in_specs=(
            P("sp", None),
            P(),
            P("sp", "tp"),
            P("sp", "tp"),
            P("sp", "tp"),
            P("sp", "tp"),
            P("sp", "tp"),
            P("tp"),
            P(None, "tp"),
            P("tp"),
            P("sp", "tp"),
            P("sp", "tp"),
        ),
        out_specs=P("sp", "tp"),
        check_vma=False,
    )
```

```python
import jax
import jax.numpy as jnp
import numpy as np
from jax import lax
from jax.experimental import pallas as pl
from jax.experimental.pallas import tpu as pltpu
from jax.sharding import PartitionSpec as P

MESH = pl.DeviceIdType.MESH
F32 = jnp.float32
BF16 = jnp.bfloat16

ROWS = 256
GROUP = 1024
D = 4096
HEAD = 64
CONV = 2048
KSIZE = 31
WINDOW = 128
WIDTH = 256
OUTW = 512
XCOLS = 384
DCOLS = 512
OUT_SPLIT = 160
SEMS = {"w": 10, "t": 13, "o": 17, "m": 15}


def rope_tables():
    freq = (10000.0 ** (-np.arange(32, dtype=np.float64) * 2.0 / HEAD)).astype(np.float32)
    lanes = np.tile(freq.astype(np.float64), 4)[None, :]
    inner = np.arange(ROWS, dtype=np.float64)[:, None] * lanes
    outer = np.arange(16, dtype=np.float64)[:, None] * ROWS * lanes
    return tuple(
        np.concatenate([np.cos(a), np.sin(a)], axis=1).astype(np.float32) for a in (inner, outer)
    )


class Net:
    def __init__(self, send_sem, recv_sem, meter, partner):
        self.send_sem, self.recv_sem, self.meter, self.partner = send_sem, recv_sem, meter, partner
        self.index, self.size, self.total = {}, {}, 0
        self.joined, self.done = {}, set()

    def join(self, name, *groups):
        for group in groups:
            self.joined[group] = name

    def send(self, group, src, dst, device):
        group = self.joined.get(group, group)
        assert group not in self.done
        k = self.index.setdefault(group, len(self.index))
        assert k < self.recv_sem.shape[0]
        count = src.dtype.itemsize
        for n in src.shape:
            count *= n
        self.size[group] = self.size.get(group, 0) + count
        self.total += count
        pltpu.make_async_remote_copy(
            src_ref=src,
            dst_ref=dst,
            send_sem=self.send_sem.at[0],
            recv_sem=self.recv_sem.at[k],
            device_id=device,
            device_id_type=MESH,
        ).start()

    def await_bytes(self, sem, count):
        tiles = count // 2048
        across = max(n for n in range(1, 33) if tiles % n == 0)
        down = tiles // across
        assert tiles * 2048 == count and down <= 128
        counted = self.meter.at[0 : down * 8, 0 : across * 128]
        pltpu.make_async_copy(counted, counted, sem).wait()

    def wait(self, group):
        group = self.joined.get(group, group)
        if group in self.done:
            return
        self.done.add(group)
        self.await_bytes(self.recv_sem.at[self.index[group]], self.size[group])

    def drain(self):
        self.await_bytes(self.send_sem.at[0], self.total)


def side(d):
    return "lo" if d == 1 else "hi"


class Ring:
    def __init__(self, net, name, ref, device):
        self.net, self.name, self.ref, self.device = net, name, ref, device

    def first(self, *groups):
        for sends in groups:
            for o, part, d in sends:
                r = self.ref(o, 0, part)
                self.net.send((self.name, "T", sends), r, r, self.device(d))

    def first_wait(self, *groups):
        for sends in groups:
            self.net.wait((self.name, "T", sends))

    def second(self, *groups):
        for sends in groups:
            for o, d in sends:
                r = self.ref(o, -d, side(d))
                self.net.send((self.name, "F", sends), r, r, self.device(d))

    def second_wait(self, *groups):
        for sends in groups:
            self.net.wait((self.name, "F", sends))

    def give(self, *groups):
        for items in groups:
            for o, off in items:
                r = self.ref(o, off, "full")
                self.net.send((self.name, "P", items), r, r, self.net.partner)

    def give_wait(self, *groups):
        for items in groups:
            self.net.wait((self.name, "P", items))


def both(*items):
    return tuple((o, part, d) for o, part in items for d in (1, -1))


OWN_A = ((0, "lo", 1), (0, "hi", -1))
OWN_B = ((0, "hi", 1), (0, "lo", -1))
SIDES_A = both((-1, "lo"), (1, "hi"))
SIDES_B = both((-1, "hi"), (1, "lo"))
FAR = both((2, "lo"), (2, "hi"))
FAR_HI, FAR_LO = both((2, "hi")), both((2, "lo"))
FAR_HF = ((2, -1),)
SOON = both((-1, "lo"), (1, "hi"), (-1, "hi"))
SOON_F = ((-1, 1), (1, -1), (-1, -1))
LATE, LATE_F = both((1, "lo")), ((1, 1),)
OWN_F = ((0, 1), (0, -1))
SIDES_AF = ((-1, 1), (1, -1))
SIDES_BF = ((-1, -1), (1, 1))
FAR_F = ((2, 1), (2, -1))
OWN0, OWN1, OWN2 = ((0, 0),), ((0, 1), (0, -1)), ((0, 2),)
SIDES0, SIDES1, SIDES2 = ((-1, 0), (1, 0)), ((-1, 1), (-1, -1), (1, 1), (1, -1)), ((-1, 2), (1, 2))
FAR0, FAR1, FAR2 = ((2, 0),), ((2, 1), (2, -1)), ((2, 2),)


def kernel(
    tokens_hbm,
    gain_hbm,
    wq_hbm,
    wk_hbm,
    wv_hbm,
    wglu_hbm,
    wgate_hbm,
    sink_hbm,
    taps_hbm,
    cgain_hbm,
    oa_hbm,
    oc_hbm,
    inner_hbm,
    outer_hbm,
    out_ref,
    wst,
    transit,
    win,
    wo,
    tok,
    nrmx,
    nrmd,
    meter,
    acc,
    qbuf,
    kvext,
    keys,
    vals,
    gtail,
    ghalo,
    gext,
    kvt,
    gain_ref,
    sink_ref,
    taps_ref,
    cgain_ref,
    gall,
    gfull,
    inner,
    outer,
    taps,
    mx,
    mixall,
    convn,
    local_sem,
    w_send,
    w_recv,
    t_send,
    t_recv,
    o_send,
    o_recv,
    m_send,
    m_recv,
    g_send,
    g_recv,
    halo_send,
    halo_recv,
):
    s = lax.axis_index("sp")
    t = lax.axis_index("tp")
    z, y = s // 4, lax.rem(s, 4)
    x, core = t // 2, lax.rem(t, 2)

    def al(v, m):
        return pl.multiple_of(v, m)

    def wrap(v, o):
        return lax.rem(v + (o + 4), 4)

    def sp_at(dz, dy):
        return wrap(z, dz) * 4 + wrap(y, dy)

    def tp_at(dx, mine=True):
        return wrap(x, dx) * 2 + (core if mine else 1 - core)

    partner = (s, tp_at(0, False))
    barrier = pltpu.get_barrier_semaphore()
    peers = [(sp_at(dz, dy), t) for dz, dy in ((0, 1), (0, -1), (1, 0), (-1, 0))]
    peers += [(s, tp_at(1)), (s, tp_at(-1)), partner]
    for peer in peers:
        pl.semaphore_signal(barrier, inc=1, device_id=peer, device_id_type=MESH)

    role_half = pl.ds(al(lax.rem(y, 2) * 128, 128), 128)
    loads = {}
    for name, src, dst in (
        ("tok", tokens_hbm, tok),
        ("gain", gain_hbm, gain_ref),
        ("wk", wk_hbm, kvt.at[0:64, :]),
        ("wv", wv_hbm, kvt.at[64:128, :]),
        ("q0", wq_hbm.at[:, 0:128], wst.at[2, :, 0:128]),
        ("q1", wq_hbm.at[:, 128:256], wst.at[3, :, 0:128]),
        ("glu0", wglu_hbm.at[:, 0:128], wst.at[0, :, 0:128]),
        ("glu1", wglu_hbm.at[:, 128:256], wst.at[1, :, 0:128]),
        ("gate0", wgate_hbm.at[:, 0:128], wst.at[0, :, 128:256]),
        ("gate1", wgate_hbm.at[:, 128:256], wst.at[1, :, 128:256]),
        ("oa", oa_hbm, wo.at[s, 0:128, :]),
        ("oc", oc_hbm, wo.at[s, 128:256, :]),
        ("taps", taps_hbm.at[:, role_half], taps_ref),
        ("cgain", cgain_hbm, cgain_ref),
        ("sink", sink_hbm, sink_ref),
        ("inner", inner_hbm, inner),
        ("outer", outer_hbm.at[pl.ds(z * 4, 4)], outer),
    ):
        copy = pltpu.make_async_copy(src, dst, local_sem.at[len(loads)])
        copy.start()
        loads[name] = copy

    def loaded(*names):
        for name in names:
            loads[name].wait()

    loaded("wk", "wv")
    kv_t = kvt[...].astype(F32).T.astype(BF16)
    wst[2, :, 128:256] = kv_t
    wst[3, :, 128:256] = kv_t
    loaded("tok", "gain")

    def norm_rows(i, carry):
        v = tok[pl.ds(al(i * 16, 16), 16), :].astype(F32)
        scale = lax.rsqrt(jnp.mean(v * v, axis=1, keepdims=True) + 1e-06)
        v = (v * scale * gain_ref[...]).astype(BF16)
        rows = pl.ds(al(y * ROWS + i * 16, 16), 16)
        for c in range(8):
            nrmx[c, rows, :] = v[:, c * XCOLS : (c + 1) * XCOLS]
        for c in range(2):
            nrmd[c, rows, :] = v[:, 8 * XCOLS + c * DCOLS : 8 * XCOLS + (c + 1) * DCOLS]
        return carry

    lax.fori_loop(0, ROWS // 16, norm_rows, 0)
    loaded("q0", "q1", "glu0", "glu1", "gate0", "gate1")
    pl.semaphore_wait(barrier, len(peers))

    w_net = Net(w_send, w_recv, meter, partner)
    t_net = Net(t_send, t_recv, meter, partner)
    o_net = Net(o_send, o_recv, meter, partner)
    m_net = Net(m_send, m_recv, meter, partner)
    g_net = Net(g_send, g_recv, meter, partner)

    def y_dev(d):
        return (sp_at(0, d), t)

    def z_dev(d):
        return (sp_at(d, 0), t)

    def x_dev(d):
        return (s, tp_at(d))

    def part_of(part, n):
        return {"full": (0, n), "lo": (0, n // 2), "hi": (n // 2, n // 2)}[part]

    def win_ref(o, off, part, mine=True):
        lo, n = part_of(part, ROWS)
        return win.at[pl.ds(al(sp_at(off, o) * ROWS + lo, 128), n), :]

    def tok_rows(o, part):
        lo, n = part_of(part, ROWS)
        return pl.ds(al(wrap(y, o) * ROWS + lo, 128), n)

    def tokx_ref(o, off, part, mine=True):
        return nrmx.at[tp_at(off, mine), tok_rows(o, part), :]

    def tokd_ref(o, off, part, mine=True):
        return nrmd.at[core if mine else 1 - core, tok_rows(o, part), :]

    def along_y(ref):
        return lambda o, off, part, mine=True: ref(off, 0, part, mine)

    tx_y = Ring(t_net, "txy", along_y(tokx_ref), y_dev)
    td_y = Ring(t_net, "tdy", along_y(tokd_ref), y_dev)
    tx_x = Ring(t_net, "txx", tokx_ref, x_dev)
    td_p = Ring(t_net, "tdp", tokd_ref, x_dev)
    w_z = Ring(w_net, "wz", win_ref, z_dev)

    def out_ref_of(h):
        base, size = ((0, OUT_SPLIT), (OUT_SPLIT, ROWS - OUT_SPLIT))[h]

        def first(o, off, part, mine=True):
            lo, n = part_of(part, size)
            src = sp_at(0, off) if h == 0 else sp_at(off, 0)
            return wo.at[src, pl.ds(base + lo, n), :]

        def second(o, off, part, mine=True):
            lo, n = part_of(part, size)
            src = sp_at(off, o) if h == 0 else sp_at(o, off)
            return wo.at[src, pl.ds(base + lo, n), :]

        return first, second

    o_first, o_second = [], []
    for h in (0, 1):
        f, g = out_ref_of(h)
        o_first.append(Ring(o_net, ("of", h), f, (y_dev, z_dev)[h]))
        o_second.append(Ring(o_net, ("os", h), g, (z_dev, y_dev)[h]))

    def w_first(name, parts):
        for d, part in zip((1, -1), parts):
            lo, n = part_of(part, ROWS)
            src = wst.at[wrap(y, d), pl.ds(lo, n), :]
            w_net.send(name, src, win_ref(0, 0, part), y_dev(d))

    for items in (SIDES0, SIDES1, SIDES2):
        t_net.join("sides", ("txx", "P", items), ("tdp", "P", items))
        m_net.join("give", ("mx", "P", items))
    for items in (FAR0, FAR1, FAR2):
        t_net.join("far", ("txx", "P", items), ("tdp", "P", items))
        m_net.join("give", ("mx", "P", items))
    for items in (OWN0, OWN1, OWN2):
        m_net.join("give", ("mx", "P", items))
    for sends in (OWN_F, SIDES_AF, SIDES_BF, FAR_F):
        w_net.join("second", ("wz", "F", sends))
        o_net.join("second", (("os", 0), "F", sends), (("os", 1), "F", sends))
    m_net.join("second", ("mx", "F", SOON_F), ("mx", "F", LATE_F))
    for sends in (SIDES_AF, SIDES_BF):
        t_net.join("second", ("txx", "F", sends))

    tx_y.first(OWN_A)
    w_first("w_a", ("lo", "hi"))
    tx_y.first(OWN_B)
    w_first("w_b", ("hi", "lo"))
    for d in (1, -1):
        lo, n = part_of(side(d), ROWS)
        w_net.send("tr", wst.at[wrap(y, 2), pl.ds(lo, n), :], transit.at[(1 - d) // 2], y_dev(d))
    for name, sends in (("wz_a", OWN_A), ("wz_b", OWN_B)):
        for o, part, d in sends:
            lo, n = part_of(part, ROWS)
            w_net.send(name, wst.at[y, pl.ds(lo, n), :], win_ref(0, 0, part), z_dev(d))
    win[pl.ds(al(s * ROWS, ROWS), ROWS), :] = wst[y]
    loaded("oa", "oc")
    o_first[1].first(OWN_A, OWN_B)

    tx_y.first_wait(OWN_A)
    tx_y.second(OWN_F)
    tx_x.first(SIDES_A)
    w_net.wait("w_a")
    w_z.first(SIDES_A)
    tx_y.first_wait(OWN_B)
    tx_x.first(SIDES_B)
    tx_x.give(SIDES0)
    w_net.wait("w_b")
    w_z.first(SIDES_B)
    w_net.wait("wz_a")
    w_z.second(OWN_F)
    o_second[0].first(OWN_A, OWN_B)
    w_net.wait("tr")
    for d in (1, -1):
        w_net.send("trf", transit.at[(1 - d) // 2], win_ref(-d, 0, side(d)), y_dev(d))
    td_y.first(OWN_A, OWN_B)
    tx_y.second_wait(OWN_F)
    tx_x.first(FAR)
    tx_x.give(FAR0)
    tx_x.first_wait(SIDES_A)
    tx_x.second(SIDES_AF)
    w_net.wait("trf")
    w_z.first(FAR)
    w_z.first_wait(SIDES_A)
    w_z.second(SIDES_AF)
    w_z.first_wait(SIDES_B)
    w_z.second(SIDES_BF)
    tx_x.first_wait(SIDES_B)
    tx_x.second(SIDES_BF)
    tx_x.give(SIDES1)
    w_net.wait("wz_b")
    loaded("taps", "cgain", "sink", "inner", "outer")
    taps[...] = taps_ref[...].astype(F32)
    gall[t] = jnp.broadcast_to(cgain_ref[...], (8, 256))
    td_y.first_wait(OWN_A)
    td_y.second(OWN_F)
    o_first[0].first(OWN_A, OWN_B)
    w_z.first_wait(FAR)
    w_z.second(FAR_F)
    tx_x.first_wait(FAR)
    tx_x.second(FAR_F)
    tx_x.give(FAR1)
    td_y.first_wait(OWN_B)
    td_p.give(SIDES0)
    o_first[1].first_wait(OWN_A)
    o_first[1].second(OWN_F)
    o_first[1].first_wait(OWN_B)
    o_second[1].first(OWN_A, OWN_B, SIDES_A, SIDES_B)
    o_second[0].first_wait(OWN_A)
    o_second[0].second(OWN_F)
    o_second[0].first_wait(OWN_B)
    td_y.second_wait(OWN_F)
    td_p.give(FAR0)
    tx_x.second_wait(SIDES_AF, SIDES_BF)
    tx_x.give(SIDES2)

    def project(o):
        rows = pl.ds(al(wrap(y, o) * ROWS, ROWS), ROWS)
        parts = [nrmx[c, rows, :] for c in range(8)] + [nrmd[c, rows, :] for c in range(2)]
        whole = jnp.concatenate(parts, axis=1)
        acc[rows, :] = jnp.dot(whole, win[...], preferred_element_type=F32)

    def halo_copy(src, dst):
        return pltpu.make_async_remote_copy(
            src_ref=src,
            dst_ref=dst,
            send_sem=halo_send.at[0],
            recv_sem=halo_recv.at[0],
            device_id=z_dev(1),
            device_id_type=MESH,
        )

    lane = lax.broadcasted_iota(jnp.int32, (ROWS, 128), 1)
    first = lax.rem(lane, 64) < 32
    low = lane < 64
    low_w = low[:WINDOW, :]
    kv_halo = halo_copy(kvext.at[pl.ds(GROUP, WINDOW), :], kvext.at[pl.ds(0, WINDOW), :])
    gate_halo = halo_copy(gtail, ghalo)

    def rotate(v, cosine, sine):
        other = jnp.where(first, pltpu.roll(v, 96, 1), pltpu.roll(v, 32, 1))
        return v * cosine + other * sine

    def fill(b):
        rows = pl.ds(al(b * ROWS, ROWS), ROWS)
        ext = pl.ds(al(b * ROWS + WINDOW, WINDOW), ROWS)
        edge = outer[b]
        co, so = edge[:, 0:128], edge[:, 128:256]
        cosine = co * inner[:, 0:128] - so * inner[:, 128:256]
        sine = so * inner[:, 0:128] + co * inner[:, 128:256]
        sine = jnp.where(first, -sine, sine)
        q = rotate(acc[rows, 0:128], cosine, sine).astype(BF16).astype(F32)
        qbuf[rows, :] = (q * 0.125).astype(BF16)
        kv = rotate(acc[rows, 128:256], jnp.where(low, cosine, 1.0), jnp.where(low, sine, 0.0))
        kv = kv.astype(BF16)
        kvext[ext, :] = kv
        kv = kv.astype(F32)
        swapped = pltpu.roll(kv, 64, 1)
        keys[ext, :] = jnp.where(low, kv, swapped).astype(BF16)
        vals[ext, :] = jnp.where(low, swapped, kv).astype(BF16)

    def attend(b):
        zero = jnp.zeros((WINDOW, 128), BF16)
        second = lax.broadcasted_iota(jnp.int32, (2 * WINDOW, 1), 0) >= WINDOW
        sink_a = jnp.where(y == 2, sink_ref[0:1, 0:1], sink_ref[0:1, 2:3])
        sink_b = jnp.where(y == 2, sink_ref[0:1, 1:2], sink_ref[0:1, 3:4])
        sink = jnp.where(second, sink_b, sink_a)
        row_i = lax.rem(lax.broadcasted_iota(jnp.int32, (2 * WINDOW, 2 * WINDOW), 0), WINDOW)
        col_j = lax.broadcasted_iota(jnp.int32, (2 * WINDOW, 2 * WINDOW), 1)
        distance = row_i + WINDOW - col_j
        near = (distance >= 0) & (distance < WINDOW)
        near = near & (z * GROUP + (b - 1) * WINDOW + col_j >= 0)
        at = al(b * WINDOW, WINDOW)
        q = qbuf[pl.ds(at, WINDOW), :]
        stacked = jnp.concatenate([jnp.where(low_w, q, zero), jnp.where(low_w, zero, q)], axis=0)
        scores = lax.dot_general(
            stacked,
            keys[pl.ds(at, 2 * WINDOW), :],
            (((1,), (1,)), ((), ())),
            preferred_element_type=F32,
        )
        scores = jnp.where(near, scores, -1e30)
        top = jnp.maximum(jnp.max(scores, axis=1, keepdims=True), sink)
        e = jnp.exp(scores - top)
        denom = jnp.sum(e, axis=1, keepdims=True) + jnp.exp(sink - top)
        probs = (e * (1.0 / denom)).astype(BF16)
        att = jnp.dot(probs, vals[pl.ds(at, 2 * WINDOW), :], preferred_element_type=F32)
        mx[pl.ds(at, WINDOW), :] = jnp.where(low_w, att[:WINDOW, :], att[WINDOW:, :]).astype(BF16)

    def take_halo():
        kv_halo.wait_recv()
        edge = kvext[0:WINDOW, :].astype(F32)
        swapped = pltpu.roll(edge, 64, 1)
        keys[0:WINDOW, :] = jnp.where(low_w, edge, swapped).astype(BF16)
        vals[0:WINDOW, :] = jnp.where(low_w, swapped, edge).astype(BF16)
        kv_halo.wait_send()

    def attend_early():
        fill(3)
        kv_halo.start()

        def fill_others(i, carry):
            fill(jnp.where(i == 0, 3 - y, 0) + 2 * i)
            return carry

        lax.fori_loop(0, 2, fill_others, 0)

        def pair(i, carry):
            attend(jnp.where(y == 2, 3 + 2 * i, 1 + 5 * i))
            attend(jnp.where(y == 2, 4 + 2 * i, 5 + 2 * i))
            return carry

        lax.fori_loop(0, 2, pair, 0)
        pl.when(y == 3)(take_halo)
        attend(jnp.where(y == 2, 7, 0))

    def attend_late():
        fill(y - 2)
        attend(y)
        attend(jnp.where(y == 2, 1, 4))
        pl.when(y == 2)(take_halo)
        attend(jnp.where(y == 2, 0, 2))

    def gate_rows(b):
        rows = slice(b * ROWS, (b + 1) * ROWS)
        g = acc[rows, 0:128] * (0.5 + 0.5 * jnp.tanh(0.5 * acc[rows, 128:256]))
        gext[b * ROWS + 32 : (b + 1) * ROWS + 32, :] = g.astype(BF16).astype(F32)

    def send_tail():
        gtail[...] = gext[GROUP : GROUP + 32, :].astype(BF16)
        gate_halo.start()

    def filter_rows(r):
        f = jnp.zeros((64, 128), F32)
        for k in range(KSIZE):
            f = f + taps[k : k + 1, :] * gext[r + 2 + k : r + 66 + k, :]
        mx[r : r + 64, :] = f.astype(BF16)

    def late_rows(far):
        return [(far * ROWS + i * 64) % GROUP for i in range(5)]

    def filter_first():
        gate_halo.wait_recv()
        gext[0:32, :] = jnp.where(z > 0, ghalo[...].astype(F32), 0.0)
        filter_rows(0)
        gate_halo.wait_send()

    def filter_early(role):
        far = (role + 2) % 4
        for b in (3, 0, 1, 2):
            if b != far:
                gate_rows(b)
                if b == 3:
                    send_tail()
        for r in range(64, GROUP, 64):
            if r not in late_rows(far):
                filter_rows(r)
        if 0 not in late_rows(far):
            filter_first()

    def filter_late(role):
        far = (role + 2) % 4
        gate_rows(far)
        if far == 3:
            send_tail()
        for r in range(64, GROUP, 64):
            if r in late_rows(far):
                filter_rows(r)
        if 0 in late_rows(far):
            filter_first()

    def by_role(conv, attention):
        for role in range(2):
            pl.when(y == role)(lambda role=role: conv(role))
        pl.when(y >= 2)(attention)

    def mix_ref(o, off, part, mine=True):
        lo, n = part_of(part, ROWS)
        yy = wrap(y, o)
        cols = pl.ds(al(tp_at(off, mine) * 256 + lax.rem(yy, 2) * 128, 128), 128)
        return mixall.at[yy // 2, pl.ds(lo, n), cols]

    m_x = Ring(m_net, "mx", mix_ref, x_dev)
    own_cols = pl.ds(al(t * 256 + lax.rem(y, 2) * 128, 128), 128)

    def m_send(name, o, part):
        lo, n = part_of(part, ROWS)
        src = mx.at[pl.ds(al(wrap(y, o) * ROWS + lo, 128), n), :]
        m_net.send(name, src, mix_ref(0, 0, part), y_dev(o))

    w_z.second_wait(OWN_F, SIDES_AF, SIDES_BF, FAR_F)
    project(0)
    o_first[0].first_wait(OWN_A)
    o_first[0].second(OWN_F)
    o_second[0].first(SIDES_A)
    tx_x.second_wait(FAR_F)
    tx_x.give(FAR2)
    tx_x.give_wait(SIDES0, SIDES1, SIDES2)
    td_p.give_wait(SIDES0)
    project(-1)
    project(1)
    o_first[0].first_wait(OWN_B)
    o_second[0].first(SIDES_B)
    by_role(filter_early, attend_early)
    m_send("m_a", 1, "lo")
    m_send("m_a", -1, "hi")
    m_send("m_a", 1, "hi")
    tx_x.give_wait(FAR0, FAR1, FAR2)
    td_p.give_wait(FAR0)
    project(2)
    mixall[y // 2, :, own_cols] = mx[pl.ds(al(y * ROWS, ROWS), ROWS), :]
    m_x.first(OWN_A, OWN_B)
    m_x.give(OWN0)
    o_first[1].second_wait(OWN_F)
    o_second[1].first(FAR)
    o_second[1].first_wait(OWN_A)
    o_second[1].second(OWN_F)
    o_second[1].first_wait(OWN_B)
    o_first[0].second_wait(OWN_F)
    o_second[0].first(FAR)
    for i in range(1, 8):
        g_net.send("gain", gall.at[t], gall.at[t], (s, lax.rem(t + i, 8)))
    by_role(filter_late, attend_late)
    m_send("m_far_hi", 2, "hi")
    m_send("m_b", -1, "lo")
    m_send("m_far_lo", 2, "lo")
    m_net.wait("m_a")
    m_x.first(SOON)
    m_x.first_wait(OWN_A)
    m_x.second(OWN_F)
    m_x.first_wait(OWN_B)
    m_x.give(OWN1)
    m_net.wait("m_b")
    m_x.first(LATE)
    m_x.give(SIDES0)
    m_net.wait("m_far_hi")
    m_x.first(FAR_HI)
    m_net.wait("m_far_lo")
    m_x.first(FAR_LO)
    m_net.send("m_far_x", mix_ref(2, 0, "lo"), mix_ref(2, 0, "lo"), x_dev(2))
    m_x.give(FAR0)
    for ring in o_second:
        ring.first_wait(SIDES_A)
        ring.second(SIDES_AF)
        ring.first_wait(SIDES_B)
        ring.second(SIDES_BF)
    m_x.second_wait(OWN_F)
    m_x.give(OWN2)
    m_x.first_wait(SOON)
    m_x.second(SOON_F)
    m_x.first_wait(LATE)
    m_x.second(LATE_F)
    m_x.give(SIDES1)
    m_x.first_wait(FAR_HI)
    m_x.second(FAR_HF)
    o_second[1].first_wait(FAR)
    o_second[1].second(FAR_F)
    o_second[0].first_wait(FAR)
    o_second[0].second(FAR_F)
    m_x.first_wait(FAR_LO)
    m_x.give(FAR1)
    g_net.wait("gain")
    for i in range(8):
        gfull[:, i * 256 : (i + 1) * 256] = gall[i, 0:1, :]
    m_x.second_wait(SOON_F, LATE_F)
    m_x.give(SIDES2)
    m_net.wait("m_far_x")
    m_x.second_wait(FAR_HF)
    m_x.give(FAR2)
    m_x.give_wait(OWN0, OWN1, OWN2, SIDES0, SIDES1, SIDES2, FAR0, FAR1, FAR2)

    def channel_norm(i, carry):
        rows = pl.ds(al(i * 32, 32), 32)
        f = mixall[0, rows, :].astype(F32)
        mean_value = jnp.sum(f, axis=1, keepdims=True) * (1.0 / CONV)
        variance = jnp.sum(f * f, axis=1, keepdims=True) * (1.0 / CONV) - mean_value * mean_value
        scaled = (f - mean_value) * lax.rsqrt(variance + 1e-05) * gfull[...]
        convn[rows, :] = (scaled * (0.5 + 0.5 * jnp.tanh(0.5 * scaled))).astype(BF16)
        return carry

    lax.fori_loop(0, ROWS // 32, channel_norm, 0)
    for ring in o_second:
        ring.second_wait(OWN_F, SIDES_AF, SIDES_BF, FAR_F)

    for c in range(0, OUTW, 256):
        w_attn = wo[:, 0:128, c : c + 256].reshape(2048, 256)
        w_conv = wo[:, 128:256, c : c + 256].reshape(2048, 256)
        v = jnp.dot(mixall[1], w_attn, preferred_element_type=F32)
        v = v + jnp.dot(convn[...], w_conv, preferred_element_type=F32)
        out_ref[:, c : c + 256] = v.astype(BF16)

    for net in (w_net, t_net, o_net, m_net, g_net):
        net.drain()


def per_device(
    tokens,
    norm_gain,
    w_query,
    w_key,
    w_value,
    w_glu,
    w_gate,
    sink_logit,
    conv_taps,
    conv_gain,
    out_attn,
    out_conv,
):
    hbm = pl.BlockSpec(memory_space=pltpu.HBM)
    vmem = pl.BlockSpec(memory_space=pltpu.VMEM)
    dma = pltpu.SemaphoreType.DMA
    inner, outer = rope_tables()
    tables = (jnp.asarray(inner), jnp.asarray(outer[:, None, :]))
    return pl.pallas_call(
        kernel,
        name="mixer_layer",
        out_shape=jax.ShapeDtypeStruct((ROWS, OUTW), BF16),
        in_specs=[hbm] * 14,
        out_specs=vmem,
        scratch_shapes=[
            pltpu.VMEM((4, ROWS, WIDTH), BF16),
            pltpu.VMEM((2, 128, WIDTH), BF16),
            pltpu.VMEM((D, WIDTH), BF16),
            pltpu.VMEM((16, ROWS, OUTW), BF16),
            pltpu.VMEM((ROWS, D), BF16),
            pltpu.VMEM((8, GROUP, XCOLS), BF16),
            pltpu.VMEM((2, GROUP, DCOLS), BF16),
            pltpu.VMEM((GROUP, D), BF16),
            pltpu.VMEM((GROUP, WIDTH), F32),
            pltpu.VMEM((GROUP, 128), BF16),
            pltpu.VMEM((GROUP + WINDOW, 128), BF16),
            pltpu.VMEM((GROUP + WINDOW, 128), BF16),
            pltpu.VMEM((GROUP + WINDOW, 128), BF16),
            pltpu.VMEM((32, 128), BF16),
            pltpu.VMEM((32, 128), BF16),
            pltpu.VMEM((GROUP + 32, 128), F32),
            pltpu.VMEM((128, ROWS), BF16),
            pltpu.VMEM((1, D), F32),
            pltpu.VMEM((1, 4), F32),
            pltpu.VMEM((KSIZE, 128), BF16),
            pltpu.VMEM((1, 256), F32),
            pltpu.VMEM((8, 8, 256), F32),
            pltpu.VMEM((1, 2048), F32),
            pltpu.VMEM((ROWS, 256), F32),
            pltpu.VMEM((4, 1, 256), F32),
            pltpu.VMEM((KSIZE, 128), F32),
            pltpu.VMEM((GROUP, 128), BF16),
            pltpu.VMEM((2, ROWS, 2048), BF16),
            pltpu.VMEM((ROWS, 2048), BF16),
            dma((17,)),
            dma((1,)),
            dma((SEMS["w"],)),
            dma((1,)),
            dma((SEMS["t"],)),
            dma((1,)),
            dma((SEMS["o"],)),
            dma((1,)),
            dma((SEMS["m"],)),
            dma((1,)),
            dma((1,)),
            dma((1,)),
            dma((1,)),
        ],
        compiler_params=pltpu.CompilerParams(
            collective_id=0, has_side_effects=True, vmem_limit_bytes=67043328
        ),
    )(
        tokens,
        norm_gain[None, :],
        w_query,
        w_key.T,
        w_value.T,
        w_glu,
        w_gate,
        sink_logit[None, :],
        conv_taps,
        conv_gain[None, :],
        out_attn,
        out_conv,
        *tables,
    )


def solution(mesh):
    return jax.shard_map(
        per_device,
        mesh=mesh,
        in_specs=(
            P("sp", None),
            P(),
            P("sp", "tp"),
            P("sp", "tp"),
            P("sp", "tp"),
            P("sp", "tp"),
            P("sp", "tp"),
            P("tp"),
            P(None, "tp"),
            P("tp"),
            P("sp", "tp"),
            P("sp", "tp"),
        ),
        out_specs=P("sp", "tp"),
        check_vma=False,
    )
```

```python
import jax
import jax.numpy as jnp
import numpy as np
from jax import lax
from jax.experimental import pallas as pl
from jax.experimental.pallas import tpu as pltpu
from jax.sharding import PartitionSpec as P

MESH = pl.DeviceIdType.MESH
F32 = jnp.float32
BF16 = jnp.bfloat16

ROWS = 256
GROUP = 1024
D = 4096
HEAD = 64
CONV = 2048
KSIZE = 31
WINDOW = 128
WIDTH = 256
OUTW = 512
XCOLS = 384
DCOLS = 512
OUT_SPLIT = 160
SEMS = {"w": 10, "t": 13, "o": 17, "m": 15}


def rope_tables():
    freq = (10000.0 ** (-np.arange(32, dtype=np.float64) * 2.0 / HEAD)).astype(np.float32)
    lanes = np.tile(freq.astype(np.float64), 4)[None, :]
    inner = np.arange(ROWS, dtype=np.float64)[:, None] * lanes
    outer = np.arange(16, dtype=np.float64)[:, None] * ROWS * lanes
    return tuple(
        np.concatenate([np.cos(a), np.sin(a)], axis=1).astype(np.float32) for a in (inner, outer)
    )


class Net:
    def __init__(self, send_sem, recv_sem, meter, partner):
        self.send_sem, self.recv_sem, self.meter, self.partner = send_sem, recv_sem, meter, partner
        self.index, self.size, self.total = {}, {}, 0
        self.joined, self.done = {}, set()

    def join(self, name, *groups):
        for group in groups:
            self.joined[group] = name

    def send(self, group, src, dst, device):
        group = self.joined.get(group, group)
        assert group not in self.done
        k = self.index.setdefault(group, len(self.index))
        assert k < self.recv_sem.shape[0]
        count = src.dtype.itemsize
        for n in src.shape:
            count *= n
        self.size[group] = self.size.get(group, 0) + count
        self.total += count
        pltpu.make_async_remote_copy(
            src_ref=src,
            dst_ref=dst,
            send_sem=self.send_sem.at[0],
            recv_sem=self.recv_sem.at[k],
            device_id=device,
            device_id_type=MESH,
        ).start()

    def await_bytes(self, sem, count):
        tiles = count // 2048
        across = max(n for n in range(1, 33) if tiles % n == 0)
        down = tiles // across
        assert tiles * 2048 == count and down <= 128
        counted = self.meter.at[0 : down * 8, 0 : across * 128]
        pltpu.make_async_copy(counted, counted, sem).wait()

    def wait(self, group):
        group = self.joined.get(group, group)
        if group in self.done:
            return
        self.done.add(group)
        self.await_bytes(self.recv_sem.at[self.index[group]], self.size[group])

    def drain(self):
        self.await_bytes(self.send_sem.at[0], self.total)


def side(d):
    return "lo" if d == 1 else "hi"


class Ring:
    def __init__(self, net, name, ref, device):
        self.net, self.name, self.ref, self.device = net, name, ref, device

    def first(self, *groups):
        for sends in groups:
            for o, part, d in sends:
                r = self.ref(o, 0, part)
                self.net.send((self.name, "T", sends), r, r, self.device(d))

    def first_wait(self, *groups):
        for sends in groups:
            self.net.wait((self.name, "T", sends))

    def second(self, *groups):
        for sends in groups:
            for o, d in sends:
                r = self.ref(o, -d, side(d))
                self.net.send((self.name, "F", sends), r, r, self.device(d))

    def second_wait(self, *groups):
        for sends in groups:
            self.net.wait((self.name, "F", sends))

    def give(self, *groups):
        for items in groups:
            for o, off in items:
                r = self.ref(o, off, "full")
                self.net.send((self.name, "P", items), r, r, self.net.partner)

    def give_wait(self, *groups):
        for items in groups:
            self.net.wait((self.name, "P", items))


def both(*items):
    return tuple((o, part, d) for o, part in items for d in (1, -1))


OWN_A = ((0, "lo", 1), (0, "hi", -1))
OWN_B = ((0, "hi", 1), (0, "lo", -1))
SIDES_A = both((-1, "lo"), (1, "hi"))
SIDES_B = both((-1, "hi"), (1, "lo"))
FAR = both((2, "lo"), (2, "hi"))
FAR_HI, FAR_LO = both((2, "hi")), both((2, "lo"))
FAR_HF = ((2, -1),)
SOON = both((-1, "lo"), (1, "hi"), (-1, "hi"))
SOON_F = ((-1, 1), (1, -1), (-1, -1))
LATE, LATE_F = both((1, "lo")), ((1, 1),)
OWN_F = ((0, 1), (0, -1))
SIDES_AF = ((-1, 1), (1, -1))
SIDES_BF = ((-1, -1), (1, 1))
FAR_F = ((2, 1), (2, -1))
OWN0, OWN1, OWN2 = ((0, 0),), ((0, 1), (0, -1)), ((0, 2),)
SIDES0, SIDES1, SIDES2 = ((-1, 0), (1, 0)), ((-1, 1), (-1, -1), (1, 1), (1, -1)), ((-1, 2), (1, 2))
FAR0, FAR1, FAR2 = ((2, 0),), ((2, 1), (2, -1)), ((2, 2),)


def kernel(
    tokens_hbm,
    gain_hbm,
    wq_hbm,
    wk_hbm,
    wv_hbm,
    wglu_hbm,
    wgate_hbm,
    sink_hbm,
    taps_hbm,
    cgain_hbm,
    oa_hbm,
    oc_hbm,
    inner_hbm,
    outer_hbm,
    out_ref,
    wst,
    transit,
    win,
    wo,
    tok,
    nrmx,
    nrmd,
    meter,
    acc,
    qbuf,
    kvext,
    keys,
    vals,
    gtail,
    ghalo,
    gext,
    kvt,
    gain_ref,
    sink_ref,
    taps_ref,
    cgain_ref,
    gall,
    gfull,
    inner,
    outer,
    taps,
    mx,
    mixall,
    convn,
    local_sem,
    w_send,
    w_recv,
    t_send,
    t_recv,
    o_send,
    o_recv,
    m_send,
    m_recv,
    g_send,
    g_recv,
    halo_send,
    halo_recv,
):
    s = lax.axis_index("sp")
    t = lax.axis_index("tp")
    z, y = s // 4, lax.rem(s, 4)
    x, core = t // 2, lax.rem(t, 2)

    def al(v, m):
        return pl.multiple_of(v, m)

    def wrap(v, o):
        return lax.rem(v + (o + 4), 4)

    def sp_at(dz, dy):
        return wrap(z, dz) * 4 + wrap(y, dy)

    def tp_at(dx, mine=True):
        return wrap(x, dx) * 2 + (core if mine else 1 - core)

    partner = (s, tp_at(0, False))
    barrier = pltpu.get_barrier_semaphore()
    peers = [(sp_at(dz, dy), t) for dz, dy in ((0, 1), (0, -1), (1, 0), (-1, 0))]
    peers += [(s, tp_at(1)), (s, tp_at(-1)), partner]
    for peer in peers:
        pl.semaphore_signal(barrier, inc=1, device_id=peer, device_id_type=MESH)

    role_half = pl.ds(al(lax.rem(y, 2) * 128, 128), 128)
    loads = {}
    for name, src, dst in (
        ("tok", tokens_hbm, tok),
        ("gain", gain_hbm, gain_ref),
        ("wk", wk_hbm, kvt.at[0:64, :]),
        ("wv", wv_hbm, kvt.at[64:128, :]),
        ("q0", wq_hbm.at[:, 0:128], wst.at[2, :, 0:128]),
        ("q1", wq_hbm.at[:, 128:256], wst.at[3, :, 0:128]),
        ("glu0", wglu_hbm.at[:, 0:128], wst.at[0, :, 0:128]),
        ("glu1", wglu_hbm.at[:, 128:256], wst.at[1, :, 0:128]),
        ("gate0", wgate_hbm.at[:, 0:128], wst.at[0, :, 128:256]),
        ("gate1", wgate_hbm.at[:, 128:256], wst.at[1, :, 128:256]),
        ("oa", oa_hbm, wo.at[s, 0:128, :]),
        ("oc", oc_hbm, wo.at[s, 128:256, :]),
        ("taps", taps_hbm.at[:, role_half], taps_ref),
        ("cgain", cgain_hbm, cgain_ref),
        ("sink", sink_hbm, sink_ref),
        ("inner", inner_hbm, inner),
        ("outer", outer_hbm.at[pl.ds(z * 4, 4)], outer),
    ):
        copy = pltpu.make_async_copy(src, dst, local_sem.at[len(loads)])
        copy.start()
        loads[name] = copy

    def loaded(*names):
        for name in names:
            loads[name].wait()

    loaded("wk", "wv")
    kv_t = kvt[...].astype(F32).T.astype(BF16)
    wst[2, :, 128:256] = kv_t
    wst[3, :, 128:256] = kv_t
    loaded("tok", "gain")

    def norm_rows(i, carry):
        v = tok[pl.ds(al(i * 16, 16), 16), :].astype(F32)
        scale = lax.rsqrt(jnp.mean(v * v, axis=1, keepdims=True) + 1e-06)
        v = (v * scale * gain_ref[...]).astype(BF16)
        rows = pl.ds(al(y * ROWS + i * 16, 16), 16)
        for c in range(8):
            nrmx[c, rows, :] = v[:, c * XCOLS : (c + 1) * XCOLS]
        for c in range(2):
            nrmd[c, rows, :] = v[:, 8 * XCOLS + c * DCOLS : 8 * XCOLS + (c + 1) * DCOLS]
        return carry

    lax.fori_loop(0, ROWS // 16, norm_rows, 0)
    loaded("q0", "q1", "glu0", "glu1", "gate0", "gate1")
    pl.semaphore_wait(barrier, len(peers))

    w_net = Net(w_send, w_recv, meter, partner)
    t_net = Net(t_send, t_recv, meter, partner)
    o_net = Net(o_send, o_recv, meter, partner)
    m_net = Net(m_send, m_recv, meter, partner)
    g_net = Net(g_send, g_recv, meter, partner)

    def y_dev(d):
        return (sp_at(0, d), t)

    def z_dev(d):
        return (sp_at(d, 0), t)

    def x_dev(d):
        return (s, tp_at(d))

    def part_of(part, n):
        return {"full": (0, n), "lo": (0, n // 2), "hi": (n // 2, n // 2)}[part]

    def win_ref(o, off, part, mine=True):
        lo, n = part_of(part, ROWS)
        return win.at[pl.ds(al(sp_at(off, o) * ROWS + lo, 128), n), :]

    def tok_rows(o, part):
        lo, n = part_of(part, ROWS)
        return pl.ds(al(wrap(y, o) * ROWS + lo, 128), n)

    def tokx_ref(o, off, part, mine=True):
        return nrmx.at[tp_at(off, mine), tok_rows(o, part), :]

    def tokd_ref(o, off, part, mine=True):
        return nrmd.at[core if mine else 1 - core, tok_rows(o, part), :]

    def along_y(ref):
        return lambda o, off, part, mine=True: ref(off, 0, part, mine)

    tx_y = Ring(t_net, "txy", along_y(tokx_ref), y_dev)
    td_y = Ring(t_net, "tdy", along_y(tokd_ref), y_dev)
    tx_x = Ring(t_net, "txx", tokx_ref, x_dev)
    td_p = Ring(t_net, "tdp", tokd_ref, x_dev)
    w_z = Ring(w_net, "wz", win_ref, z_dev)

    def out_ref_of(h):
        base, size = ((0, OUT_SPLIT), (OUT_SPLIT, ROWS - OUT_SPLIT))[h]

        def first(o, off, part, mine=True):
            lo, n = part_of(part, size)
            src = sp_at(0, off) if h == 0 else sp_at(off, 0)
            return wo.at[src, pl.ds(base + lo, n), :]

        def second(o, off, part, mine=True):
            lo, n = part_of(part, size)
            src = sp_at(off, o) if h == 0 else sp_at(o, off)
            return wo.at[src, pl.ds(base + lo, n), :]

        return first, second

    o_first, o_second = [], []
    for h in (0, 1):
        f, g = out_ref_of(h)
        o_first.append(Ring(o_net, ("of", h), f, (y_dev, z_dev)[h]))
        o_second.append(Ring(o_net, ("os", h), g, (z_dev, y_dev)[h]))

    def w_first(name, parts):
        for d, part in zip((1, -1), parts):
            lo, n = part_of(part, ROWS)
            src = wst.at[wrap(y, d), pl.ds(lo, n), :]
            w_net.send(name, src, win_ref(0, 0, part), y_dev(d))

    for items in (SIDES0, SIDES1, SIDES2):
        t_net.join("sides", ("txx", "P", items), ("tdp", "P", items))
        m_net.join("give", ("mx", "P", items))
    for items in (FAR0, FAR1, FAR2):
        t_net.join("far", ("txx", "P", items), ("tdp", "P", items))
        m_net.join("give", ("mx", "P", items))
    for items in (OWN0, OWN1, OWN2):
        m_net.join("give", ("mx", "P", items))
    for sends in (OWN_F, SIDES_AF, SIDES_BF, FAR_F):
        w_net.join("second", ("wz", "F", sends))
        o_net.join("second", (("os", 0), "F", sends), (("os", 1), "F", sends))
    m_net.join("second", ("mx", "F", SOON_F), ("mx", "F", LATE_F))
    for sends in (SIDES_AF, SIDES_BF):
        t_net.join("second", ("txx", "F", sends))

    tx_y.first(OWN_A)
    w_first("w_a", ("lo", "hi"))
    tx_y.first(OWN_B)
    w_first("w_b", ("hi", "lo"))
    for d in (1, -1):
        lo, n = part_of(side(d), ROWS)
        w_net.send("tr", wst.at[wrap(y, 2), pl.ds(lo, n), :], transit.at[(1 - d) // 2], y_dev(d))
    for name, sends in (("wz_a", OWN_A), ("wz_b", OWN_B)):
        for o, part, d in sends:
            lo, n = part_of(part, ROWS)
            w_net.send(name, wst.at[y, pl.ds(lo, n), :], win_ref(0, 0, part), z_dev(d))
    win[pl.ds(al(s * ROWS, ROWS), ROWS), :] = wst[y]
    loaded("oa", "oc")
    o_first[1].first(OWN_A, OWN_B)

    tx_y.first_wait(OWN_A)
    tx_y.second(OWN_F)
    tx_x.first(SIDES_A)
    w_net.wait("w_a")
    w_z.first(SIDES_A)
    tx_y.first_wait(OWN_B)
    tx_x.first(SIDES_B)
    tx_x.give(SIDES0)
    w_net.wait("w_b")
    w_z.first(SIDES_B)
    w_net.wait("wz_a")
    w_z.second(OWN_F)
    o_second[0].first(OWN_A, OWN_B)
    w_net.wait("tr")
    for d in (1, -1):
        w_net.send("trf", transit.at[(1 - d) // 2], win_ref(-d, 0, side(d)), y_dev(d))
    td_y.first(OWN_A, OWN_B)
    tx_y.second_wait(OWN_F)
    tx_x.first(FAR)
    tx_x.give(FAR0)
    tx_x.first_wait(SIDES_A)
    tx_x.second(SIDES_AF)
    w_net.wait("trf")
    w_z.first(FAR)
    w_z.first_wait(SIDES_A)
    w_z.second(SIDES_AF)
    w_z.first_wait(SIDES_B)
    w_z.second(SIDES_BF)
    tx_x.first_wait(SIDES_B)
    tx_x.second(SIDES_BF)
    tx_x.give(SIDES1)
    w_net.wait("wz_b")
    loaded("taps", "cgain", "sink", "inner", "outer")
    taps[...] = taps_ref[...].astype(F32)
    gall[t] = jnp.broadcast_to(cgain_ref[...], (8, 256))
    td_y.first_wait(OWN_A)
    td_y.second(OWN_F)
    o_first[0].first(OWN_A, OWN_B)
    w_z.first_wait(FAR)
    w_z.second(FAR_F)
    tx_x.first_wait(FAR)
    tx_x.second(FAR_F)
    tx_x.give(FAR1)
    td_y.first_wait(OWN_B)
    td_p.give(SIDES0)
    o_first[1].first_wait(OWN_A)
    o_first[1].second(OWN_F)
    o_first[1].first_wait(OWN_B)
    o_second[1].first(OWN_A, OWN_B, SIDES_A, SIDES_B)
    o_second[0].first_wait(OWN_A)
    o_second[0].second(OWN_F)
    o_second[0].first_wait(OWN_B)
    td_y.second_wait(OWN_F)
    td_p.give(FAR0)
    tx_x.second_wait(SIDES_AF, SIDES_BF)
    tx_x.give(SIDES2)

    def project(o):
        rows = pl.ds(al(wrap(y, o) * ROWS, ROWS), ROWS)
        parts = [nrmx[c, rows, :] for c in range(8)] + [nrmd[c, rows, :] for c in range(2)]
        whole = jnp.concatenate(parts, axis=1)
        acc[rows, :] = jnp.dot(whole, win[...], preferred_element_type=F32)

    def halo_copy(src, dst):
        return pltpu.make_async_remote_copy(
            src_ref=src,
            dst_ref=dst,
            send_sem=halo_send.at[0],
            recv_sem=halo_recv.at[0],
            device_id=z_dev(1),
            device_id_type=MESH,
        )

    lane = lax.broadcasted_iota(jnp.int32, (ROWS, 128), 1)
    first = lax.rem(lane, 64) < 32
    low = lane < 64
    low_w = low[:WINDOW, :]
    kv_halo = halo_copy(kvext.at[pl.ds(GROUP, WINDOW), :], kvext.at[pl.ds(0, WINDOW), :])
    gate_halo = halo_copy(gtail, ghalo)

    def rotate(v, cosine, sine):
        other = jnp.where(first, pltpu.roll(v, 96, 1), pltpu.roll(v, 32, 1))
        return v * cosine + other * sine

    def fill(b):
        rows = pl.ds(al(b * ROWS, ROWS), ROWS)
        ext = pl.ds(al(b * ROWS + WINDOW, WINDOW), ROWS)
        edge = outer[b]
        co, so = edge[:, 0:128], edge[:, 128:256]
        cosine = co * inner[:, 0:128] - so * inner[:, 128:256]
        sine = so * inner[:, 0:128] + co * inner[:, 128:256]
        sine = jnp.where(first, -sine, sine)
        q = rotate(acc[rows, 0:128], cosine, sine).astype(BF16).astype(F32)
        qbuf[rows, :] = (q * 0.125).astype(BF16)
        kv = rotate(acc[rows, 128:256], jnp.where(low, cosine, 1.0), jnp.where(low, sine, 0.0))
        kv = kv.astype(BF16)
        kvext[ext, :] = kv
        kv = kv.astype(F32)
        swapped = pltpu.roll(kv, 64, 1)
        keys[ext, :] = jnp.where(low, kv, swapped).astype(BF16)
        vals[ext, :] = jnp.where(low, swapped, kv).astype(BF16)

    def attend(b):
        zero = jnp.zeros((WINDOW, 128), BF16)
        second = lax.broadcasted_iota(jnp.int32, (2 * WINDOW, 1), 0) >= WINDOW
        sink_a = jnp.where(y == 2, sink_ref[0:1, 0:1], sink_ref[0:1, 2:3])
        sink_b = jnp.where(y == 2, sink_ref[0:1, 1:2], sink_ref[0:1, 3:4])
        sink = jnp.where(second, sink_b, sink_a)
        row_i = lax.rem(lax.broadcasted_iota(jnp.int32, (2 * WINDOW, 2 * WINDOW), 0), WINDOW)
        col_j = lax.broadcasted_iota(jnp.int32, (2 * WINDOW, 2 * WINDOW), 1)
        distance = row_i + WINDOW - col_j
        near = (distance >= 0) & (distance < WINDOW)
        near = near & (z * GROUP + (b - 1) * WINDOW + col_j >= 0)
        at = al(b * WINDOW, WINDOW)
        q = qbuf[pl.ds(at, WINDOW), :]
        stacked = jnp.concatenate([jnp.where(low_w, q, zero), jnp.where(low_w, zero, q)], axis=0)
        scores = lax.dot_general(
            stacked,
            keys[pl.ds(at, 2 * WINDOW), :],
            (((1,), (1,)), ((), ())),
            preferred_element_type=F32,
        )
        scores = jnp.where(near, scores, -1e30)
        top = jnp.maximum(jnp.max(scores, axis=1, keepdims=True), sink)
        e = jnp.exp(scores - top)
        denom = jnp.sum(e, axis=1, keepdims=True) + jnp.exp(sink - top)
        probs = (e * (1.0 / denom)).astype(BF16)
        att = jnp.dot(probs, vals[pl.ds(at, 2 * WINDOW), :], preferred_element_type=F32)
        mx[pl.ds(at, WINDOW), :] = jnp.where(low_w, att[:WINDOW, :], att[WINDOW:, :]).astype(BF16)

    def take_halo():
        kv_halo.wait_recv()
        edge = kvext[0:WINDOW, :].astype(F32)
        swapped = pltpu.roll(edge, 64, 1)
        keys[0:WINDOW, :] = jnp.where(low_w, edge, swapped).astype(BF16)
        vals[0:WINDOW, :] = jnp.where(low_w, swapped, edge).astype(BF16)
        kv_halo.wait_send()

    def attend_early():
        fill(3)
        kv_halo.start()

        def fill_others(i, carry):
            fill(jnp.where(i == 0, 3 - y, 0) + 2 * i)
            return carry

        lax.fori_loop(0, 2, fill_others, 0)

        def pair(i, carry):
            attend(jnp.where(y == 2, 3 + 2 * i, 1 + 5 * i))
            attend(jnp.where(y == 2, 4 + 2 * i, 5 + 2 * i))
            return carry

        lax.fori_loop(0, 2, pair, 0)
        pl.when(y == 3)(take_halo)
        attend(jnp.where(y == 2, 7, 0))

    def attend_late():
        fill(y - 2)
        attend(y)
        attend(jnp.where(y == 2, 1, 4))
        pl.when(y == 2)(take_halo)
        attend(jnp.where(y == 2, 0, 2))

    def gate_rows(b):
        rows = slice(b * ROWS, (b + 1) * ROWS)
        g = acc[rows, 0:128] * (0.5 + 0.5 * jnp.tanh(0.5 * acc[rows, 128:256]))
        gext[b * ROWS + 32 : (b + 1) * ROWS + 32, :] = g.astype(BF16).astype(F32)

    def send_tail():
        gtail[...] = gext[GROUP : GROUP + 32, :].astype(BF16)
        gate_halo.start()

    def filter_rows(r):
        f = jnp.zeros((64, 128), F32)
        for k in range(KSIZE):
            f = f + taps[k : k + 1, :] * gext[r + 2 + k : r + 66 + k, :]
        mx[r : r + 64, :] = f.astype(BF16)

    def late_rows(far):
        return [(far * ROWS + i * 64) % GROUP for i in range(5)]

    def filter_first():
        gate_halo.wait_recv()
        gext[0:32, :] = jnp.where(z > 0, ghalo[...].astype(F32), 0.0)
        filter_rows(0)
        gate_halo.wait_send()

    def filter_early(role):
        far = (role + 2) % 4
        for b in (3, 0, 1, 2):
            if b != far:
                gate_rows(b)
                if b == 3:
                    send_tail()
        for r in range(64, GROUP, 64):
            if r not in late_rows(far):
                filter_rows(r)
        if 0 not in late_rows(far):
            filter_first()

    def filter_late(role):
        far = (role + 2) % 4
        gate_rows(far)
        if far == 3:
            send_tail()
        for r in range(64, GROUP, 64):
            if r in late_rows(far):
                filter_rows(r)
        if 0 in late_rows(far):
            filter_first()

    def by_role(conv, attention):
        for role in range(2):
            pl.when(y == role)(lambda role=role: conv(role))
        pl.when(y >= 2)(attention)

    def mix_ref(o, off, part, mine=True):
        lo, n = part_of(part, ROWS)
        yy = wrap(y, o)
        cols = pl.ds(al(tp_at(off, mine) * 256 + lax.rem(yy, 2) * 128, 128), 128)
        return mixall.at[yy // 2, pl.ds(lo, n), cols]

    m_x = Ring(m_net, "mx", mix_ref, x_dev)
    own_cols = pl.ds(al(t * 256 + lax.rem(y, 2) * 128, 128), 128)

    def m_send(name, o, part):
        lo, n = part_of(part, ROWS)
        src = mx.at[pl.ds(al(wrap(y, o) * ROWS + lo, 128), n), :]
        m_net.send(name, src, mix_ref(0, 0, part), y_dev(o))

    w_z.second_wait(OWN_F, SIDES_AF, SIDES_BF, FAR_F)
    project(0)
    o_first[0].first_wait(OWN_A)
    o_first[0].second(OWN_F)
    o_second[0].first(SIDES_A)
    tx_x.second_wait(FAR_F)
    tx_x.give(FAR2)
    tx_x.give_wait(SIDES0, SIDES1, SIDES2)
    td_p.give_wait(SIDES0)
    project(-1)
    project(1)
    o_first[0].first_wait(OWN_B)
    o_second[0].first(SIDES_B)
    by_role(filter_early, attend_early)
    m_send("m_a", 1, "lo")
    m_send("m_a", -1, "hi")
    m_send("m_a", 1, "hi")
    tx_x.give_wait(FAR0, FAR1, FAR2)
    td_p.give_wait(FAR0)
    project(2)
    mixall[y // 2, :, own_cols] = mx[pl.ds(al(y * ROWS, ROWS), ROWS), :]
    m_x.first(OWN_A, OWN_B)
    m_x.give(OWN0)
    o_first[1].second_wait(OWN_F)
    o_second[1].first(FAR)
    o_second[1].first_wait(OWN_A)
    o_second[1].second(OWN_F)
    o_second[1].first_wait(OWN_B)
    for i in range(1, 8):
        g_net.send("gain", gall.at[t], gall.at[t], (s, lax.rem(t + i, 8)))
    by_role(filter_late, attend_late)
    m_send("m_far_hi", 2, "hi")
    m_send("m_b", -1, "lo")
    m_send("m_far_lo", 2, "lo")
    o_first[0].second_wait(OWN_F)
    o_second[0].first(FAR)
    m_net.wait("m_a")
    m_x.first(SOON)
    m_x.first_wait(OWN_A)
    m_x.second(OWN_F)
    m_x.first_wait(OWN_B)
    m_x.give(OWN1)
    m_net.wait("m_b")
    m_x.first(LATE)
    m_x.give(SIDES0)
    m_net.wait("m_far_hi")
    m_x.first(FAR_HI)
    m_net.wait("m_far_lo")
    m_x.first(FAR_LO)
    m_net.send("m_far_x", mix_ref(2, 0, "lo"), mix_ref(2, 0, "lo"), x_dev(2))
    m_x.give(FAR0)
    for ring in o_second:
        ring.first_wait(SIDES_A)
        ring.second(SIDES_AF)
        ring.first_wait(SIDES_B)
        ring.second(SIDES_BF)
    m_x.second_wait(OWN_F)
    m_x.give(OWN2)
    m_x.first_wait(SOON)
    m_x.second(SOON_F)
    m_x.first_wait(LATE)
    m_x.second(LATE_F)
    m_x.give(SIDES1)
    m_x.first_wait(FAR_HI)
    m_x.second(FAR_HF)
    o_second[1].first_wait(FAR)
    o_second[1].second(FAR_F)
    o_second[0].first_wait(FAR)
    o_second[0].second(FAR_F)
    m_x.first_wait(FAR_LO)
    m_x.give(FAR1)
    g_net.wait("gain")
    for i in range(8):
        gfull[:, i * 256 : (i + 1) * 256] = gall[i, 0:1, :]
    m_x.second_wait(SOON_F, LATE_F)
    m_x.give(SIDES2)
    m_net.wait("m_far_x")
    m_x.second_wait(FAR_HF)
    m_x.give(FAR2)
    m_x.give_wait(OWN0, OWN1, OWN2, SIDES0, SIDES1, SIDES2, FAR0, FAR1, FAR2)

    def channel_norm(i, carry):
        rows = pl.ds(al(i * 32, 32), 32)
        f = mixall[0, rows, :].astype(F32)
        mean_value = jnp.sum(f, axis=1, keepdims=True) * (1.0 / CONV)
        variance = jnp.sum(f * f, axis=1, keepdims=True) * (1.0 / CONV) - mean_value * mean_value
        scaled = (f - mean_value) * lax.rsqrt(variance + 1e-05) * gfull[...]
        convn[rows, :] = (scaled * (0.5 + 0.5 * jnp.tanh(0.5 * scaled))).astype(BF16)
        return carry

    lax.fori_loop(0, ROWS // 32, channel_norm, 0)
    for ring in o_second:
        ring.second_wait(OWN_F, SIDES_AF, SIDES_BF, FAR_F)

    for c in range(0, OUTW, 256):
        w_attn = wo[:, 0:128, c : c + 256].reshape(2048, 256)
        w_conv = wo[:, 128:256, c : c + 256].reshape(2048, 256)
        v = jnp.dot(mixall[1], w_attn, preferred_element_type=F32)
        v = v + jnp.dot(convn[...], w_conv, preferred_element_type=F32)
        out_ref[:, c : c + 256] = v.astype(BF16)

    for net in (w_net, t_net, o_net, m_net, g_net):
        net.drain()


def per_device(
    tokens,
    norm_gain,
    w_query,
    w_key,
    w_value,
    w_glu,
    w_gate,
    sink_logit,
    conv_taps,
    conv_gain,
    out_attn,
    out_conv,
):
    hbm = pl.BlockSpec(memory_space=pltpu.HBM)
    vmem = pl.BlockSpec(memory_space=pltpu.VMEM)
    dma = pltpu.SemaphoreType.DMA
    inner, outer = rope_tables()
    tables = (jnp.asarray(inner), jnp.asarray(outer[:, None, :]))
    return pl.pallas_call(
        kernel,
        name="mixer_layer",
        out_shape=jax.ShapeDtypeStruct((ROWS, OUTW), BF16),
        in_specs=[hbm] * 14,
        out_specs=vmem,
        scratch_shapes=[
            pltpu.VMEM((4, ROWS, WIDTH), BF16),
            pltpu.VMEM((2, 128, WIDTH), BF16),
            pltpu.VMEM((D, WIDTH), BF16),
            pltpu.VMEM((16, ROWS, OUTW), BF16),
            pltpu.VMEM((ROWS, D), BF16),
            pltpu.VMEM((8, GROUP, XCOLS), BF16),
            pltpu.VMEM((2, GROUP, DCOLS), BF16),
            pltpu.VMEM((GROUP, D), BF16),
            pltpu.VMEM((GROUP, WIDTH), F32),
            pltpu.VMEM((GROUP, 128), BF16),
            pltpu.VMEM((GROUP + WINDOW, 128), BF16),
            pltpu.VMEM((GROUP + WINDOW, 128), BF16),
            pltpu.VMEM((GROUP + WINDOW, 128), BF16),
            pltpu.VMEM((32, 128), BF16),
            pltpu.VMEM((32, 128), BF16),
            pltpu.VMEM((GROUP + 32, 128), F32),
            pltpu.VMEM((128, ROWS), BF16),
            pltpu.VMEM((1, D), F32),
            pltpu.VMEM((1, 4), F32),
            pltpu.VMEM((KSIZE, 128), BF16),
            pltpu.VMEM((1, 256), F32),
            pltpu.VMEM((8, 8, 256), F32),
            pltpu.VMEM((1, 2048), F32),
            pltpu.VMEM((ROWS, 256), F32),
            pltpu.VMEM((4, 1, 256), F32),
            pltpu.VMEM((KSIZE, 128), F32),
            pltpu.VMEM((GROUP, 128), BF16),
            pltpu.VMEM((2, ROWS, 2048), BF16),
            pltpu.VMEM((ROWS, 2048), BF16),
            dma((17,)),
            dma((1,)),
            dma((SEMS["w"],)),
            dma((1,)),
            dma((SEMS["t"],)),
            dma((1,)),
            dma((SEMS["o"],)),
            dma((1,)),
            dma((SEMS["m"],)),
            dma((1,)),
            dma((1,)),
            dma((1,)),
            dma((1,)),
        ],
        compiler_params=pltpu.CompilerParams(
            collective_id=0, has_side_effects=True, vmem_limit_bytes=67043328
        ),
    )(
        tokens,
        norm_gain[None, :],
        w_query,
        w_key.T,
        w_value.T,
        w_glu,
        w_gate,
        sink_logit[None, :],
        conv_taps,
        conv_gain[None, :],
        out_attn,
        out_conv,
        *tables,
    )


def solution(mesh):
    return jax.shard_map(
        per_device,
        mesh=mesh,
        in_specs=(
            P("sp", None),
            P(),
            P("sp", "tp"),
            P("sp", "tp"),
            P("sp", "tp"),
            P("sp", "tp"),
            P("sp", "tp"),
            P("tp"),
            P(None, "tp"),
            P("tp"),
            P("sp", "tp"),
            P("sp", "tp"),
        ),
        out_specs=P("sp", "tp"),
        check_vma=False,
    )
```
